512 devices in a mesh: sp: 32 (over z, core), tp: 16 (over y, x).
Axes of the slice: x: 4, y: 4, z: 16, core: 2. Of those that a mesh axis runs over, the one named last changes fastest.
Arguments:
- moe_input: bfloat16 [6144, 2048], P('sp'), may hold values from -6 to 6
- out_grad: bfloat16 [6144, 2048], P('sp'), may hold values from -6 to 6
- route_ids: int32 [6144, 2], P('sp'), may hold values from 0 to 31, all different within a row; in each aligned block of 192 rows (0 to 191, 192 to 383, ...) at most 18 rows name the same one
- route_weights: float32 [6144, 2], P('sp'), may hold values from 0.2 to 2
- expert_gate: bfloat16 [32, 2048, 2048], P('sp', None, 'tp'), may hold values from -0.125 to 0.125
- expert_up: bfloat16 [32, 2048, 2048], P('sp', None, 'tp'), may hold values from -0.125 to 0.125
- expert_down: bfloat16 [32, 2048, 2048], P('sp', 'tp'), may hold values from -0.125 to 0.125
- proj_weight: bfloat16 [1024, 2048], P(None, 'tp'), may hold values from -0.1875 to 0.1875
- glu_value: bfloat16 [1024, 6144], P('tp', 'sp'), may hold values from -6 to 6
- glu_gate: bfloat16 [1024, 6144], P('tp', 'sp'), may hold values from -8 to 8
- conv_taps: float32 [1024, 31], P('tp'), may hold values from -1 to 1
- norm_input: bfloat16 [1024, 6144], P('tp', 'sp'), may hold values from -6 to 6
- norm_gain: float32 [1024], replicated, may hold values from 0.1 to 1.9
Outputs:
- grad_gate: bfloat16 [32, 2048, 2048], P('sp', None, 'tp')
- grad_up: bfloat16 [32, 2048, 2048], P('sp', None, 'tp')
- grad_down: bfloat16 [32, 2048, 2048], P('sp', 'tp')
- grad_proj: float32 [1024, 2048], P('sp', 'tp')
- grad_value: bfloat16 [1024, 6144], P('tp', 'sp')
- grad_glu_gate: bfloat16 [1024, 6144], P('tp', 'sp')
The draws below stay inside these ranges and needn't reach their ends.
Inputs may be any that keep to these rules, and one draw needn't show every extreme that they name: `route_ids`: within the rows of one device, the 2 ids of a position differ and no expert is named by more than 18 pairs; some expert is named by exactly 18.
All inputs are finite; a program needn't handle non-finite values.
Results may differ from the reference program's by a relative error of at most 0.025.
Values may be sent and summed in bfloat16 or wider, within the bound.
No kernel may reach another device: no remote copies, remote signals or barrier semaphores. Data moves between devices by JAX's collectives and lax.ppermute only.
A program may use at most 64 MiB of HBM per device.

```python
import math
import jax
import jax.numpy as jnp
import numpy as np
from jax import lax

D = 2048
FF = 2048
C = 1024
TAPS = 31
TOPK = 2
TOK_DEV = 192
TOKENS = 6144
EXPERTS = 32
CAP = 18
N_SP = 32
N_TP = 16


def spiked(values, stream_key, source, target, parts, factor):
    owner, partner = [(jnp.arange(values.shape[position]) // (values.shape[position] // parts)).reshape([-1 if axis == position else 1 for axis in range(values.ndim)]) for position in (source, target)]
    chosen = jax.random.permutation(stream_key, parts)[partner]
    strong = (owner == chosen) | (owner == (partner + parts // 2) % parts)
    return jnp.where(strong, factor * values, values)


def steps_of(stream_key, extent, pieces, low, largest):
    def one(axis_at, blocks):
        heights = jax.random.uniform(jax.random.fold_in(jax.random.fold_in(stream_key, 6), axis_at), (blocks,), jnp.float32, low / len(pieces), largest / len(pieces))
        return jnp.repeat(jnp.exp(heights), extent[axis_at] // blocks).reshape((-1,) + (1,) * (len(extent) - axis_at - 1))

    loudness = one(*pieces[0])
    for cut in pieces[1:]:
        loudness = loudness * one(*cut)
    return loudness


def deal_out(own_key, own, number, rows, amount, top, limit, lean):
    ranking = jax.random.permutation(own_key, amount)
    heavy_load, ordinary = shares(amount, rows * top, limit, lean, True), shares(amount, rows * top, limit, lean, False)
    places = jnp.arange(amount)

    def named(tallies, turn):
        used = int((tallies > 0).sum())
        fixed = max(1, used // 4)
        moved = fixed + (places - fixed + turn * (used - fixed)) % max(1, amount - fixed)
        return jnp.zeros((amount,), jnp.int32).at[ranking[jnp.where(places < fixed, places, moved)]].set(jnp.asarray(tallies, jnp.int32))

    tallies = jnp.where(number % 4 == 0, named(heavy_load, number // 4), named(ordinary, number - number // 4 - 1))
    mixed = jax.random.permutation(jax.random.fold_in(own, 3), amount)
    donor, taker = mixed[0:amount // 2 * 2:2], mixed[1:amount // 2 * 2:2]
    slack = jnp.minimum(tallies[donor] - 1, limit - tallies[taker]) // 2
    slack = jnp.where((donor == ranking[0]) | (taker == ranking[0]) | (tallies[taker] == 0), 0, jnp.maximum(slack, 0))
    moved = jax.random.randint(jax.random.fold_in(own, 4), (amount // 2,), 0, 1 << 20) % (slack + 1)
    tallies = tallies.at[donor].add(-moved).at[taker].add(moved)
    items = jnp.searchsorted(jnp.cumsum(tallies), jnp.arange(rows * top), side="right").astype(jnp.int32)
    table = items.reshape(top, rows).T
    table = table[jax.random.permutation(jax.random.fold_in(own, 1), rows)]
    turn = jax.random.randint(jax.random.fold_in(own, 2), (rows, 1), 0, top)
    return jnp.take_along_axis(table, (jnp.arange(top)[None, :] + turn) % top, axis=1)


def shares(number_of, total, limit, slope, full):
    weights = [(1 << 20) // math.isqrt(rank ** slope) + 1 for rank in range(1, number_of + 1)]
    largest = limit if full else min(limit, max(-(-total // number_of), total * weights[0] // sum(weights)))
    least = 1 if total - largest >= number_of - 1 else 0
    holding, surplus = [largest] + [least] * (number_of - 1), total - largest - least * (number_of - 1)
    while surplus > 0:
        candidates = [i for i in range(1, number_of) if holding[i] < largest] or [i for i in range(1, number_of) if holding[i] < limit]
        mass, budget = sum([weights[i] for i in candidates]), surplus
        for i in candidates:
            extra = min(limit - holding[i], max(1, budget * weights[i] // mass), surplus)
            holding[i] = holding[i] + extra
            surplus = surplus - extra
    return np.array(holding)


def normal_values(own_key, shape, deviation, limit, pieces=(), kind=jnp.bfloat16):
    result = deviation * jax.random.normal(own_key, shape, jnp.float32)
    if pieces:
        result = result * steps_of(own_key, shape, pieces, -0.22, 0.18)
    return jnp.clip(result, -limit, limit).astype(kind)


def noise_with(rng, shape, width, reach, pieces, heavy, kind=jnp.bfloat16):
    result = width * jax.random.normal(rng, shape, jnp.float32)
    if pieces:
        result = result * steps_of(rng, shape, pieces, -0.22, 0.18)
    return jnp.clip(spiked(result, jax.random.fold_in(rng, 3), *heavy), -reach, reach).astype(kind)


def setup_inputs(seed: int = 0) -> dict:
    key_of = jax.random.split(jax.random.key(seed), 14)
    moe_input = normal_values(key_of[0], (TOKENS, D), 1.0, 6.0, ((0, 32),))
    out_grad = noise_with(key_of[1], (TOKENS, D), 1.0, 6.0, ((0, 32),), (0, 1, 32, 2.75))
    route_ids_keys = jax.random.split(jax.random.fold_in(key_of[2], 1), TOKENS // TOK_DEV)
    route_ids_turns = jax.random.permutation(jax.random.fold_in(key_of[2], 3), TOKENS // TOK_DEV)
    route_ids = jax.vmap(lambda own, number: deal_out(jax.random.fold_in(key_of[2], 2), own, number, TOK_DEV, EXPERTS, TOPK, CAP, 2))(route_ids_keys, route_ids_turns).reshape((TOKENS, TOPK))
    route_weights = jnp.clip(jnp.exp(math.log(2.0) - 2.3025851 * jax.random.uniform(key_of[3], (TOKENS, TOPK), jnp.float32) ** steps_of(key_of[3], (TOKENS, TOPK), ((0, 32),), -0.2, 0.2)), 0.2, 2.0)
    expert_gate = normal_values(key_of[4], (EXPERTS, D, FF), D ** -0.5, 0.125, ((0, 32), (2, 16)))
    expert_up = normal_values(key_of[5], (EXPERTS, D, FF), D ** -0.5, 0.125, ((0, 32), (2, 16)))
    expert_down = normal_values(key_of[6], (EXPERTS, FF, D), FF ** -0.5, 0.125, ((0, 32), (1, 16)))
    proj_weight = normal_values(key_of[7], (C, D), C ** -0.5, 0.1875, ((1, 16),))
    glu_value = normal_values(key_of[8], (C, TOKENS), 1.0, 6.0, ((0, 16), (1, 32)))
    glu_gate = normal_values(key_of[9], (C, TOKENS), 1.5, 8.0, ((0, 16), (1, 32)))
    conv_taps = normal_values(key_of[10], (C, TAPS), TAPS ** -0.5, 1.0, ((0, 16),), jnp.float32)
    norm_input = normal_values(key_of[11], (C, TOKENS), 1.0, 6.0, ((0, 16), (1, 32)))
    norm_gain = jnp.clip(1.0 + 0.18 * jax.random.normal(key_of[12], (C,), jnp.float32), 0.1, 1.9)
    return {"moe_input": moe_input, "out_grad": out_grad, "route_ids": route_ids, "route_weights": route_weights, "expert_gate": expert_gate, "expert_up": expert_up, "expert_down": expert_down, "proj_weight": proj_weight, "glu_value": glu_value, "glu_gate": glu_gate, "conv_taps": conv_taps, "norm_input": norm_input, "norm_gain": norm_gain}


norm_eps = 1e-05

def silu_grad(pre):
    sigmoid_pre = jax.nn.sigmoid(pre)
    return sigmoid_pre * (1.0 + pre * (1.0 - sigmoid_pre))

def reference(moe_input, out_grad, route_ids, route_weights, expert_gate, expert_up, expert_down, proj_weight, glu_value, glu_gate, conv_taps, norm_input, norm_gain):
    pair_ids = route_ids.reshape(N_SP, TOK_DEV * TOPK)
    onehot = (pair_ids[:, :, None] == jnp.arange(EXPERTS, dtype=jnp.int32)[None, None, :]).astype(jnp.int32)
    slot_index = lax.optimization_barrier(jnp.sum((jnp.cumsum(onehot, axis=1) - onehot) * onehot, axis=2))
    source = jnp.arange(N_SP, dtype=jnp.int32)[:, None]
    buffer_row = (source * CAP + slot_index).reshape(-1).astype(jnp.int32)
    expert_of = pair_ids.reshape(-1).astype(jnp.int32)
    pair_token = (jnp.arange(TOKENS * TOPK, dtype=jnp.int32) // TOPK).astype(jnp.int32)
    token_table = jnp.full((EXPERTS, N_SP * CAP), TOKENS, jnp.int32).at[expert_of, buffer_row].set(pair_token)
    weight_table = jnp.zeros((EXPERTS, N_SP * CAP), jnp.float32).at[expert_of, buffer_row].set(route_weights.reshape(-1))
    padded_input = jnp.concatenate([moe_input, jnp.zeros((1, D), jnp.bfloat16)], axis=0)
    padded_grad = jnp.concatenate([out_grad, jnp.zeros((1, D), jnp.bfloat16)], axis=0)

    def one_expert(operands):
        expert_tokens, expert_weights, w_gate, w_up, w_down = operands
        token_rows = padded_input[expert_tokens]
        grad_rows = (padded_grad[expert_tokens].astype(jnp.float32) * expert_weights[:, None]).astype(jnp.bfloat16)
        gate_pre = jnp.dot(token_rows, w_gate, preferred_element_type=jnp.float32)
        up_pre = jnp.dot(token_rows, w_up, preferred_element_type=jnp.float32)
        gate_act = jax.nn.silu(gate_pre)
        hidden = (gate_act * up_pre).astype(jnp.bfloat16)
        down_grad = lax.dot_general(hidden, grad_rows, (((0,), (0,)), ((), ())), preferred_element_type=jnp.float32).astype(jnp.bfloat16)
        grad_hidden = lax.dot_general(grad_rows, w_down, (((1,), (1,)), ((), ())), preferred_element_type=jnp.float32)
        gate_grad = (grad_hidden * up_pre * silu_grad(gate_pre)).astype(jnp.bfloat16)
        up_grad = (grad_hidden * gate_act).astype(jnp.bfloat16)
        gate_wgrad = lax.dot_general(token_rows, gate_grad, (((0,), (0,)), ((), ())), preferred_element_type=jnp.float32).astype(jnp.bfloat16)
        up_wgrad = lax.dot_general(token_rows, up_grad, (((0,), (0,)), ((), ())), preferred_element_type=jnp.float32).astype(jnp.bfloat16)
        rows_count = token_rows.shape[0]
        block_width = FF // N_TP
        gate_blocks = gate_grad.astype(jnp.float32).reshape(rows_count, N_TP, block_width)
        up_blocks = up_grad.astype(jnp.float32).reshape(rows_count, N_TP, block_width)
        wgate_blocks = w_gate.astype(jnp.float32).reshape(D, N_TP, block_width)
        wup_blocks = w_up.astype(jnp.float32).reshape(D, N_TP, block_width)
        partial_value = jnp.einsum('rtf,dtf->trd', gate_blocks, wgate_blocks) + jnp.einsum('rtf,dtf->trd', up_blocks, wup_blocks)
        rounded = lax.optimization_barrier(partial_value.astype(jnp.bfloat16))
        input_grad = lax.optimization_barrier(jnp.sum(rounded.astype(jnp.float32), axis=0)).astype(jnp.bfloat16)
        return (gate_wgrad, up_wgrad, down_grad, input_grad)
    grad_gate, grad_up, grad_down, row_grad = lax.map(one_expert, (token_table, weight_table, expert_gate, expert_up, expert_down))
    moe_grad = jnp.zeros((TOKENS + 1, D), jnp.float32).at[token_table.reshape(-1)].add(row_grad.reshape(-1, D).astype(jnp.float32))[:TOKENS]
    mix_grad = (out_grad.astype(jnp.float32) + moe_grad).astype(jnp.bfloat16)
    conv_values = norm_input.astype(jnp.float32)
    centred = conv_values - lax.optimization_barrier(jnp.mean(conv_values, axis=0, keepdims=True))
    inv_scale = lax.rsqrt(lax.optimization_barrier(jnp.mean(centred * centred, axis=0, keepdims=True)) + norm_eps)
    normed = centred * inv_scale
    scaled = normed * norm_gain[:, None]
    act = jax.nn.silu(scaled).astype(jnp.bfloat16)
    grad_proj = jnp.dot(act, mix_grad, preferred_element_type=jnp.float32)
    grad_act = lax.dot_general(proj_weight, mix_grad, (((1,), (1,)), ((), ())), preferred_element_type=jnp.float32)
    grad_normed = grad_act * silu_grad(scaled) * norm_gain[:, None]
    mean_grad = lax.optimization_barrier(jnp.mean(grad_normed, axis=0, keepdims=True))
    mean_cross = lax.optimization_barrier(jnp.mean(grad_normed * normed, axis=0, keepdims=True))
    grad_conv = inv_scale * (grad_normed - mean_grad - normed * mean_cross)
    reach_back = TAPS - 1
    extended = jnp.pad(grad_conv, ((0, 0), (0, reach_back)))
    grad_glu = jnp.zeros_like(grad_conv)
    for tap_index in range(TAPS):
        grad_glu = grad_glu + conv_taps[:, tap_index:tap_index + 1] * extended[:, reach_back - tap_index:reach_back - tap_index + TOKENS]
    sigmoid_gate = jax.nn.sigmoid(glu_gate.astype(jnp.float32))
    grad_value = (grad_glu * sigmoid_gate).astype(jnp.bfloat16)
    grad_glu_gate = (grad_glu * glu_value.astype(jnp.float32) * sigmoid_gate * (1.0 - sigmoid_gate)).astype(jnp.bfloat16)
    return (grad_gate, grad_up, grad_down, grad_proj, grad_value, grad_glu_gate)
```

```python
import jax
import jax.numpy as jnp
from jax import lax
from jax.experimental import pallas as pl
from jax.experimental.pallas import tpu as pltpu
from jax.sharding import Mesh
from jax.sharding import PartitionSpec as P

TP = ("ty", "tx")
SP = ("z", "core")
PLANE = ("core", "ty", "tx")

norm_eps = 1e-05

bf16, f32, i32 = jnp.bfloat16, jnp.float32, jnp.int32


def exchanged(blocks, axis, index_groups=None):
    return lax.all_to_all(blocks, axis, 0, 0, axis_index_groups=index_groups, tiled=True)


def line_groups(ny, nx):
    along_x = [[y * nx + x for x in range(nx)] for y in range(ny)]
    along_y = [[y * nx + x for y in range(ny)] for x in range(nx)]
    count = ny * nx

    def of_core_one(lines):
        return [[count + i for i in line] for line in lines]

    return along_x + of_core_one(along_y), along_y + of_core_one(along_x)


def silu_grad(pre):
    sig = jax.nn.sigmoid(pre)
    return sig * (1.0 + pre * (1.0 - sig))


def contract(a, b, dim_a, dim_b):
    return lax.dot_general(a, b, (((dim_a,), (dim_b,)), ((), ())), preferred_element_type=f32)


def iota(shape, dim):
    return lax.broadcasted_iota(i32, shape, dim)


def whole():
    return pl.BlockSpec(memory_space=pltpu.VMEM)


def scalar():
    return pl.BlockSpec(memory_space=pltpu.SMEM)


def params(mib):
    return pltpu.CompilerParams(vmem_limit_bytes=mib * 1024 * 1024)


def cost(flops, size):
    return pl.CostEstimate(flops=flops, bytes_accessed=size, transcendentals=0)


def one_if(condition):
    return jnp.where(condition, 1.0, 0.0).astype(bf16)


def prep_kernel(lane_ref, ids_ref, scale_ref, input_ref, grad_ref, *outs, capacity, experts):
    del lane_ref
    sent_ref, back_ref, own_ref = outs
    tok = input_ref.shape[0]
    e0, e1 = ids_ref[0:1, :], ids_ref[1:2, :]
    s0, s1 = scale_ref[0:1, :], scale_ref[1:2, :]
    rows = iota((experts, tok), 0)
    hit0, hit1 = rows == e0, rows == e1
    earlier = one_if(iota((tok, tok), 0) < iota((tok, tok), 1))
    before = jnp.dot(one_if(hit0 | hit1), earlier, preferred_element_type=f32)
    slot0 = jnp.sum(jnp.where(hit0, before, 0.0), axis=0, keepdims=True).astype(i32)
    slot1 = jnp.sum(jnp.where(hit1, before, 0.0), axis=0, keepdims=True).astype(i32)
    x = input_ref[...]
    grad = grad_ref[...]
    own_ref[...] = grad
    diagonal = iota((tok, tok), 0) == iota((tok, tok), 1)
    c0 = jnp.sum(jnp.where(diagonal, s0, 0.0), axis=1, keepdims=True)
    c1 = jnp.sum(jnp.where(diagonal, s1, 0.0), axis=1, keepdims=True)
    g = grad.astype(f32)
    g0, g1 = (g * c0).astype(bf16), (g * c1).astype(bf16)
    pitch = sent_ref.shape[0] // experts
    r = iota((sent_ref.shape[0], tok), 0)
    a0, a1 = e0 * pitch + slot0, e1 * pitch + slot1
    half = pitch // 2
    sent = jnp.dot(one_if((r == a0) | (r == a1)), x, preferred_element_type=f32)
    sent = sent + jnp.dot(one_if(r == a0 + half), g0, preferred_element_type=f32)
    sent = sent + jnp.dot(one_if(r == a1 + half), g1, preferred_element_type=f32)
    sent_ref[...] = sent.astype(bf16)
    back_pitch = back_ref.shape[0] // experts
    r = iota((back_ref.shape[0], tok), 0)
    back_ref[...] = one_if((r == e0 * back_pitch + slot0) | (r == e1 * back_pitch + slot1))


def packed(block):
    lanes = 128
    wide = block[:, :lanes]
    rest = block[:, lanes:]
    rows = rest.shape[0] // 2
    return wide, jnp.concatenate([rest[:rows], rest[rows:]], axis=1)


def unpacked(wide, rest):
    lanes = rest.shape[1] // 2
    tail = jnp.concatenate([rest[:, :lanes], rest[:, lanes:]], axis=0)
    return jnp.concatenate([wide, tail], axis=1)


def compact_kernel(part_ref, norm_ref, out_ref, *, capacity, pitch, sources, group):
    copies, _, width = out_ref.shape
    total = sources * capacity
    rows_in, rows_out = group * pitch, group * capacity
    into, outof = iota((rows_out, rows_in), 0), iota((rows_out, rows_in), 1)
    pick_x = one_if(outof == (into // capacity) * pitch + into % capacity)
    pick_g = one_if(outof == (into // capacity) * pitch + into % capacity + pitch // 2)
    for start in range(0, sources // group):
        piece = part_ref[pl.ds(start * rows_in, rows_in), :]
        x = jnp.dot(pick_x, piece, preferred_element_type=f32).astype(bf16)
        g = jnp.dot(pick_g, piece, preferred_element_type=f32).astype(bf16)
        for c in range(copies):
            out_ref[c, pl.ds(start * rows_out, rows_out), :] = x
            out_ref[c, pl.ds(total + start * rows_out, rows_out), :] = g
    wide, rest = packed(norm_ref[...].astype(f32))
    for c in range(copies):
        out_ref[c, pl.ds(2 * total, wide.shape[0]), :] = wide.astype(bf16)
        out_ref[c, pl.ds(2 * total + wide.shape[0], rest.shape[0]), :] = rest.astype(bf16)


def piece_at(core, y, x):
    return jnp.where(core == 0, y, x), jnp.where(core == 0, x, y)


def expert_kernel(core_ref, rows_ref, grads_ref, gate_ref, up_ref, down_ref, *outs):
    back_ref, hidden_ref, both_ref = outs
    core = core_ref[0]
    ny, nx, _, width = rows_ref.shape
    w_both = jnp.concatenate([gate_ref[...], up_ref[...]], axis=1)
    ff = gate_ref.shape[1]

    def features(ref):
        pieces = []
        for y in range(ny):
            for x in range(nx):
                a, b = piece_at(core, y, x)
                pieces.append(ref[a, b])
        return jnp.concatenate(pieces, axis=1)

    pre = jnp.dot(features(rows_ref), w_both, preferred_element_type=f32)
    gate_pre, up_pre = pre[:, :ff], pre[:, ff:]
    d_hidden = contract(features(grads_ref), down_ref[...], 1, 1)
    sig = jax.nn.sigmoid(gate_pre)
    gate_act = gate_pre * sig
    hidden_ref[...] = (gate_act * up_pre).astype(bf16)
    d_gate = d_hidden * up_pre * (sig * (1.0 + gate_pre * (1.0 - sig)))
    d_up = d_hidden * gate_act
    both = jnp.concatenate([d_gate.astype(bf16), d_up.astype(bf16)], axis=1)
    both_ref[...] = both
    back = contract(both, w_both, 1, 1).astype(bf16)
    for j in range(ny * nx):
        back_ref[j] = back[:, j * width : (j + 1) * width]


def weight_kernel(core_ref, rows_ref, grads_ref, hidden_ref, both_ref, *outs):
    del core_ref
    gate_ref, up_ref, down_ref = outs
    ff = hidden_ref.shape[1]
    pair = contract(rows_ref[0, 0], both_ref[...], 0, 0)
    gate_ref[...] = pair[:, :ff].astype(bf16)
    up_ref[...] = pair[:, ff:].astype(bf16)
    down_ref[...] = contract(hidden_ref[...], grads_ref[0, 0], 0, 0).astype(bf16)


def norm_kernel(core_ref, parts_ref, gain_ref, *outs):
    act_ref, slope_ref, cross_ref, stats_ref = outs
    core = core_ref[0]
    ny, nx, height, _ = parts_ref.shape
    part = height * 2 // 3
    blocks = []
    for y in range(ny):
        for x in range(nx):
            a, b = piece_at(core, y, x)
            block = parts_ref[a, b].astype(f32)
            blocks.append(unpacked(block[:part], block[part:]))
    values = jnp.concatenate(blocks, axis=0)
    channels = values.shape[0]
    mean = jnp.sum(values, axis=0, keepdims=True) / channels
    centred = values - mean
    inv = lax.rsqrt(jnp.sum(centred * centred, axis=0, keepdims=True) / channels + norm_eps)
    gain = gain_ref[...]
    normed = centred * inv
    scaled = normed * gain
    sig = jax.nn.sigmoid(scaled)
    act_ref[...] = (scaled * sig).astype(bf16)
    slope = sig * (1.0 + scaled * (1.0 - sig)) * gain
    slope_ref[...] = slope
    cross_ref[...] = slope * normed
    stats_ref[0:1, :] = mean
    stats_ref[1:2, :] = inv


def row_sum_kernel(parts_ref, out_ref, *, capacity, pitch, group):
    count, total, _ = parts_ref.shape
    rows_in, rows_out = group * capacity, group * pitch
    into, outof = iota((rows_out, rows_in), 0), iota((rows_out, rows_in), 1)
    spread = one_if(
        (outof == (into // pitch) * capacity + into % pitch) & (into % pitch < capacity)
    )
    for start in range(0, total // rows_in):
        at = pl.ds(start * rows_in, rows_in)
        acc = parts_ref[0, at, :].astype(f32)
        for j in range(1, count):
            acc = acc + parts_ref[j, at, :].astype(f32)
        moved = jnp.dot(spread, acc.astype(bf16), preferred_element_type=f32)
        out_ref[pl.ds(start * rows_out, rows_out), :] = moved.astype(bf16)


def mix_kernel(core_ref, back_ref, returned_ref, own_ref, proj_ref, act_ref, slope_ref, cross_ref, *outs):
    kept_ref, given_ref, blocks_ref = outs
    core = core_ref[0]
    moe = contract(back_ref[...], returned_ref[...], 0, 0)
    mix = (own_ref[...].astype(f32) + moe).astype(bf16)
    d_act = contract(proj_ref[...], mix, 1, 1)
    lanes = 128

    def as_rows(line):
        rest = line[:, lanes:]
        return [line[:, :lanes], jnp.concatenate([rest, jnp.zeros_like(rest)], axis=1)]

    tail = []
    for ref in (slope_ref, cross_ref):
        line = jnp.sum(ref[...] * d_act, axis=0, keepdims=True)
        high = line.astype(bf16).astype(f32)
        tail += as_rows(high) + as_rows(line - high)
    tail = jnp.concatenate(tail, axis=0).astype(bf16)
    count = blocks_ref.shape[0]
    part = d_act.shape[0] // count
    for j in range(count):
        wide, rest = packed(d_act[j * part : (j + 1) * part])
        blocks_ref[j, pl.ds(0, part), :] = wide.astype(bf16)
        blocks_ref[j, pl.ds(part, part // 2), :] = rest.astype(bf16)
        blocks_ref[j, pl.ds(part * 3 // 2, 8), :] = tail
    grad = jnp.dot(act_ref[...], mix, preferred_element_type=f32)
    size = kept_ref.shape[1]
    for k in range(kept_ref.shape[0]):
        even = grad[2 * k * size : (2 * k + 1) * size]
        odd = grad[(2 * k + 1) * size : (2 * k + 2) * size]
        kept_ref[k] = jnp.where(core == 0, even, odd)
        given_ref[k] = jnp.where(core == 0, odd, even).astype(bf16)


def conv_grad_kernel(blocks_ref, norm_ref, gain_ref, stats_ref, out_ref, head_ref, *, channels):
    count, height, _ = blocks_ref.shape
    acc = blocks_ref[0].astype(f32)
    for j in range(1, count):
        acc = acc + blocks_ref[j].astype(f32)
    part = out_ref.shape[0]
    grad_act = unpacked(acc[:part], acc[part : part * 3 // 2])
    tail = acc[part * 3 // 2 :]

    def line(at):
        rest = tail[at + 1 : at + 2] + tail[at + 3 : at + 4]
        return jnp.concatenate([tail[at : at + 1] + tail[at + 2 : at + 3], rest[:, : rest.shape[1] // 2]], axis=1)

    mean, inv = stats_ref[0:1, :], stats_ref[1:2, :]
    gain = gain_ref[...]
    normed = (norm_ref[...].astype(f32) - mean) * inv
    grad_normed = grad_act * silu_grad(normed * gain) * gain
    out = inv * (grad_normed - line(0) / channels - normed * (line(4) / channels))
    out_ref[...] = out
    head_ref[...] = out[:, : head_ref.shape[1]]


def body(
    moe_input,
    out_grad,
    route_ids,
    route_weights,
    expert_gate,
    expert_up,
    expert_down,
    proj_weight,
    glu_value,
    glu_gate,
    conv_taps,
    norm_input,
    norm_gain,
):
    groups = lax.axis_size(SP)
    ny, nx = lax.axis_size("ty"), lax.axis_size("tx")
    lane_count = ny * nx
    lane_index = lax.axis_index(TP)
    core = lax.axis_index("core").astype(i32).reshape(1)
    tok_rows, model_width = moe_input.shape
    top_count = route_ids.shape[1]
    capacity = tok_rows * top_count * 3 // (2 * groups)
    total = groups * capacity
    width = model_width // lane_count
    pitch = 40
    back_pitch = 24
    first_groups, second_groups = line_groups(ny, nx)
    channel_part = norm_input.shape[0]
    channels = channel_part * lane_count
    struct = jax.ShapeDtypeStruct

    own_block = pl.BlockSpec((tok_rows, width), lambda i, lane: (0, lane[0]))

    def fixed(*shape):
        return pl.BlockSpec(shape, lambda i, lane: (0,) * len(shape))

    sent, back_place, own_grad = pl.pallas_call(
        lambda *refs: prep_kernel(*refs, capacity=capacity, experts=groups),
        grid_spec=pltpu.PrefetchScalarGridSpec(
            num_scalar_prefetch=1,
            grid=(1,),
            in_specs=[fixed(top_count, tok_rows), fixed(top_count, tok_rows), own_block, own_block],
            out_specs=[fixed(groups * pitch, width), fixed(groups * back_pitch, tok_rows), fixed(tok_rows, width)],
        ),
        out_shape=[
            struct((groups * pitch, width), bf16),
            struct((groups * back_pitch, tok_rows), bf16),
            struct((tok_rows, width), bf16),
        ],
        compiler_params=params(16),
        name="prep",
    )(lane_index.astype(i32).reshape(1), route_ids.T, route_weights.T, moe_input, out_grad)

    part = exchanged(sent.reshape(groups, pitch, width), SP)

    gathered_rows = 2 * total + channel_part * 3 // 2
    spread = pl.pallas_call(
        lambda *refs: compact_kernel(*refs, capacity=capacity, pitch=pitch, sources=groups, group=8),
        out_shape=struct((nx, gathered_rows, width), bf16),
        in_specs=[whole(), whole()],
        out_specs=whole(),
        compiler_params=params(16),
        name="compact",
    )(part.reshape(groups * pitch, width), norm_input)
    line = exchanged(spread, PLANE, first_groups)
    gathered = exchanged(jnp.broadcast_to(line[None], (ny, *line.shape)), PLANE, second_groups)

    w_gate, w_up, w_down = expert_gate[0], expert_up[0], expert_down[0]
    ff = w_gate.shape[1]
    steps = 2
    chunk = total // steps

    def chunk_of(at):
        return pl.BlockSpec((ny, nx, chunk, width), lambda i, s: (0, 0, i + at, 0))

    input_grad, hidden, both = pl.pallas_call(
        expert_kernel,
        grid_spec=pltpu.PrefetchScalarGridSpec(
            num_scalar_prefetch=1,
            grid=(steps,),
            in_specs=[
                chunk_of(0),
                chunk_of(steps),
                fixed(model_width, ff),
                fixed(model_width, ff),
                fixed(ff, model_width),
            ],
            out_specs=[
                pl.BlockSpec((lane_count, chunk, width), lambda i, s: (0, i, 0)),
                pl.BlockSpec((chunk, ff), lambda i, s: (i, 0)),
                pl.BlockSpec((chunk, 2 * ff), lambda i, s: (i, 0)),
            ],
        ),
        out_shape=[
            struct((lane_count, total, width), bf16),
            struct((total, ff), bf16),
            struct((total, 2 * ff), bf16),
        ],
        compiler_params=params(36),
        cost_estimate=cost(10 * total * model_width * ff, 10 * total * model_width),
        name="expert",
    )(core, gathered, gathered, w_gate, w_up, w_down)

    summed_parts = exchanged(input_grad, TP)

    def piece_block(at):
        def index(j, s):
            y, x = j // nx, j % nx
            return (jnp.where(s[0] == 0, y, x), jnp.where(s[0] == 0, x, y), at, 0)

        return pl.BlockSpec((1, 1, total, width), index)

    gate_wgrad, up_wgrad, down_grad = pl.pallas_call(
        weight_kernel,
        grid_spec=pltpu.PrefetchScalarGridSpec(
            num_scalar_prefetch=1,
            grid=(lane_count,),
            in_specs=[piece_block(0), piece_block(1), fixed(total, ff), fixed(total, 2 * ff)],
            out_specs=[
                pl.BlockSpec((width, ff), lambda j, s: (j, 0)),
                pl.BlockSpec((width, ff), lambda j, s: (j, 0)),
                pl.BlockSpec((ff, width), lambda j, s: (0, j)),
            ],
        ),
        out_shape=[
            struct((model_width, ff), bf16),
            struct((model_width, ff), bf16),
            struct((ff, model_width), bf16),
        ],
        compiler_params=params(16),
        cost_estimate=cost(6 * total * model_width * ff, 10 * total * model_width),
        name="weights",
    )(core, gathered, gathered, hidden, both)

    norm_rows = channel_part * 3 // 2
    act, slope, cross, stats = pl.pallas_call(
        norm_kernel,
        grid_spec=pltpu.PrefetchScalarGridSpec(
            num_scalar_prefetch=1,
            grid=(1,),
            in_specs=[
                pl.BlockSpec((ny, nx, norm_rows, width), lambda i, s: (0, 0, 2 * total // norm_rows, 0)),
                fixed(channels, 1),
            ],
            out_specs=[
                fixed(channels, tok_rows),
                fixed(channels, tok_rows),
                fixed(channels, tok_rows),
                fixed(2, tok_rows),
            ],
        ),
        out_shape=[
            struct((channels, tok_rows), bf16),
            struct((channels, tok_rows), f32),
            struct((channels, tok_rows), f32),
            struct((2, tok_rows), f32),
        ],
        compiler_params=params(24),
        cost_estimate=cost(6 * total * model_width * ff, 10 * total * model_width),
        name="norm",
    )(core, gathered, norm_gain[:, None])

    summed_grad = pl.pallas_call(
        lambda *refs: row_sum_kernel(*refs, capacity=capacity, pitch=back_pitch, group=8),
        out_shape=struct((groups * back_pitch, width), bf16),
        in_specs=[whole()],
        out_specs=whole(),
        compiler_params=params(16),
        name="row_sum",
    )(summed_parts)
    returned = exchanged(summed_grad.reshape(groups, back_pitch, width), SP)

    proj_size = channels // groups
    block_rows = norm_rows + 8
    kept, given, blocks = pl.pallas_call(
        mix_kernel,
        out_shape=[
            struct((groups // 2, proj_size, width), f32),
            struct((groups // 2, proj_size, width), bf16),
            struct((lane_count, block_rows, width), bf16),
        ],
        in_specs=[scalar()] + [whole()] * 7,
        out_specs=[whole()] * 3,
        compiler_params=params(24),
        name="mix",
    )(
        core,
        back_place,
        returned.reshape(groups * back_pitch, width),
        own_grad,
        proj_weight,
        act,
        slope,
        cross,
    )
    arrived = exchanged(blocks, TP)
    from_pair = lax.ppermute(given, "core", [(0, 1), (1, 0)])
    chip_sum = (kept + from_pair.astype(f32)).astype(bf16)
    chip_sum, arrived = lax.optimization_barrier((chip_sum, arrived))
    grad_proj = jnp.sum(exchanged(chip_sum, "z").astype(f32), axis=0)

    taps_count = conv_taps.shape[1]
    reach_back = taps_count - 1
    gain_own = lax.dynamic_slice_in_dim(norm_gain, lane_index * channel_part, channel_part, 0)
    grad_conv, head = pl.pallas_call(
        lambda *refs: conv_grad_kernel(*refs, channels=channels),
        out_shape=[struct((channel_part, tok_rows), f32), struct((channel_part, reach_back), f32)],
        in_specs=[whole()] * 4,
        out_specs=[whole()] * 2,
        compiler_params=params(16),
        name="conv_grad",
    )(arrived, norm_input, gain_own[:, None], stats)

    pairs = [(i, i - 1) for i in range(1, groups)]
    ahead_rows = lax.ppermute(head, SP, pairs)
    extended = jnp.concatenate([grad_conv, ahead_rows], axis=1)
    grad_glu = jnp.zeros_like(grad_conv)
    for tap_index in range(taps_count):
        grad_glu = (
            grad_glu
            + conv_taps[:, tap_index : tap_index + 1]
            * extended[:, reach_back - tap_index : reach_back - tap_index + tok_rows]
        )
    sigmoid_gate = jax.nn.sigmoid(glu_gate.astype(f32))
    grad_value = (grad_glu * sigmoid_gate).astype(bf16)
    grad_glu_gate = (
        grad_glu * glu_value.astype(f32) * sigmoid_gate * (1.0 - sigmoid_gate)
    ).astype(bf16)
    return (gate_wgrad[None], up_wgrad[None], down_grad[None], grad_proj, grad_value, grad_glu_gate)


def solution(mesh):
    finer = Mesh(mesh.devices.reshape(mesh.shape["sp"] // 2, 2, 4, 4), ("z", "core", "ty", "tx"))
    return jax.shard_map(
        body,
        mesh=finer,
        in_specs=(
            P(SP, None),
            P(SP, None),
            P(SP, None),
            P(SP, None),
            P(SP, None, TP),
            P(SP, None, TP),
            P(SP, TP, None),
            P(None, TP),
            P(TP, SP),
            P(TP, SP),
            P(TP, None),
            P(TP, SP),
            P(),
        ),
        out_specs=(
            P(SP, None, TP),
            P(SP, None, TP),
            P(SP, TP, None),
            P(SP, TP),
            P(TP, SP),
            P(TP, SP),
        ),
        check_vma=False,
    )
```

```python
import jax
import jax.numpy as jnp
from jax import lax
from jax.experimental import pallas as pl
from jax.experimental.pallas import tpu as pltpu
from jax.sharding import Mesh
from jax.sharding import PartitionSpec as P

TP = ("ty", "tx")
SP = ("z", "core")
PLANE = ("core", "ty", "tx")


norm_eps = 1e-05

bf16, f32, i32 = jnp.bfloat16, jnp.float32, jnp.int32


def exchanged(blocks, axis, index_groups=None):
    return lax.all_to_all(blocks, axis, 0, 0, axis_index_groups=index_groups, tiled=True)


def line_groups(ny, nx):
    along_x = [[y * nx + x for x in range(nx)] for y in range(ny)]
    along_y = [[ny * nx + y * nx + x for y in range(ny)] for x in range(nx)]
    return along_x + along_y


def line_pairs(ny, nx, by):
    pairs = []
    for y in range(ny):
        for x in range(nx):
            pairs.append((y * nx + x, (y + by) % ny * nx + x))
            pairs.append((ny * nx + y * nx + x, ny * nx + y * nx + (x + by) % nx))
    return pairs


def silu_grad(pre):
    sig = jax.nn.sigmoid(pre)
    return sig * (1.0 + pre * (1.0 - sig))


def contract(a, b, dim_a, dim_b):
    return lax.dot_general(a, b, (((dim_a,), (dim_b,)), ((), ())), preferred_element_type=f32)


def iota(shape, dim):
    return lax.broadcasted_iota(i32, shape, dim)


def whole():
    return pl.BlockSpec(memory_space=pltpu.VMEM)


def scalar():
    return pl.BlockSpec(memory_space=pltpu.SMEM)


def params(mib):
    return pltpu.CompilerParams(vmem_limit_bytes=mib * 1024 * 1024)


def cost(flops, size):
    return pl.CostEstimate(flops=flops, bytes_accessed=size, transcendentals=0)


def one_if(condition):
    return jnp.where(condition, 1.0, 0.0).astype(bf16)


def prep_kernel(lane_ref, ids_hbm, scale_hbm, input_hbm, grad_hbm, *refs, experts):
    sent_ref, back_ref, own_ref, ids_ref, scale_ref, input_ref, sems = refs
    tok, width = input_ref.shape
    columns = pl.ds(pl.multiple_of(lane_ref[0] * width, width), width)
    copies = [
        pltpu.make_async_copy(ids_hbm, ids_ref, sems.at[0]),
        pltpu.make_async_copy(scale_hbm, scale_ref, sems.at[1]),
        pltpu.make_async_copy(input_hbm.at[:, columns], input_ref, sems.at[2]),
        pltpu.make_async_copy(grad_hbm.at[:, columns], own_ref, sems.at[3]),
    ]
    for copy in copies:
        copy.start()
    for copy in copies:
        copy.wait()
    e0, e1 = ids_ref[0:1, :], ids_ref[1:2, :]
    s0, s1 = scale_ref[0:1, :], scale_ref[1:2, :]
    rows = iota((experts, tok), 0)
    hit0, hit1 = rows == e0, rows == e1
    earlier = one_if(iota((tok, tok), 0) < iota((tok, tok), 1))
    before = jnp.dot(one_if(hit0 | hit1), earlier, preferred_element_type=f32)
    slot0 = jnp.sum(jnp.where(hit0, before, 0.0), axis=0, keepdims=True).astype(i32)
    slot1 = jnp.sum(jnp.where(hit1, before, 0.0), axis=0, keepdims=True).astype(i32)
    x = input_ref[...]
    grad = own_ref[...]
    diagonal = iota((tok, tok), 0) == iota((tok, tok), 1)
    c0 = jnp.sum(jnp.where(diagonal, s0, 0.0), axis=1, keepdims=True)
    c1 = jnp.sum(jnp.where(diagonal, s1, 0.0), axis=1, keepdims=True)
    g = grad.astype(f32)
    g0, g1 = (g * c0).astype(bf16), (g * c1).astype(bf16)
    pitch = sent_ref.shape[0] // experts
    r = iota((sent_ref.shape[0], tok), 0)
    a0, a1 = e0 * pitch + slot0, e1 * pitch + slot1
    half = pitch // 2
    sent = jnp.dot(one_if((r == a0) | (r == a1)), x, preferred_element_type=f32)
    sent = sent + jnp.dot(one_if(r == a0 + half), g0, preferred_element_type=f32)
    sent = sent + jnp.dot(one_if(r == a1 + half), g1, preferred_element_type=f32)
    sent_ref[...] = sent.astype(bf16)
    back_pitch = back_ref.shape[0] // experts
    r = iota((back_ref.shape[0], tok), 0)
    back_ref[...] = one_if((r == e0 * back_pitch + slot0) | (r == e1 * back_pitch + slot1))


def packed(block):
    lanes = 128
    wide = block[:, :lanes]
    rest = block[:, lanes:]
    rows = rest.shape[0] // 2
    return wide, jnp.concatenate([rest[:rows], rest[rows:]], axis=1)


def unpacked(wide, rest):
    lanes = rest.shape[1] // 2
    tail = jnp.concatenate([rest[:, :lanes], rest[:, lanes:]], axis=0)
    return jnp.concatenate([wide, tail], axis=1)


def compact_kernel(part_ref, norm_ref, out_ref, *, capacity, pitch, sources, group):
    copies, _, width = out_ref.shape
    total = sources * capacity
    rows_in, rows_out = group * pitch, group * capacity
    into, outof = iota((rows_out, rows_in), 0), iota((rows_out, rows_in), 1)
    pick_x = one_if(outof == (into // capacity) * pitch + into % capacity)
    pick_g = one_if(outof == (into // capacity) * pitch + into % capacity + pitch // 2)
    for start in range(0, sources // group):
        piece = part_ref[pl.ds(start * rows_in, rows_in), :]
        x = jnp.dot(pick_x, piece, preferred_element_type=f32).astype(bf16)
        g = jnp.dot(pick_g, piece, preferred_element_type=f32).astype(bf16)
        for c in range(copies):
            out_ref[c, pl.ds(start * rows_out, rows_out), :] = x
            out_ref[c, pl.ds(total + start * rows_out, rows_out), :] = g
    wide, rest = packed(norm_ref[...].astype(f32))
    for c in range(copies):
        out_ref[c, pl.ds(2 * total, wide.shape[0]), :] = wide.astype(bf16)
        out_ref[c, pl.ds(2 * total + wide.shape[0], rest.shape[0]), :] = rest.astype(bf16)


def pieces_of(meta_ref, line_refs):
    core, place = meta_ref[0], meta_ref[1]
    own, behind, ahead, low, high = line_refs
    count = own.shape[0]
    half = low.shape[0]
    found = []
    for ref, away in ((own, 0), (behind, count - 1), (ahead, 1)):
        found += [(ref, i, i, away) for i in range(count)]
    found += [(low, i, i, count // 2) for i in range(half)]
    found += [(high, i, i + half, count // 2) for i in range(count - half)]
    located = []
    for ref, at, i, away in found:
        line = (place + away) % count
        located.append((ref, at, jnp.where(core == 0, line * count + i, i * count + line)))
    return located


def aligned(index, size):
    return pl.ds(pl.multiple_of(index * size, size), size)


def expert_kernel(meta_ref, *refs):
    rows_refs, grads_refs = refs[0:5], refs[5:10]
    gate_ref, up_ref, down_ref, back_ref, hidden_ref, both_ref, w_both_ref, w_down_ref = refs[10:]
    rows_at = pieces_of(meta_ref, rows_refs)
    grads_at = pieces_of(meta_ref, grads_refs)
    width, ff = back_ref.shape[2], gate_ref.shape[1]

    @pl.when(pl.program_id(0) == 0)
    def _():
        for k, (_, _, j) in enumerate(rows_at):
            at, place = pl.ds(k * width, width), aligned(j, width)
            w_both_ref[at, :ff] = gate_ref[place, :]
            w_both_ref[at, ff:] = up_ref[place, :]
            w_down_ref[:, at] = down_ref[:, place]

    w_both = w_both_ref[...]
    x = jnp.concatenate([ref[at] for ref, at, _ in rows_at], axis=1)
    pre = jnp.dot(x, w_both, preferred_element_type=f32)
    gate_pre, up_pre = pre[:, :ff], pre[:, ff:]
    g = jnp.concatenate([ref[at] for ref, at, _ in grads_at], axis=1)
    d_hidden = contract(g, w_down_ref[...], 1, 1)
    sig = jax.nn.sigmoid(gate_pre)
    gate_act = gate_pre * sig
    hidden_ref[...] = (gate_act * up_pre).astype(bf16)
    d_gate = d_hidden * up_pre * (sig * (1.0 + gate_pre * (1.0 - sig)))
    d_up = d_hidden * gate_act
    both = jnp.concatenate([d_gate.astype(bf16), d_up.astype(bf16)], axis=1)
    both_ref[...] = both
    back = contract(both, w_both, 1, 1).astype(bf16)
    for k, (_, _, j) in enumerate(rows_at):
        back_ref[j] = back[:, k * width : (k + 1) * width]


def weight_kernel(meta_ref, own, behind, ahead, low, high, hidden_ref, both_ref, *outs):
    gate_ref, up_ref, down_ref = outs
    width = own.shape[2]
    total, ff = hidden_ref.shape
    both, hidden = both_ref[...], hidden_ref[...]
    for ref, at, j in pieces_of(meta_ref, (own, behind, ahead, low, high)):
        place = aligned(j, width)
        pair = contract(ref[at, pl.ds(0, total), :], both, 0, 0)
        gate_ref[place, :] = pair[:, :ff].astype(bf16)
        up_ref[place, :] = pair[:, ff:].astype(bf16)
        down_ref[:, place] = contract(hidden, ref[at, pl.ds(total, total), :], 0, 0).astype(bf16)


def norm_kernel(meta_ref, own, behind, ahead, low, high, gain_ref, *refs, skip):
    act_ref, slope_ref, cross_ref, stats_ref, values_ref = refs
    height = own.shape[1] - skip
    part = height * 2 // 3
    for ref, at, j in pieces_of(meta_ref, (own, behind, ahead, low, high)):
        block = ref[at, pl.ds(skip, height), :].astype(f32)
        values_ref[aligned(j, part), :] = unpacked(block[:part], block[part:])
    values = values_ref[...]
    channels = values.shape[0]
    mean = jnp.sum(values, axis=0, keepdims=True) / channels
    centred = values - mean
    inv = lax.rsqrt(jnp.sum(centred * centred, axis=0, keepdims=True) / channels + norm_eps)
    gain = gain_ref[...]
    normed = centred * inv
    scaled = normed * gain
    sig = jax.nn.sigmoid(scaled)
    act_ref[...] = (scaled * sig).astype(bf16)
    slope = sig * (1.0 + scaled * (1.0 - sig)) * gain
    slope_ref[...] = slope.astype(bf16)
    cross_ref[...] = (slope * normed).astype(bf16)
    stats_ref[0:1, :] = mean
    stats_ref[1:2, :] = inv


def row_sum_kernel(parts_ref, out_ref, *, capacity, pitch, group):
    count, total, _ = parts_ref.shape
    rows_in, rows_out = group * capacity, group * pitch
    into, outof = iota((rows_out, rows_in), 0), iota((rows_out, rows_in), 1)
    spread = one_if(
        (outof == (into // pitch) * capacity + into % pitch) & (into % pitch < capacity)
    )
    for start in range(0, total // rows_in):
        at = pl.ds(start * rows_in, rows_in)
        acc = parts_ref[0, at, :].astype(f32)
        for j in range(1, count):
            acc = acc + parts_ref[j, at, :].astype(f32)
        moved = jnp.dot(spread, acc.astype(bf16), preferred_element_type=f32)
        out_ref[pl.ds(start * rows_out, rows_out), :] = moved.astype(bf16)


def mix_kernel(meta_ref, *refs):
    sources, outs, local, sems = refs[:7], refs[7:10], refs[10:17], refs[17]
    kept_ref, given_ref, blocks_ref = outs
    back_ref, returned_ref, own_ref, proj_ref, slope_ref, cross_ref, act_ref = local
    core = meta_ref[0]
    copies = [
        pltpu.make_async_copy(source, target, sems.at[i])
        for i, (source, target) in enumerate(zip(sources, local, strict=True))
    ]
    for copy in copies:
        copy.start()
    for copy in copies[:3]:
        copy.wait()
    moe = contract(back_ref[...], returned_ref[...], 0, 0)
    mix = (own_ref[...].astype(f32) + moe).astype(bf16)
    for copy in copies[3:]:
        copy.wait()
    d_act = contract(proj_ref[...], mix, 1, 1)
    lanes = 128

    def as_rows(line):
        rest = line[:, lanes:]
        return [line[:, :lanes], jnp.concatenate([rest, jnp.zeros_like(rest)], axis=1)]

    tail = []
    for ref in (slope_ref, cross_ref):
        line = jnp.sum(ref[...].astype(f32) * d_act, axis=0, keepdims=True)
        high = line.astype(bf16).astype(f32)
        tail += as_rows(high) + as_rows(line - high)
    tail = jnp.concatenate(tail, axis=0).astype(bf16)
    count = blocks_ref.shape[0]
    part = d_act.shape[0] // count
    for j in range(count):
        wide, rest = packed(d_act[j * part : (j + 1) * part])
        blocks_ref[j, pl.ds(0, part), :] = wide.astype(bf16)
        blocks_ref[j, pl.ds(part, part // 2), :] = rest.astype(bf16)
        blocks_ref[j, pl.ds(part * 3 // 2, 8), :] = tail
    grad = jnp.dot(act_ref[...], mix, preferred_element_type=f32)
    size = kept_ref.shape[1]
    for k in range(kept_ref.shape[0]):
        even = grad[2 * k * size : (2 * k + 1) * size]
        odd = grad[(2 * k + 1) * size : (2 * k + 2) * size]
        kept_ref[k] = jnp.where(core == 0, even, odd).astype(bf16)
        given_ref[k] = jnp.where(core == 0, odd, even).astype(bf16)


def conv_grad_kernel(blocks_ref, norm_ref, gain_ref, stats_ref, out_ref, head_ref, *, channels):
    count, height, _ = blocks_ref.shape
    acc = blocks_ref[0].astype(f32)
    for j in range(1, count):
        acc = acc + blocks_ref[j].astype(f32)
    part = out_ref.shape[0]
    grad_act = unpacked(acc[:part], acc[part : part * 3 // 2])
    tail = acc[part * 3 // 2 :]

    def line(at):
        rest = tail[at + 1 : at + 2] + tail[at + 3 : at + 4]
        return jnp.concatenate([tail[at : at + 1] + tail[at + 2 : at + 3], rest[:, : rest.shape[1] // 2]], axis=1)

    mean, inv = stats_ref[0:1, :], stats_ref[1:2, :]
    gain = gain_ref[...]
    normed = (norm_ref[...].astype(f32) - mean) * inv
    grad_normed = grad_act * silu_grad(normed * gain) * gain
    out = inv * (grad_normed - line(0) / channels - normed * (line(4) / channels))
    out_ref[...] = out
    head_ref[...] = out[:, : head_ref.shape[1]]


def body(
    moe_input,
    out_grad,
    route_ids,
    route_weights,
    expert_gate,
    expert_up,
    expert_down,
    proj_weight,
    glu_value,
    glu_gate,
    conv_taps,
    norm_input,
    norm_gain,
):
    groups = lax.axis_size(SP)
    ny, nx = lax.axis_size("ty"), lax.axis_size("tx")
    lane_count = ny * nx
    lane_index = lax.axis_index(TP)
    tok_rows, model_width = moe_input.shape
    top_count = route_ids.shape[1]
    capacity = tok_rows * top_count * 3 // (2 * groups)
    total = groups * capacity
    width = model_width // lane_count
    pitch = 40
    back_pitch = 24
    channel_part = norm_input.shape[0]
    channels = channel_part * lane_count
    struct = jax.ShapeDtypeStruct

    sent, back_place, own_grad = pl.pallas_call(
        lambda *refs: prep_kernel(*refs, experts=groups),
        in_specs=[scalar()] + [pl.BlockSpec(memory_space=pltpu.HBM)] * 4,
        out_specs=[whole()] * 3,
        out_shape=[
            struct((groups * pitch, width), bf16),
            struct((groups * back_pitch, tok_rows), bf16),
            struct((tok_rows, width), bf16),
        ],
        scratch_shapes=[
            pltpu.VMEM((top_count, tok_rows), i32),
            pltpu.VMEM((top_count, tok_rows), f32),
            pltpu.VMEM((tok_rows, width), bf16),
            pltpu.SemaphoreType.DMA((4,)),
        ],
        compiler_params=params(58),
        name="prep",
    )(lane_index.astype(i32).reshape(1), route_ids.T, route_weights.T, moe_input, out_grad)

    part = exchanged(sent.reshape(groups, pitch, width), SP)

    gathered_rows = 2 * total + channel_part * 3 // 2
    spread = pl.pallas_call(
        lambda *refs: compact_kernel(*refs, capacity=capacity, pitch=pitch, sources=groups, group=8),
        out_shape=struct((nx, gathered_rows, width), bf16),
        in_specs=[whole(), whole()],
        out_specs=whole(),
        compiler_params=params(16),
        name="compact",
    )(part.reshape(groups * pitch, width), norm_input)
    line = exchanged(spread, PLANE, line_groups(ny, nx))
    onward, backward = line_pairs(ny, nx, 1), line_pairs(ny, nx, -1)
    behind = lax.ppermute(line, PLANE, onward)
    ahead = lax.ppermute(line, PLANE, backward)
    low = lax.ppermute(behind[: nx // 2], PLANE, onward)
    high = lax.ppermute(ahead[nx // 2 :], PLANE, backward)
    lines = (line, behind, ahead, low, high)
    core = lax.axis_index("core")
    place = jnp.where(core == 0, lax.axis_index("ty"), lax.axis_index("tx"))
    meta = jnp.stack([core, place]).astype(i32)

    w_gate, w_up, w_down = expert_gate[0], expert_up[0], expert_down[0]
    ff = w_gate.shape[1]
    steps = 3
    chunk = total // steps

    def chunks(at):
        return [
            pl.BlockSpec((piece.shape[0], chunk, width), lambda i, m: (0, i + at, 0)) for piece in lines
        ]

    def fixed(*shape):
        return pl.BlockSpec(shape, lambda i, m: (0,) * len(shape))

    input_grad, hidden, both = pl.pallas_call(
        expert_kernel,
        grid_spec=pltpu.PrefetchScalarGridSpec(
            num_scalar_prefetch=1,
            grid=(steps,),
            in_specs=[
                *chunks(0),
                *chunks(steps),
                fixed(model_width, ff),
                fixed(model_width, ff),
                fixed(ff, model_width),
            ],
            out_specs=[
                pl.BlockSpec((lane_count, chunk, width), lambda i, m: (0, i, 0)),
                pl.BlockSpec((chunk, ff), lambda i, m: (i, 0)),
                pl.BlockSpec((chunk, 2 * ff), lambda i, m: (i, 0)),
            ],
            scratch_shapes=[pltpu.VMEM((model_width, 2 * ff), bf16), pltpu.VMEM((ff, model_width), bf16)],
        ),
        out_shape=[
            struct((lane_count, total, width), bf16),
            struct((total, ff), bf16),
            struct((total, 2 * ff), bf16),
        ],
        compiler_params=params(58),
        cost_estimate=cost(10 * total * model_width * ff, 10 * total * model_width),
        name="expert",
    )(meta, *lines, *lines, w_gate, w_up, w_down)

    summed_parts = exchanged(input_grad, TP)

    gate_wgrad, up_wgrad, down_grad = pl.pallas_call(
        weight_kernel,
        in_specs=[scalar()] + [whole()] * 7,
        out_specs=[whole()] * 3,
        out_shape=[
            struct((model_width, ff), bf16),
            struct((model_width, ff), bf16),
            struct((ff, model_width), bf16),
        ],
        compiler_params=params(58),
        cost_estimate=cost(6 * total * model_width * ff, 10 * total * model_width),
        name="weights",
    )(meta, *lines, hidden, both)
    summed_parts, gate_wgrad, up_wgrad, down_grad = lax.optimization_barrier(
        (summed_parts, gate_wgrad, up_wgrad, down_grad)
    )

    norm_rows = channel_part * 3 // 2
    act, slope, cross, stats = pl.pallas_call(
        lambda *refs: norm_kernel(*refs, skip=2 * total),
        in_specs=[scalar()] + [whole()] * 6,
        out_specs=[whole()] * 4,
        out_shape=[
            struct((channels, tok_rows), bf16),
            struct((channels, tok_rows), bf16),
            struct((channels, tok_rows), bf16),
            struct((2, tok_rows), f32),
        ],
        scratch_shapes=[pltpu.VMEM((channels, tok_rows), f32)],
        compiler_params=params(58),
        cost_estimate=cost(6 * total * model_width * ff, 10 * total * model_width),
        name="norm",
    )(meta, *lines, norm_gain[:, None])

    summed_grad = pl.pallas_call(
        lambda *refs: row_sum_kernel(*refs, capacity=capacity, pitch=back_pitch, group=8),
        out_shape=struct((groups * back_pitch, width), bf16),
        in_specs=[whole()],
        out_specs=whole(),
        compiler_params=params(16),
        name="row_sum",
    )(summed_parts)
    returned = exchanged(summed_grad.reshape(groups, back_pitch, width), SP)

    proj_size = channels // groups
    block_rows = norm_rows + 8
    mix_inputs = (
        back_place,
        returned.reshape(groups * back_pitch, width),
        own_grad,
        proj_weight,
        slope,
        cross,
        act,
    )
    kept, given, blocks = pl.pallas_call(
        mix_kernel,
        out_shape=[
            struct((groups // 2, proj_size, width), bf16),
            struct((groups // 2, proj_size, width), bf16),
            struct((lane_count, block_rows, width), bf16),
        ],
        in_specs=[scalar()] + [pl.BlockSpec(memory_space=pltpu.HBM)] * len(mix_inputs),
        out_specs=[whole()] * 3,
        scratch_shapes=[pltpu.VMEM(value.shape, value.dtype) for value in mix_inputs]
        + [pltpu.SemaphoreType.DMA((len(mix_inputs),))],
        compiler_params=params(58),
        name="mix",
    )(meta, *mix_inputs)
    arrived = exchanged(blocks, TP)
    from_pair = lax.ppermute(given, "core", [(0, 1), (1, 0)])
    chip_sum = (kept.astype(f32) + from_pair.astype(f32)).astype(bf16)
    chip_sum, arrived = lax.optimization_barrier((chip_sum, arrived))
    grad_proj = jnp.sum(exchanged(chip_sum, "z").astype(f32), axis=0)

    taps_count = conv_taps.shape[1]
    reach_back = taps_count - 1
    gain_own = lax.dynamic_slice_in_dim(norm_gain, lane_index * channel_part, channel_part, 0)
    grad_conv, head = pl.pallas_call(
        lambda *refs: conv_grad_kernel(*refs, channels=channels),
        out_shape=[struct((channel_part, tok_rows), f32), struct((channel_part, reach_back), f32)],
        in_specs=[whole()] * 4,
        out_specs=[whole()] * 2,
        compiler_params=params(16),
        name="conv_grad",
    )(arrived, norm_input, gain_own[:, None], stats)

    pairs = [(i, i - 1) for i in range(1, groups)]
    ahead_rows = lax.ppermute(head, SP, pairs)
    extended = jnp.concatenate([grad_conv, ahead_rows], axis=1)
    grad_glu = jnp.zeros_like(grad_conv)
    for tap_index in range(taps_count):
        grad_glu = (
            grad_glu
            + conv_taps[:, tap_index : tap_index + 1]
            * extended[:, reach_back - tap_index : reach_back - tap_index + tok_rows]
        )
    sigmoid_gate = jax.nn.sigmoid(glu_gate.astype(f32))
    grad_value = (grad_glu * sigmoid_gate).astype(bf16)
    grad_glu_gate = (
        grad_glu * glu_value.astype(f32) * sigmoid_gate * (1.0 - sigmoid_gate)
    ).astype(bf16)
    return (gate_wgrad[None], up_wgrad[None], down_grad[None], grad_proj, grad_value, grad_glu_gate)


def solution(mesh):
    finer = Mesh(mesh.devices.reshape(mesh.shape["sp"] // 2, 2, 4, 4), ("z", "core", "ty", "tx"))
    return jax.shard_map(
        body,
        mesh=finer,
        in_specs=(
            P(SP, None),
            P(SP, None),
            P(SP, None),
            P(SP, None),
            P(SP, None, TP),
            P(SP, None, TP),
            P(SP, TP, None),
            P(None, TP),
            P(TP, SP),
            P(TP, SP),
            P(TP, None),
            P(TP, SP),
            P(),
        ),
        out_specs=(
            P(SP, None, TP),
            P(SP, None, TP),
            P(SP, TP, None),
            P(SP, TP),
            P(TP, SP),
            P(TP, SP),
        ),
        check_vma=False,
    )
```

```python
import jax
import jax.numpy as jnp
from jax import lax
from jax.experimental import pallas as pl
from jax.experimental.pallas import tpu as pltpu
from jax.sharding import Mesh
from jax.sharding import PartitionSpec as P

TP = ("ty", "tx")
SP = ("z", "core")
PLANE = ("core", "ty", "tx")


norm_eps = 1e-05

bf16, f32, i32 = jnp.bfloat16, jnp.float32, jnp.int32


def exchanged(blocks, axis, index_groups=None):
    return lax.all_to_all(blocks, axis, 0, 0, axis_index_groups=index_groups, tiled=True)


def line_groups(ny, nx):
    along_x = [[y * nx + x for x in range(nx)] for y in range(ny)]
    along_y = [[y * nx + x for y in range(ny)] for x in range(nx)]

    def of_core_one(lines):
        return [[ny * nx + i for i in line] for line in lines]

    return along_x + of_core_one(along_y), along_y + of_core_one(along_x)


def line_pairs(ny, nx, by):
    pairs = []
    for y in range(ny):
        for x in range(nx):
            pairs.append((y * nx + x, y * nx + (x + by) % nx))
            pairs.append((ny * nx + y * nx + x, ny * nx + (y + by) % ny * nx + x))
    return pairs


def silu_grad(pre):
    sig = jax.nn.sigmoid(pre)
    return sig * (1.0 + pre * (1.0 - sig))


def contract(a, b, dim_a, dim_b):
    return lax.dot_general(a, b, (((dim_a,), (dim_b,)), ((), ())), preferred_element_type=f32)


def iota(shape, dim):
    return lax.broadcasted_iota(i32, shape, dim)


def whole():
    return pl.BlockSpec(memory_space=pltpu.VMEM)


def scalar():
    return pl.BlockSpec(memory_space=pltpu.SMEM)


def params(mib):
    return pltpu.CompilerParams(vmem_limit_bytes=mib * 1024 * 1024)


def cost(flops, size):
    return pl.CostEstimate(flops=flops, bytes_accessed=size, transcendentals=0)


def one_if(condition):
    return jnp.where(condition, 1.0, 0.0).astype(bf16)


def prep_kernel(lane_ref, ids_hbm, scale_hbm, input_hbm, grad_hbm, *refs, experts):
    sent_ref, back_ref, own_ref, ids_ref, scale_ref, input_ref, sems = refs
    tok, width = input_ref.shape
    columns = pl.ds(pl.multiple_of(lane_ref[0] * width, width), width)
    copies = [
        pltpu.make_async_copy(ids_hbm, ids_ref, sems.at[0]),
        pltpu.make_async_copy(scale_hbm, scale_ref, sems.at[1]),
        pltpu.make_async_copy(input_hbm.at[:, columns], input_ref, sems.at[2]),
        pltpu.make_async_copy(grad_hbm.at[:, columns], own_ref, sems.at[3]),
    ]
    for copy in copies:
        copy.start()
    for copy in copies:
        copy.wait()
    e0, e1 = ids_ref[0:1, :], ids_ref[1:2, :]
    s0, s1 = scale_ref[0:1, :], scale_ref[1:2, :]
    rows = iota((experts, tok), 0)
    hit0, hit1 = rows == e0, rows == e1
    earlier = one_if(iota((tok, tok), 0) < iota((tok, tok), 1))
    before = jnp.dot(one_if(hit0 | hit1), earlier, preferred_element_type=f32)
    slot0 = jnp.sum(jnp.where(hit0, before, 0.0), axis=0, keepdims=True).astype(i32)
    slot1 = jnp.sum(jnp.where(hit1, before, 0.0), axis=0, keepdims=True).astype(i32)
    x = input_ref[...]
    grad = own_ref[...]
    diagonal = iota((tok, tok), 0) == iota((tok, tok), 1)
    c0 = jnp.sum(jnp.where(diagonal, s0, 0.0), axis=1, keepdims=True)
    c1 = jnp.sum(jnp.where(diagonal, s1, 0.0), axis=1, keepdims=True)
    g = grad.astype(f32)
    g0, g1 = (g * c0).astype(bf16), (g * c1).astype(bf16)
    pitch = sent_ref.shape[0] // experts
    r = iota((sent_ref.shape[0], tok), 0)
    a0, a1 = e0 * pitch + slot0, e1 * pitch + slot1
    half = pitch // 2
    sent = jnp.dot(one_if((r == a0) | (r == a1)), x, preferred_element_type=f32)
    sent = sent + jnp.dot(one_if(r == a0 + half), g0, preferred_element_type=f32)
    sent = sent + jnp.dot(one_if(r == a1 + half), g1, preferred_element_type=f32)
    sent_ref[...] = sent.astype(bf16)
    back_pitch = back_ref.shape[0] // experts
    r = iota((back_ref.shape[0], tok), 0)
    back_ref[...] = one_if((r == e0 * back_pitch + slot0) | (r == e1 * back_pitch + slot1))


def packed(block):
    lanes = 128
    wide = block[:, :lanes]
    rest = block[:, lanes:]
    rows = rest.shape[0] // 2
    return wide, jnp.concatenate([rest[:rows], rest[rows:]], axis=1)


def unpacked(wide, rest):
    lanes = rest.shape[1] // 2
    tail = jnp.concatenate([rest[:, :lanes], rest[:, lanes:]], axis=0)
    return jnp.concatenate([wide, tail], axis=1)


def compact_kernel(part_ref, norm_ref, out_ref, *, capacity, pitch):
    count = out_ref.shape[0]
    rows_in = part_ref.shape[0] // count
    rows_out = rows_in // pitch * capacity
    into, outof = iota((rows_out, rows_in), 0), iota((rows_out, rows_in), 1)
    pick_x = one_if(outof == (into // capacity) * pitch + into % capacity)
    pick_g = one_if(outof == (into // capacity) * pitch + into % capacity + pitch // 2)
    wide, rest = packed(norm_ref[...].astype(f32))
    wide, rest = wide.astype(bf16), rest.astype(bf16)
    for q in range(count):
        piece = part_ref[pl.ds(q * rows_in, rows_in), :]
        out_ref[q, pl.ds(0, rows_out), :] = jnp.dot(pick_x, piece, preferred_element_type=f32).astype(bf16)
        out_ref[q, pl.ds(rows_out, rows_out), :] = jnp.dot(pick_g, piece, preferred_element_type=f32).astype(bf16)
        out_ref[q, pl.ds(2 * rows_out, wide.shape[0]), :] = wide
        out_ref[q, pl.ds(2 * rows_out + wide.shape[0], rest.shape[0]), :] = rest


def pieces_of(core_ref, ny, nx):
    core = core_ref[0]
    return [
        (jnp.where(core == 0, y, x), jnp.where(core == 0, x, y)) for y in range(ny) for x in range(nx)
    ]


def pack_kernel(gate_ref, up_ref, down_ref, out_ref, sems):
    height, width = gate_ref.shape
    copies = [
        pltpu.make_async_copy(gate_ref, out_ref.at[pl.ds(0, height)], sems.at[0]),
        pltpu.make_async_copy(up_ref, out_ref.at[pl.ds(height, height)], sems.at[1]),
    ]
    for k in range(height // width):
        copies.append(
            pltpu.make_async_copy(
                down_ref.at[:, pl.ds(k * width, width)],
                out_ref.at[pl.ds(2 * height + k * width, width)],
                sems.at[2 + k],
            )
        )
    for copy in copies:
        copy.start()
    for copy in copies:
        copy.wait()


def expert_kernel(core_ref, rows_hbm, *refs):
    weights_hbm = refs[0:4]
    back_ref, hidden_ref, both_ref, rows_ref = refs[4:8]
    weights, acc_ref, sems = refs[8:12], refs[12], refs[13]
    copies = [
        pltpu.make_async_copy(source, target, sems.at[i])
        for i, (source, target) in enumerate(zip((rows_hbm, *weights_hbm), (rows_ref, *weights), strict=True))
    ]
    for copy in copies:
        copy.start()
    ny, nx, _, width = rows_ref.shape
    count = hidden_ref.shape[0]
    pieces = pieces_of(core_ref, ny, nx)
    height = ny * nx * width
    copies[0].wait()
    x = jnp.concatenate([rows_ref[a, b, pl.ds(0, count), :] for a, b in pieces], axis=1)
    g = jnp.concatenate([rows_ref[a, b, pl.ds(count, count), :] for a, b in pieces], axis=1)
    for k, block in enumerate(weights):
        copies[1 + k].wait()
        w_both = jnp.concatenate([block[pl.ds(0, height), :], block[pl.ds(height, height), :]], axis=1)
        w_down = jnp.concatenate(
            [block[pl.ds(2 * height + i * width, width), :] for i in range(ny * nx)], axis=1
        )
        pre = jnp.dot(x, w_both, preferred_element_type=f32)
        gate_pre, up_pre = pre[:, :width], pre[:, width:]
        d_hidden = contract(g, w_down, 1, 1)
        sig = jax.nn.sigmoid(gate_pre)
        gate_act = gate_pre * sig
        hidden_ref[:, pl.ds(k * width, width)] = (gate_act * up_pre).astype(bf16)
        d_gate = d_hidden * up_pre * (sig * (1.0 + gate_pre * (1.0 - sig)))
        d_up = d_hidden * gate_act
        both = jnp.concatenate([d_gate.astype(bf16), d_up.astype(bf16)], axis=1)
        both_ref[:, pl.ds(2 * k * width, 2 * width)] = both
        back = contract(both, w_both, 1, 1)
        acc_ref[...] = back if k == 0 else acc_ref[...] + back
    for j, (a, b) in enumerate(pieces):
        back_ref[a, b] = acc_ref[:, pl.ds(j * width, width)].astype(bf16)


def weight_kernel(core_ref, rows_ref, hidden_ref, both_ref, *outs):
    ny, nx, _, width = rows_ref.shape
    count = hidden_ref.shape[0]
    height = ny * nx * width
    for j, (a, b) in enumerate(pieces_of(core_ref, ny, nx)):
        pairs = contract(rows_ref[a, b, pl.ds(0, count), :], both_ref[...], 0, 0).astype(bf16)
        downs = contract(hidden_ref[...], rows_ref[a, b, pl.ds(count, count), :], 0, 0).astype(bf16)
        for k, out_ref in enumerate(outs):
            out_ref[pl.ds(j * width, width), :] = pairs[:, 2 * k * width : (2 * k + 1) * width]
            out_ref[pl.ds(height + j * width, width), :] = pairs[:, (2 * k + 1) * width : (2 * k + 2) * width]
            out_ref[pl.ds(2 * height + j * width, width), :] = downs[k * width : (k + 1) * width]


def weight_sum_kernel(p0, p1, p2, p3, gate_ref, up_ref, down_ref):
    def summed(part):
        return (
            (p0[part, 0].astype(f32) + p1[part, 0].astype(f32)) + (p2[part, 0].astype(f32) + p3[part, 0].astype(f32))
        ).astype(bf16)

    gate_ref[...] = summed(0)
    up_ref[...] = summed(1)
    down = summed(2)
    size = down_ref.shape[0]
    for k in range(down.shape[0] // size):
        down_ref[:, pl.ds(k * size, size)] = down[k * size : (k + 1) * size]


def norm_kernel(core_ref, parts_ref, gain_ref, act_ref, slope_ref, cross_ref, stats_ref):
    ny, nx, height, _ = parts_ref.shape
    part = height * 2 // 3
    blocks = []
    for a, b in pieces_of(core_ref, ny, nx):
        block = parts_ref[a, b].astype(f32)
        blocks.append(unpacked(block[:part], block[part:]))
    values = jnp.concatenate(blocks, axis=0)
    channels = values.shape[0]
    mean = jnp.sum(values, axis=0, keepdims=True) / channels
    centred = values - mean
    inv = lax.rsqrt(jnp.sum(centred * centred, axis=0, keepdims=True) / channels + norm_eps)
    gain = gain_ref[...]
    normed = centred * inv
    scaled = normed * gain
    sig = jax.nn.sigmoid(scaled)
    act_ref[...] = (scaled * sig).astype(bf16)
    slope = sig * (1.0 + scaled * (1.0 - sig)) * gain
    slope_ref[...] = slope.astype(bf16)
    cross_ref[...] = (slope * normed).astype(bf16)
    stats_ref[0:1, :] = mean
    stats_ref[1:2, :] = inv


def line_sum_kernel(parts_ref, out_ref):
    acc = parts_ref[0].astype(f32)
    for j in range(1, parts_ref.shape[0]):
        acc = acc + parts_ref[j].astype(f32)
    out_ref[...] = acc.astype(bf16)


def spread_kernel(rows_ref, out_ref, *, capacity, pitch):
    count, rows_in, _ = rows_ref.shape
    rows_out = rows_in // capacity * pitch
    into, outof = iota((rows_out, rows_in), 0), iota((rows_out, rows_in), 1)
    spread = one_if((outof == (into // pitch) * capacity + into % pitch) & (into % pitch < capacity))
    for q in range(count):
        moved = jnp.dot(spread, rows_ref[q], preferred_element_type=f32)
        out_ref[pl.ds(q * rows_out, rows_out), :] = moved.astype(bf16)


def mix_kernel(core_ref, *refs):
    sources, outs, local, sems = refs[:7], refs[7:10], refs[10:17], refs[17]
    kept_ref, given_ref, blocks_ref = outs
    back_ref, returned_ref, own_ref, proj_ref, slope_ref, cross_ref, act_ref = local
    core = core_ref[0]
    copies = [
        pltpu.make_async_copy(source, target, sems.at[i])
        for i, (source, target) in enumerate(zip(sources, local, strict=True))
    ]
    for copy in copies:
        copy.start()
    for copy in copies[:3]:
        copy.wait()
    moe = contract(back_ref[...], returned_ref[...], 0, 0)
    mix = (own_ref[...].astype(f32) + moe).astype(bf16)
    for copy in copies[3:]:
        copy.wait()
    d_act = contract(proj_ref[...], mix, 1, 1)
    lanes = 128

    def as_rows(line):
        rest = line[:, lanes:]
        return [line[:, :lanes], jnp.concatenate([rest, jnp.zeros_like(rest)], axis=1)]

    tail = []
    for ref in (slope_ref, cross_ref):
        line = jnp.sum(ref[...].astype(f32) * d_act, axis=0, keepdims=True)
        high = line.astype(bf16).astype(f32)
        tail += as_rows(high) + as_rows(line - high)
    tail = jnp.concatenate(tail, axis=0).astype(bf16)
    count = blocks_ref.shape[0]
    part = d_act.shape[0] // count
    for j in range(count):
        wide, rest = packed(d_act[j * part : (j + 1) * part])
        blocks_ref[j, pl.ds(0, part), :] = wide.astype(bf16)
        blocks_ref[j, pl.ds(part, part // 2), :] = rest.astype(bf16)
        blocks_ref[j, pl.ds(part * 3 // 2, 8), :] = tail
    grad = jnp.dot(act_ref[...], mix, preferred_element_type=f32)
    size = kept_ref.shape[1]
    for k in range(kept_ref.shape[0]):
        even = grad[2 * k * size : (2 * k + 1) * size]
        odd = grad[(2 * k + 1) * size : (2 * k + 2) * size]
        kept_ref[k] = jnp.where(core == 0, even, odd).astype(bf16)
        given_ref[k] = jnp.where(core == 0, odd, even).astype(bf16)


def conv_grad_kernel(blocks_ref, norm_ref, gain_ref, stats_ref, out_ref, head_ref, *, channels):
    count, height, _ = blocks_ref.shape
    acc = blocks_ref[0].astype(f32)
    for j in range(1, count):
        acc = acc + blocks_ref[j].astype(f32)
    part = out_ref.shape[0]
    grad_act = unpacked(acc[:part], acc[part : part * 3 // 2])
    tail = acc[part * 3 // 2 :]

    def line(at):
        rest = tail[at + 1 : at + 2] + tail[at + 3 : at + 4]
        return jnp.concatenate([tail[at : at + 1] + tail[at + 2 : at + 3], rest[:, : rest.shape[1] // 2]], axis=1)

    mean, inv = stats_ref[0:1, :], stats_ref[1:2, :]
    gain = gain_ref[...]
    normed = (norm_ref[...].astype(f32) - mean) * inv
    grad_normed = grad_act * silu_grad(normed * gain) * gain
    out = inv * (grad_normed - line(0) / channels - normed * (line(4) / channels))
    out_ref[...] = out
    head_ref[...] = out[:, : head_ref.shape[1]]


def body(
    moe_input,
    out_grad,
    route_ids,
    route_weights,
    expert_gate,
    expert_up,
    expert_down,
    proj_weight,
    glu_value,
    glu_gate,
    conv_taps,
    norm_input,
    norm_gain,
):
    groups = lax.axis_size(SP)
    ny, nx = lax.axis_size("ty"), lax.axis_size("tx")
    lane_count = ny * nx
    lane_index = lax.axis_index(TP)
    tok_rows, model_width = moe_input.shape
    top_count = route_ids.shape[1]
    capacity = tok_rows * top_count * 3 // (2 * groups)
    total = groups * capacity
    width = model_width // lane_count
    pitch = 40
    back_pitch = 24
    channel_part = norm_input.shape[0]
    channels = channel_part * lane_count
    struct = jax.ShapeDtypeStruct

    sent, back_place, own_grad = pl.pallas_call(
        lambda *refs: prep_kernel(*refs, experts=groups),
        in_specs=[scalar()] + [pl.BlockSpec(memory_space=pltpu.HBM)] * 4,
        out_specs=[whole()] * 3,
        out_shape=[
            struct((groups * pitch, width), bf16),
            struct((groups * back_pitch, tok_rows), bf16),
            struct((tok_rows, width), bf16),
        ],
        scratch_shapes=[
            pltpu.VMEM((top_count, tok_rows), i32),
            pltpu.VMEM((top_count, tok_rows), f32),
            pltpu.VMEM((tok_rows, width), bf16),
            pltpu.SemaphoreType.DMA((4,)),
        ],
        compiler_params=params(58),
        name="prep",
    )(lane_index.astype(i32).reshape(1), route_ids.T, route_weights.T, moe_input, out_grad)

    part = exchanged(sent.reshape(groups, pitch, width), SP)

    core = lax.axis_index("core").astype(i32).reshape(1)
    first_groups, second_groups = line_groups(ny, nx)
    w_gate, w_up, w_down = expert_gate[0], expert_up[0], expert_down[0]
    ff = w_gate.shape[1]
    hbm = pl.BlockSpec(memory_space=pltpu.HBM)
    w_gate, w_up, w_down, _ = lax.optimization_barrier((w_gate, w_up, w_down, sent))
    own_weights = pl.pallas_call(
        pack_kernel,
        out_shape=struct((3 * model_width, ff), bf16),
        in_specs=[hbm] * 3,
        out_specs=hbm,
        scratch_shapes=[pltpu.SemaphoreType.DMA((2 + lane_count,))],
        compiler_params=params(58),
        cost_estimate=cost(8 * total * model_width * ff, 6 * model_width * ff),
        name="pack",
    )(w_gate, w_up, w_down)
    onward, backward, across = [line_pairs(ny, nx, by) for by in (1, -1, 2)]
    with jax.named_scope("weights_out"):
        weights = (
            own_weights,
            lax.ppermute(own_weights, PLANE, onward),
            lax.ppermute(own_weights, PLANE, backward),
            lax.ppermute(own_weights, PLANE, across),
        )

    quarter = total // nx
    norm_rows = channel_part * 3 // 2
    rows_height = 2 * quarter + norm_rows
    quarters = pl.pallas_call(
        lambda *refs: compact_kernel(*refs, capacity=capacity, pitch=pitch),
        out_shape=struct((nx, rows_height, width), bf16),
        in_specs=[whole(), whole()],
        out_specs=whole(),
        compiler_params=params(16),
        name="compact",
    )(part.reshape(groups * pitch, width), norm_input)
    quarters = exchanged(quarters, PLANE, first_groups)
    gathered = exchanged(jnp.broadcast_to(quarters[None], (ny, *quarters.shape)), PLANE, second_groups)

    packed_weights = pltpu.VMEM((3 * model_width, ff), bf16)
    back, hidden, both = pl.pallas_call(
        expert_kernel,
        in_specs=[scalar()] + [hbm] * 5,
        out_specs=[whole()] * 3,
        out_shape=[
            struct((ny, nx, quarter, width), bf16),
            struct((quarter, nx * ff), bf16),
            struct((quarter, 2 * nx * ff), bf16),
        ],
        scratch_shapes=[
            pltpu.VMEM((ny, nx, rows_height, width), bf16),
            packed_weights,
            packed_weights,
            packed_weights,
            packed_weights,
            pltpu.VMEM((quarter, model_width), f32),
            pltpu.SemaphoreType.DMA((5,)),
        ],
        compiler_params=params(58),
        cost_estimate=cost(10 * total * model_width * ff, 10 * total * model_width),
        name="expert",
    )(core, gathered, *weights)

    with jax.named_scope("line_sum"):
        line_parts = exchanged(back, PLANE, second_groups)
    line_rows = pl.pallas_call(
        line_sum_kernel,
        out_shape=struct((nx, quarter, width), bf16),
        in_specs=[whole()],
        out_specs=whole(),
        compiler_params=params(16),
        name="line_sum",
    )(line_parts)
    own_rows = exchanged(line_rows, PLANE, first_groups)
    summed_grad = pl.pallas_call(
        lambda *refs: spread_kernel(*refs, capacity=capacity, pitch=back_pitch),
        out_shape=struct((groups * back_pitch, width), bf16),
        in_specs=[whole()],
        out_specs=whole(),
        compiler_params=params(16),
        name="spread",
    )(own_rows)
    with jax.named_scope("rows_back"):
        returned = exchanged(summed_grad.reshape(groups, back_pitch, width), SP)

    wgrads = pl.pallas_call(
        weight_kernel,
        in_specs=[scalar()] + [whole()] * 3,
        out_specs=[whole()] * nx,
        out_shape=[struct((3 * model_width, ff), bf16)] * nx,
        compiler_params=params(58),
        cost_estimate=cost(6 * total * model_width * ff, 10 * total * model_width),
        name="weights",
    )(core, gathered, hidden, both)
    with jax.named_scope("weights_back"):
        line_wgrads = (
            wgrads[0],
            lax.ppermute(wgrads[1], PLANE, backward),
            lax.ppermute(wgrads[2], PLANE, onward),
            lax.ppermute(wgrads[3], PLANE, across),
        )

    act, slope, cross, stats = pl.pallas_call(
        norm_kernel,
        grid_spec=pltpu.PrefetchScalarGridSpec(
            num_scalar_prefetch=1,
            grid=(1,),
            in_specs=[
                pl.BlockSpec((ny, nx, norm_rows, width), lambda i, m: (0, 0, 2 * quarter // norm_rows, 0)),
                pl.BlockSpec((channels, 1), lambda i, m: (0, 0)),
            ],
            out_specs=[pl.BlockSpec((channels, tok_rows), lambda i, m: (0, 0))] * 3
            + [pl.BlockSpec((2, tok_rows), lambda i, m: (0, 0))],
        ),
        out_shape=[struct((channels, tok_rows), bf16)] * 3 + [struct((2, tok_rows), f32)],
        compiler_params=params(58),
        cost_estimate=cost(6 * total * model_width * ff, 10 * total * model_width),
        name="norm",
    )(core, gathered, norm_gain[:, None])

    proj_size = channels // groups
    block_rows = norm_rows + 8
    mix_inputs = (
        back_place,
        returned.reshape(groups * back_pitch, width),
        own_grad,
        proj_weight,
        slope,
        cross,
        act,
    )
    kept, given, blocks = pl.pallas_call(
        mix_kernel,
        out_shape=[
            struct((groups // 2, proj_size, width), bf16),
            struct((groups // 2, proj_size, width), bf16),
            struct((lane_count, block_rows, width), bf16),
        ],
        in_specs=[scalar()] + [pl.BlockSpec(memory_space=pltpu.HBM)] * len(mix_inputs),
        out_specs=[whole()] * 3,
        scratch_shapes=[pltpu.VMEM(value.shape, value.dtype) for value in mix_inputs]
        + [pltpu.SemaphoreType.DMA((len(mix_inputs),))],
        compiler_params=params(58),
        name="mix",
    )(core, *mix_inputs)
    arrived = exchanged(blocks, TP)
    from_pair = lax.ppermute(given, "core", [(0, 1), (1, 0)])
    chip_sum = (kept.astype(f32) + from_pair.astype(f32)).astype(bf16)
    chip_sum, arrived = lax.optimization_barrier((chip_sum, arrived))
    grad_proj = jnp.sum(exchanged(chip_sum, "z").astype(f32), axis=0)

    taps_count = conv_taps.shape[1]
    reach_back = taps_count - 1
    gain_own = lax.dynamic_slice_in_dim(norm_gain, lane_index * channel_part, channel_part, 0)
    grad_conv, head = pl.pallas_call(
        lambda *refs: conv_grad_kernel(*refs, channels=channels),
        out_shape=[struct((channel_part, tok_rows), f32), struct((channel_part, reach_back), f32)],
        in_specs=[whole()] * 4,
        out_specs=[whole()] * 2,
        compiler_params=params(16),
        name="conv_grad",
    )(arrived, norm_input, gain_own[:, None], stats)

    pairs = [(i, i - 1) for i in range(1, groups)]
    ahead_rows = lax.ppermute(head, SP, pairs)
    extended = jnp.concatenate([grad_conv, ahead_rows], axis=1)
    grad_glu = jnp.zeros_like(grad_conv)
    for tap_index in range(taps_count):
        grad_glu = (
            grad_glu
            + conv_taps[:, tap_index : tap_index + 1]
            * extended[:, reach_back - tap_index : reach_back - tap_index + tok_rows]
        )
    sigmoid_gate = jax.nn.sigmoid(glu_gate.astype(f32))
    grad_value = (grad_glu * sigmoid_gate).astype(bf16)
    grad_glu_gate = (
        grad_glu * glu_value.astype(f32) * sigmoid_gate * (1.0 - sigmoid_gate)
    ).astype(bf16)
    sum_rows = 256
    sum_steps = model_width // sum_rows
    parts = [value.reshape(3, sum_steps, sum_rows, ff) for value in line_wgrads]
    gate_wgrad, up_wgrad, down_grad = pl.pallas_call(
        weight_sum_kernel,
        grid=(sum_steps,),
        in_specs=[pl.BlockSpec((3, 1, sum_rows, ff), lambda i: (0, i, 0, 0))] * 4,
        out_specs=[
            pl.BlockSpec((sum_rows, ff), lambda i: (i, 0)),
            pl.BlockSpec((sum_rows, ff), lambda i: (i, 0)),
            pl.BlockSpec((ff, sum_rows), lambda i: (0, i)),
        ],
        out_shape=[
            struct((model_width, ff), bf16),
            struct((model_width, ff), bf16),
            struct((ff, model_width), bf16),
        ],
        compiler_params=params(58),
        cost_estimate=cost(6 * total * model_width * ff, 10 * total * model_width),
        name="weight_sum",
    )(*parts)
    return (gate_wgrad[None], up_wgrad[None], down_grad[None], grad_proj, grad_value, grad_glu_gate)


def solution(mesh):
    finer = Mesh(mesh.devices.reshape(mesh.shape["sp"] // 2, 2, 4, 4), ("z", "core", "ty", "tx"))
    return jax.shard_map(
        body,
        mesh=finer,
        in_specs=(
            P(SP, None),
            P(SP, None),
            P(SP, None),
            P(SP, None),
            P(SP, None, TP),
            P(SP, None, TP),
            P(SP, TP, None),
            P(None, TP),
            P(TP, SP),
            P(TP, SP),
            P(TP, None),
            P(TP, SP),
            P(),
        ),
        out_specs=(
            P(SP, None, TP),
            P(SP, None, TP),
            P(SP, TP, None),
            P(SP, TP),
            P(TP, SP),
            P(TP, SP),
        ),
        check_vma=False,
    )
```

```python
import jax
import jax.numpy as jnp
from jax import lax
from jax.experimental import pallas as pl
from jax.experimental.pallas import tpu as pltpu
from jax.sharding import Mesh
from jax.sharding import PartitionSpec as P

TP = ("ty", "tx")
SP = ("z", "core")
PLANE = ("core", "ty", "tx")


norm_eps = 1e-05

bf16, f32, i32 = jnp.bfloat16, jnp.float32, jnp.int32


def exchanged(blocks, axis, index_groups=None):
    return lax.all_to_all(blocks, axis, 0, 0, axis_index_groups=index_groups, tiled=True)


def line_groups(ny, nx):
    along_x = [[y * nx + x for x in range(nx)] for y in range(ny)]
    along_y = [[y * nx + x for y in range(ny)] for x in range(nx)]

    def of_core_one(lines):
        return [[ny * nx + i for i in line] for line in lines]

    return along_x + of_core_one(along_y), along_y + of_core_one(along_x)


def line_pairs(ny, nx, by):
    pairs = []
    for y in range(ny):
        for x in range(nx):
            pairs.append((y * nx + x, y * nx + (x + by) % nx))
            pairs.append((ny * nx + y * nx + x, ny * nx + (y + by) % ny * nx + x))
    return pairs


def silu_grad(pre):
    sig = jax.nn.sigmoid(pre)
    return sig * (1.0 + pre * (1.0 - sig))


def contract(a, b, dim_a, dim_b):
    return lax.dot_general(a, b, (((dim_a,), (dim_b,)), ((), ())), preferred_element_type=f32)


def iota(shape, dim):
    return lax.broadcasted_iota(i32, shape, dim)


def whole():
    return pl.BlockSpec(memory_space=pltpu.VMEM)


def scalar():
    return pl.BlockSpec(memory_space=pltpu.SMEM)


def params(mib):
    return pltpu.CompilerParams(vmem_limit_bytes=mib * 1024 * 1024)


def cost(flops, size):
    return pl.CostEstimate(flops=flops, bytes_accessed=size, transcendentals=0)


def one_if(condition):
    return jnp.where(condition, 1.0, 0.0).astype(bf16)


def prep_kernel(lane_ref, ids_hbm, scale_hbm, input_hbm, grad_hbm, *refs, experts):
    sent_ref, back_ref, own_ref, ids_ref, scale_ref, input_ref, sems = refs
    tok, width = input_ref.shape
    columns = pl.ds(pl.multiple_of(lane_ref[0] * width, width), width)
    copies = [
        pltpu.make_async_copy(ids_hbm, ids_ref, sems.at[0]),
        pltpu.make_async_copy(scale_hbm, scale_ref, sems.at[1]),
        pltpu.make_async_copy(input_hbm.at[:, columns], input_ref, sems.at[2]),
        pltpu.make_async_copy(grad_hbm.at[:, columns], own_ref, sems.at[3]),
    ]
    for copy in copies:
        copy.start()
    for copy in copies:
        copy.wait()
    e0, e1 = ids_ref[0:1, :], ids_ref[1:2, :]
    s0, s1 = scale_ref[0:1, :], scale_ref[1:2, :]
    rows = iota((experts, tok), 0)
    hit0, hit1 = rows == e0, rows == e1
    earlier = one_if(iota((tok, tok), 0) < iota((tok, tok), 1))
    before = jnp.dot(one_if(hit0 | hit1), earlier, preferred_element_type=f32)
    slot0 = jnp.sum(jnp.where(hit0, before, 0.0), axis=0, keepdims=True).astype(i32)
    slot1 = jnp.sum(jnp.where(hit1, before, 0.0), axis=0, keepdims=True).astype(i32)
    x = input_ref[...]
    grad = own_ref[...]
    diagonal = iota((tok, tok), 0) == iota((tok, tok), 1)
    c0 = jnp.sum(jnp.where(diagonal, s0, 0.0), axis=1, keepdims=True)
    c1 = jnp.sum(jnp.where(diagonal, s1, 0.0), axis=1, keepdims=True)
    g = grad.astype(f32)
    g0, g1 = (g * c0).astype(bf16), (g * c1).astype(bf16)
    pitch = sent_ref.shape[0] // experts
    r = iota((sent_ref.shape[0], tok), 0)
    a0, a1 = e0 * pitch + slot0, e1 * pitch + slot1
    half = pitch // 2
    sent = jnp.dot(one_if((r == a0) | (r == a1)), x, preferred_element_type=f32)
    sent = sent + jnp.dot(one_if(r == a0 + half), g0, preferred_element_type=f32)
    sent = sent + jnp.dot(one_if(r == a1 + half), g1, preferred_element_type=f32)
    sent_ref[...] = sent.astype(bf16)
    back_pitch = back_ref.shape[0] // experts
    r = iota((back_ref.shape[0], tok), 0)
    back_ref[...] = one_if((r == e0 * back_pitch + slot0) | (r == e1 * back_pitch + slot1))


def packed(block):
    lanes = 128
    wide = block[:, :lanes]
    rest = block[:, lanes:]
    rows = rest.shape[0] // 2
    return wide, jnp.concatenate([rest[:rows], rest[rows:]], axis=1)


def unpacked(wide, rest):
    lanes = rest.shape[1] // 2
    tail = jnp.concatenate([rest[:, :lanes], rest[:, lanes:]], axis=0)
    return jnp.concatenate([wide, tail], axis=1)


def compact_kernel(part_ref, norm_ref, out_ref, *, capacity, pitch):
    count = out_ref.shape[0]
    rows_in = part_ref.shape[0] // count
    rows_out = rows_in // pitch * capacity
    into, outof = iota((rows_out, rows_in), 0), iota((rows_out, rows_in), 1)
    pick_x = one_if(outof == (into // capacity) * pitch + into % capacity)
    pick_g = one_if(outof == (into // capacity) * pitch + into % capacity + pitch // 2)
    wide, rest = packed(norm_ref[...].astype(f32))
    wide, rest = wide.astype(bf16), rest.astype(bf16)
    for q in range(count):
        piece = part_ref[pl.ds(q * rows_in, rows_in), :]
        out_ref[q, pl.ds(0, rows_out), :] = jnp.dot(pick_x, piece, preferred_element_type=f32).astype(bf16)
        out_ref[q, pl.ds(rows_out, rows_out), :] = jnp.dot(pick_g, piece, preferred_element_type=f32).astype(bf16)
        out_ref[q, pl.ds(2 * rows_out, wide.shape[0]), :] = wide
        out_ref[q, pl.ds(2 * rows_out + wide.shape[0], rest.shape[0]), :] = rest


def pieces_of(core_ref, ny, nx):
    core = core_ref[0]
    return [
        (jnp.where(core == 0, y, x), jnp.where(core == 0, x, y)) for y in range(ny) for x in range(nx)
    ]


def pack_kernel(gate_ref, up_ref, down_ref, out_ref):
    height, width = gate_ref.shape
    out_ref[pl.ds(0, height), :] = gate_ref[...]
    out_ref[pl.ds(height, height), :] = up_ref[...]
    for k in range(height // width):
        out_ref[pl.ds(2 * height + k * width, width), :] = down_ref[:, pl.ds(k * width, width)]


def expert_kernel(core_ref, rows_hbm, *refs):
    weights_hbm = refs[0:4]
    back_ref, hidden_ref, both_ref, rows_ref = refs[4:8]
    weights, acc_ref, sems = refs[8:12], refs[12], refs[13]
    copies = [
        pltpu.make_async_copy(source, target, sems.at[i])
        for i, (source, target) in enumerate(zip((rows_hbm, *weights_hbm), (rows_ref, *weights), strict=True))
    ]
    for copy in copies:
        copy.start()
    ny, nx, _, width = rows_ref.shape
    count = hidden_ref.shape[0]
    pieces = pieces_of(core_ref, ny, nx)
    height = ny * nx * width
    copies[0].wait()
    x = jnp.concatenate([rows_ref[a, b, pl.ds(0, count), :] for a, b in pieces], axis=1)
    g = jnp.concatenate([rows_ref[a, b, pl.ds(count, count), :] for a, b in pieces], axis=1)
    for k, block in enumerate(weights):
        copies[1 + k].wait()
        w_both = jnp.concatenate([block[pl.ds(0, height), :], block[pl.ds(height, height), :]], axis=1)
        w_down = jnp.concatenate(
            [block[pl.ds(2 * height + i * width, width), :] for i in range(ny * nx)], axis=1
        )
        pre = jnp.dot(x, w_both, preferred_element_type=f32)
        gate_pre, up_pre = pre[:, :width], pre[:, width:]
        d_hidden = contract(g, w_down, 1, 1)
        sig = jax.nn.sigmoid(gate_pre)
        gate_act = gate_pre * sig
        hidden_ref[:, pl.ds(k * width, width)] = (gate_act * up_pre).astype(bf16)
        d_gate = d_hidden * up_pre * (sig * (1.0 + gate_pre * (1.0 - sig)))
        d_up = d_hidden * gate_act
        both = jnp.concatenate([d_gate.astype(bf16), d_up.astype(bf16)], axis=1)
        both_ref[:, pl.ds(2 * k * width, 2 * width)] = both
        back = contract(both, w_both, 1, 1)
        acc_ref[...] = back if k == 0 else acc_ref[...] + back
    for j, (a, b) in enumerate(pieces):
        back_ref[a, b] = acc_ref[:, pl.ds(j * width, width)].astype(bf16)


def weight_kernel(core_ref, rows_ref, hidden_ref, both_ref, *outs):
    ny, nx, _, width = rows_ref.shape
    count = hidden_ref.shape[0]
    height = ny * nx * width
    for j, (a, b) in enumerate(pieces_of(core_ref, ny, nx)):
        pairs = contract(rows_ref[a, b, pl.ds(0, count), :], both_ref[...], 0, 0).astype(bf16)
        downs = contract(hidden_ref[...], rows_ref[a, b, pl.ds(count, count), :], 0, 0).astype(bf16)
        for k, out_ref in enumerate(outs):
            out_ref[pl.ds(j * width, width), :] = pairs[:, 2 * k * width : (2 * k + 1) * width]
            out_ref[pl.ds(height + j * width, width), :] = pairs[:, (2 * k + 1) * width : (2 * k + 2) * width]
            out_ref[pl.ds(2 * height + j * width, width), :] = downs[k * width : (k + 1) * width]


def weight_sum_kernel(p0, p1, p2, p3, gate_ref, up_ref, down_ref):
    def summed(part):
        return (
            (p0[part, 0].astype(f32) + p1[part, 0].astype(f32)) + (p2[part, 0].astype(f32) + p3[part, 0].astype(f32))
        ).astype(bf16)

    gate_ref[...] = summed(0)
    up_ref[...] = summed(1)
    down = summed(2)
    size = down_ref.shape[0]
    for k in range(down.shape[0] // size):
        down_ref[:, pl.ds(k * size, size)] = down[k * size : (k + 1) * size]


def norm_kernel(core_ref, parts_ref, gain_ref, act_ref, slope_ref, cross_ref, stats_ref):
    ny, nx, height, _ = parts_ref.shape
    part = height * 2 // 3
    blocks = []
    for a, b in pieces_of(core_ref, ny, nx):
        block = parts_ref[a, b].astype(f32)
        blocks.append(unpacked(block[:part], block[part:]))
    values = jnp.concatenate(blocks, axis=0)
    channels = values.shape[0]
    mean = jnp.sum(values, axis=0, keepdims=True) / channels
    centred = values - mean
    inv = lax.rsqrt(jnp.sum(centred * centred, axis=0, keepdims=True) / channels + norm_eps)
    gain = gain_ref[...]
    normed = centred * inv
    scaled = normed * gain
    sig = jax.nn.sigmoid(scaled)
    act_ref[...] = (scaled * sig).astype(bf16)
    slope = sig * (1.0 + scaled * (1.0 - sig)) * gain
    slope_ref[...] = slope.astype(bf16)
    cross_ref[...] = (slope * normed).astype(bf16)
    stats_ref[0:1, :] = mean
    stats_ref[1:2, :] = inv


def line_sum_kernel(parts_ref, out_ref):
    acc = parts_ref[0].astype(f32)
    for j in range(1, parts_ref.shape[0]):
        acc = acc + parts_ref[j].astype(f32)
    out_ref[...] = acc.astype(bf16)


def spread_kernel(rows_ref, out_ref, *, capacity, pitch):
    count, rows_in, _ = rows_ref.shape
    rows_out = rows_in // capacity * pitch
    into, outof = iota((rows_out, rows_in), 0), iota((rows_out, rows_in), 1)
    spread = one_if((outof == (into // pitch) * capacity + into % pitch) & (into % pitch < capacity))
    for q in range(count):
        moved = jnp.dot(spread, rows_ref[q], preferred_element_type=f32)
        out_ref[pl.ds(q * rows_out, rows_out), :] = moved.astype(bf16)


def mix_kernel(core_ref, *refs):
    sources, outs, local, sems = refs[:7], refs[7:10], refs[10:17], refs[17]
    kept_ref, given_ref, blocks_ref = outs
    back_ref, returned_ref, own_ref, proj_ref, slope_ref, cross_ref, act_ref = local
    core = core_ref[0]
    copies = [
        pltpu.make_async_copy(source, target, sems.at[i])
        for i, (source, target) in enumerate(zip(sources, local, strict=True))
    ]
    for copy in copies:
        copy.start()
    for copy in copies[:3]:
        copy.wait()
    moe = contract(back_ref[...], returned_ref[...], 0, 0)
    mix = (own_ref[...].astype(f32) + moe).astype(bf16)
    for copy in copies[3:]:
        copy.wait()
    d_act = contract(proj_ref[...], mix, 1, 1)
    lanes = 128

    def as_rows(line):
        rest = line[:, lanes:]
        return [line[:, :lanes], jnp.concatenate([rest, jnp.zeros_like(rest)], axis=1)]

    tail = []
    for ref in (slope_ref, cross_ref):
        line = jnp.sum(ref[...].astype(f32) * d_act, axis=0, keepdims=True)
        high = line.astype(bf16).astype(f32)
        tail += as_rows(high) + as_rows(line - high)
    tail = jnp.concatenate(tail, axis=0).astype(bf16)
    count = blocks_ref.shape[0]
    part = d_act.shape[0] // count
    for j in range(count):
        wide, rest = packed(d_act[j * part : (j + 1) * part])
        blocks_ref[j, pl.ds(0, part), :] = wide.astype(bf16)
        blocks_ref[j, pl.ds(part, part // 2), :] = rest.astype(bf16)
        blocks_ref[j, pl.ds(part * 3 // 2, 8), :] = tail
    grad = jnp.dot(act_ref[...], mix, preferred_element_type=f32)
    size = kept_ref.shape[1]
    for k in range(kept_ref.shape[0]):
        even = grad[2 * k * size : (2 * k + 1) * size]
        odd = grad[(2 * k + 1) * size : (2 * k + 2) * size]
        kept_ref[k] = jnp.where(core == 0, even, odd).astype(bf16)
        given_ref[k] = jnp.where(core == 0, odd, even).astype(bf16)


def conv_grad_kernel(blocks_ref, norm_ref, gain_ref, stats_ref, out_ref, head_ref, *, channels):
    count, height, _ = blocks_ref.shape
    acc = blocks_ref[0].astype(f32)
    for j in range(1, count):
        acc = acc + blocks_ref[j].astype(f32)
    part = out_ref.shape[0]
    grad_act = unpacked(acc[:part], acc[part : part * 3 // 2])
    tail = acc[part * 3 // 2 :]

    def line(at):
        rest = tail[at + 1 : at + 2] + tail[at + 3 : at + 4]
        return jnp.concatenate([tail[at : at + 1] + tail[at + 2 : at + 3], rest[:, : rest.shape[1] // 2]], axis=1)

    mean, inv = stats_ref[0:1, :], stats_ref[1:2, :]
    gain = gain_ref[...]
    normed = (norm_ref[...].astype(f32) - mean) * inv
    grad_normed = grad_act * silu_grad(normed * gain) * gain
    out = inv * (grad_normed - line(0) / channels - normed * (line(4) / channels))
    out_ref[...] = out
    head_ref[...] = out[:, : head_ref.shape[1]]


def body(
    moe_input,
    out_grad,
    route_ids,
    route_weights,
    expert_gate,
    expert_up,
    expert_down,
    proj_weight,
    glu_value,
    glu_gate,
    conv_taps,
    norm_input,
    norm_gain,
):
    groups = lax.axis_size(SP)
    ny, nx = lax.axis_size("ty"), lax.axis_size("tx")
    lane_count = ny * nx
    lane_index = lax.axis_index(TP)
    tok_rows, model_width = moe_input.shape
    top_count = route_ids.shape[1]
    capacity = tok_rows * top_count * 3 // (2 * groups)
    total = groups * capacity
    width = model_width // lane_count
    pitch = 40
    back_pitch = 24
    channel_part = norm_input.shape[0]
    channels = channel_part * lane_count
    struct = jax.ShapeDtypeStruct

    sent, back_place, own_grad = pl.pallas_call(
        lambda *refs: prep_kernel(*refs, experts=groups),
        in_specs=[scalar()] + [pl.BlockSpec(memory_space=pltpu.HBM)] * 4,
        out_specs=[whole()] * 3,
        out_shape=[
            struct((groups * pitch, width), bf16),
            struct((groups * back_pitch, tok_rows), bf16),
            struct((tok_rows, width), bf16),
        ],
        scratch_shapes=[
            pltpu.VMEM((top_count, tok_rows), i32),
            pltpu.VMEM((top_count, tok_rows), f32),
            pltpu.VMEM((tok_rows, width), bf16),
            pltpu.SemaphoreType.DMA((4,)),
        ],
        compiler_params=params(58),
        name="prep",
    )(lane_index.astype(i32).reshape(1), route_ids.T, route_weights.T, moe_input, out_grad)

    part = exchanged(sent.reshape(groups, pitch, width), SP)

    core = lax.axis_index("core").astype(i32).reshape(1)
    first_groups, second_groups = line_groups(ny, nx)
    w_gate, w_up, w_down = expert_gate[0], expert_up[0], expert_down[0]
    ff = w_gate.shape[1]
    hbm = pl.BlockSpec(memory_space=pltpu.HBM)
    w_gate, w_up, w_down, _ = lax.optimization_barrier((w_gate, w_up, w_down, sent))
    own_weights = pl.pallas_call(
        pack_kernel,
        out_shape=struct((3 * model_width, ff), bf16),
        in_specs=[whole()] * 3,
        out_specs=whole(),
        compiler_params=params(58),
        cost_estimate=cost(8 * total * model_width * ff, 6 * model_width * ff),
        name="pack",
    )(w_gate, w_up, w_down)
    onward, backward, across = [line_pairs(ny, nx, by) for by in (1, -1, 2)]
    with jax.named_scope("weights_out"):
        weights = (
            own_weights,
            lax.ppermute(own_weights, PLANE, onward),
            lax.ppermute(own_weights, PLANE, backward),
            lax.ppermute(own_weights, PLANE, across),
        )

    quarter = total // nx
    norm_rows = channel_part * 3 // 2
    rows_height = 2 * quarter + norm_rows
    quarters = pl.pallas_call(
        lambda *refs: compact_kernel(*refs, capacity=capacity, pitch=pitch),
        out_shape=struct((nx, rows_height, width), bf16),
        in_specs=[whole(), whole()],
        out_specs=whole(),
        compiler_params=params(16),
        name="compact",
    )(part.reshape(groups * pitch, width), norm_input)
    quarters = exchanged(quarters, PLANE, first_groups)
    gathered = exchanged(jnp.broadcast_to(quarters[None], (ny, *quarters.shape)), PLANE, second_groups)

    packed_weights = pltpu.VMEM((3 * model_width, ff), bf16)
    back, hidden, both = pl.pallas_call(
        expert_kernel,
        in_specs=[scalar()] + [hbm] * 5,
        out_specs=[whole()] * 3,
        out_shape=[
            struct((ny, nx, quarter, width), bf16),
            struct((quarter, nx * ff), bf16),
            struct((quarter, 2 * nx * ff), bf16),
        ],
        scratch_shapes=[
            pltpu.VMEM((ny, nx, rows_height, width), bf16),
            packed_weights,
            packed_weights,
            packed_weights,
            packed_weights,
            pltpu.VMEM((quarter, model_width), f32),
            pltpu.SemaphoreType.DMA((5,)),
        ],
        compiler_params=params(58),
        cost_estimate=cost(10 * total * model_width * ff, 10 * total * model_width),
        name="expert",
    )(core, gathered, *weights)

    with jax.named_scope("line_sum"):
        line_parts = exchanged(back, PLANE, second_groups)
    wgrads = pl.pallas_call(
        weight_kernel,
        in_specs=[scalar()] + [whole()] * 3,
        out_specs=[whole()] * nx,
        out_shape=[struct((3 * model_width, ff), bf16)] * nx,
        compiler_params=params(58),
        cost_estimate=cost(6 * total * model_width * ff, 10 * total * model_width),
        name="weights",
    )(core, gathered, hidden, both)
    line_parts, *wgrads = lax.optimization_barrier((line_parts, *wgrads))
    line_rows = pl.pallas_call(
        line_sum_kernel,
        out_shape=struct((nx, quarter, width), bf16),
        in_specs=[whole()],
        out_specs=whole(),
        compiler_params=params(16),
        name="line_sum",
    )(line_parts)
    own_rows = exchanged(line_rows, PLANE, first_groups)
    summed_grad = pl.pallas_call(
        lambda *refs: spread_kernel(*refs, capacity=capacity, pitch=back_pitch),
        out_shape=struct((groups * back_pitch, width), bf16),
        in_specs=[whole()],
        out_specs=whole(),
        compiler_params=params(16),
        name="spread",
    )(own_rows)
    with jax.named_scope("rows_back"):
        returned = exchanged(summed_grad.reshape(groups, back_pitch, width), SP)

    sent_wgrads = lax.optimization_barrier((summed_grad, *wgrads[1:]))[1:]
    with jax.named_scope("weights_back"):
        from_across = lax.ppermute(sent_wgrads[2], PLANE, across)
        line_wgrads = (
            wgrads[0],
            lax.ppermute(sent_wgrads[0], PLANE, backward),
            lax.ppermute(sent_wgrads[1], PLANE, onward),
            from_across,
        )

    act, slope, cross, stats = pl.pallas_call(
        norm_kernel,
        grid_spec=pltpu.PrefetchScalarGridSpec(
            num_scalar_prefetch=1,
            grid=(1,),
            in_specs=[
                pl.BlockSpec((ny, nx, norm_rows, width), lambda i, m: (0, 0, 2 * quarter // norm_rows, 0)),
                pl.BlockSpec((channels, 1), lambda i, m: (0, 0)),
            ],
            out_specs=[pl.BlockSpec((channels, tok_rows), lambda i, m: (0, 0))] * 3
            + [pl.BlockSpec((2, tok_rows), lambda i, m: (0, 0))],
        ),
        out_shape=[struct((channels, tok_rows), bf16)] * 3 + [struct((2, tok_rows), f32)],
        compiler_params=params(58),
        cost_estimate=cost(6 * total * model_width * ff, 10 * total * model_width),
        name="norm",
    )(core, gathered, norm_gain[:, None])

    proj_size = channels // groups
    block_rows = norm_rows + 8
    mix_inputs = (
        back_place,
        returned.reshape(groups * back_pitch, width),
        own_grad,
        proj_weight,
        slope,
        cross,
        act,
    )
    kept, given, blocks = pl.pallas_call(
        mix_kernel,
        out_shape=[
            struct((groups // 2, proj_size, width), bf16),
            struct((groups // 2, proj_size, width), bf16),
            struct((lane_count, block_rows, width), bf16),
        ],
        in_specs=[scalar()] + [pl.BlockSpec(memory_space=pltpu.HBM)] * len(mix_inputs),
        out_specs=[whole()] * 3,
        scratch_shapes=[pltpu.VMEM(value.shape, value.dtype) for value in mix_inputs]
        + [pltpu.SemaphoreType.DMA((len(mix_inputs),))],
        compiler_params=params(58),
        name="mix",
    )(core, *mix_inputs)
    arrived = exchanged(blocks, TP)
    from_pair = lax.ppermute(given, "core", [(0, 1), (1, 0)])
    chip_sum = (kept.astype(f32) + from_pair.astype(f32)).astype(bf16)
    chip_sum, arrived = lax.optimization_barrier((chip_sum, arrived))
    grad_proj = jnp.sum(exchanged(chip_sum, "z").astype(f32), axis=0)

    taps_count = conv_taps.shape[1]
    reach_back = taps_count - 1
    gain_own = lax.dynamic_slice_in_dim(norm_gain, lane_index * channel_part, channel_part, 0)
    grad_conv, head = pl.pallas_call(
        lambda *refs: conv_grad_kernel(*refs, channels=channels),
        out_shape=[struct((channel_part, tok_rows), f32), struct((channel_part, reach_back), f32)],
        in_specs=[whole()] * 4,
        out_specs=[whole()] * 2,
        compiler_params=params(16),
        name="conv_grad",
    )(arrived, norm_input, gain_own[:, None], stats)

    pairs = [(i, i - 1) for i in range(1, groups)]
    ahead_rows = lax.ppermute(head, SP, pairs)
    extended = jnp.concatenate([grad_conv, ahead_rows], axis=1)
    grad_glu = jnp.zeros_like(grad_conv)
    for tap_index in range(taps_count):
        grad_glu = (
            grad_glu
            + conv_taps[:, tap_index : tap_index + 1]
            * extended[:, reach_back - tap_index : reach_back - tap_index + tok_rows]
        )
    sigmoid_gate = jax.nn.sigmoid(glu_gate.astype(f32))
    grad_value = (grad_glu * sigmoid_gate).astype(bf16)
    grad_glu_gate = (
        grad_glu * glu_value.astype(f32) * sigmoid_gate * (1.0 - sigmoid_gate)
    ).astype(bf16)
    sum_rows = 256
    sum_steps = model_width // sum_rows
    parts = [value.reshape(3, sum_steps, sum_rows, ff) for value in line_wgrads]
    gate_wgrad, up_wgrad, down_grad = pl.pallas_call(
        weight_sum_kernel,
        grid=(sum_steps,),
        in_specs=[pl.BlockSpec((3, 1, sum_rows, ff), lambda i: (0, i, 0, 0))] * 4,
        out_specs=[
            pl.BlockSpec((sum_rows, ff), lambda i: (i, 0)),
            pl.BlockSpec((sum_rows, ff), lambda i: (i, 0)),
            pl.BlockSpec((ff, sum_rows), lambda i: (0, i)),
        ],
        out_shape=[
            struct((model_width, ff), bf16),
            struct((model_width, ff), bf16),
            struct((ff, model_width), bf16),
        ],
        compiler_params=params(58),
        cost_estimate=cost(6 * total * model_width * ff, 10 * total * model_width),
        name="weight_sum",
    )(*parts)
    return (gate_wgrad[None], up_wgrad[None], down_grad[None], grad_proj, grad_value, grad_glu_gate)


def solution(mesh):
    finer = Mesh(mesh.devices.reshape(mesh.shape["sp"] // 2, 2, 4, 4), ("z", "core", "ty", "tx"))
    return jax.shard_map(
        body,
        mesh=finer,
        in_specs=(
            P(SP, None),
            P(SP, None),
            P(SP, None),
            P(SP, None),
            P(SP, None, TP),
            P(SP, None, TP),
            P(SP, TP, None),
            P(None, TP),
            P(TP, SP),
            P(TP, SP),
            P(TP, None),
            P(TP, SP),
            P(),
        ),
        out_specs=(
            P(SP, None, TP),
            P(SP, None, TP),
            P(SP, TP, None),
            P(SP, TP),
            P(TP, SP),
            P(TP, SP),
        ),
        check_vma=False,
    )
```

```python
import jax
import jax.numpy as jnp
from jax import lax
from jax.experimental import pallas as pl
from jax.experimental.pallas import tpu as pltpu
from jax.sharding import Mesh
from jax.sharding import PartitionSpec as P

TP = ("ty", "tx")
SP = ("z", "core")
PLANE = ("core", "ty", "tx")


norm_eps = 1e-05

bf16, f32, i32 = jnp.bfloat16, jnp.float32, jnp.int32


def exchanged(blocks, axis, index_groups=None):
    return lax.all_to_all(blocks, axis, 0, 0, axis_index_groups=index_groups, tiled=True)


def line_groups(ny, nx):
    along_x = [[y * nx + x for x in range(nx)] for y in range(ny)]
    along_y = [[y * nx + x for y in range(ny)] for x in range(nx)]

    def of_core_one(lines):
        return [[ny * nx + i for i in line] for line in lines]

    return along_x + of_core_one(along_y), along_y + of_core_one(along_x)


def line_pairs(ny, nx, by):
    pairs = []
    for y in range(ny):
        for x in range(nx):
            pairs.append((y * nx + x, y * nx + (x + by) % nx))
            pairs.append((ny * nx + y * nx + x, ny * nx + (y + by) % ny * nx + x))
    return pairs


def silu_grad(pre):
    sig = jax.nn.sigmoid(pre)
    return sig * (1.0 + pre * (1.0 - sig))


def contract(a, b, dim_a, dim_b):
    return lax.dot_general(a, b, (((dim_a,), (dim_b,)), ((), ())), preferred_element_type=f32)


def iota(shape, dim):
    return lax.broadcasted_iota(i32, shape, dim)


def whole():
    return pl.BlockSpec(memory_space=pltpu.VMEM)


def scalar():
    return pl.BlockSpec(memory_space=pltpu.SMEM)


def params(mib):
    return pltpu.CompilerParams(vmem_limit_bytes=mib * 1024 * 1024)


def cost(flops, size):
    return pl.CostEstimate(flops=flops, bytes_accessed=size, transcendentals=0)


def one_if(condition):
    return jnp.where(condition, 1.0, 0.0).astype(bf16)


def prep_kernel(lane_ref, ids_hbm, scale_hbm, input_hbm, grad_hbm, *refs, experts):
    sent_ref, back_ref, own_ref, ids_ref, scale_ref, input_ref, sems = refs
    tok, width = input_ref.shape
    columns = pl.ds(pl.multiple_of(lane_ref[0] * width, width), width)
    copies = [
        pltpu.make_async_copy(ids_hbm, ids_ref, sems.at[0]),
        pltpu.make_async_copy(scale_hbm, scale_ref, sems.at[1]),
        pltpu.make_async_copy(input_hbm.at[:, columns], input_ref, sems.at[2]),
        pltpu.make_async_copy(grad_hbm.at[:, columns], own_ref, sems.at[3]),
    ]
    for copy in copies:
        copy.start()
    for copy in copies:
        copy.wait()
    e0, e1 = ids_ref[0:1, :], ids_ref[1:2, :]
    s0, s1 = scale_ref[0:1, :], scale_ref[1:2, :]
    rows = iota((experts, tok), 0)
    hit0, hit1 = rows == e0, rows == e1
    earlier = one_if(iota((tok, tok), 0) < iota((tok, tok), 1))
    before = jnp.dot(one_if(hit0 | hit1), earlier, preferred_element_type=f32)
    slot0 = jnp.sum(jnp.where(hit0, before, 0.0), axis=0, keepdims=True).astype(i32)
    slot1 = jnp.sum(jnp.where(hit1, before, 0.0), axis=0, keepdims=True).astype(i32)
    x = input_ref[...]
    grad = own_ref[...]
    diagonal = iota((tok, tok), 0) == iota((tok, tok), 1)
    c0 = jnp.sum(jnp.where(diagonal, s0, 0.0), axis=1, keepdims=True)
    c1 = jnp.sum(jnp.where(diagonal, s1, 0.0), axis=1, keepdims=True)
    g = grad.astype(f32)
    g0, g1 = (g * c0).astype(bf16), (g * c1).astype(bf16)
    pitch = sent_ref.shape[0] // experts
    r = iota((sent_ref.shape[0], tok), 0)
    a0, a1 = e0 * pitch + slot0, e1 * pitch + slot1
    half = pitch // 2
    sent = jnp.dot(one_if((r == a0) | (r == a1)), x, preferred_element_type=f32)
    sent = sent + jnp.dot(one_if(r == a0 + half), g0, preferred_element_type=f32)
    sent = sent + jnp.dot(one_if(r == a1 + half), g1, preferred_element_type=f32)
    sent_ref[...] = sent.astype(bf16)
    back_pitch = back_ref.shape[0] // experts
    r = iota((back_ref.shape[0], tok), 0)
    back_ref[...] = one_if((r == e0 * back_pitch + slot0) | (r == e1 * back_pitch + slot1))


def packed(block):
    lanes = 128
    wide = block[:, :lanes]
    rest = block[:, lanes:]
    rows = rest.shape[0] // 2
    return wide, jnp.concatenate([rest[:rows], rest[rows:]], axis=1)


def unpacked(wide, rest):
    lanes = rest.shape[1] // 2
    tail = jnp.concatenate([rest[:, :lanes], rest[:, lanes:]], axis=0)
    return jnp.concatenate([wide, tail], axis=1)


def compact_kernel(part_ref, norm_ref, out_ref, *, capacity, pitch):
    count = out_ref.shape[0]
    rows_in = part_ref.shape[0] // count
    rows_out = rows_in // pitch * capacity
    into, outof = iota((rows_out, rows_in), 0), iota((rows_out, rows_in), 1)
    pick_x = one_if(outof == (into // capacity) * pitch + into % capacity)
    pick_g = one_if(outof == (into // capacity) * pitch + into % capacity + pitch // 2)
    wide, rest = packed(norm_ref[...].astype(f32))
    wide, rest = wide.astype(bf16), rest.astype(bf16)
    for q in range(count):
        piece = part_ref[pl.ds(q * rows_in, rows_in), :]
        out_ref[q, pl.ds(0, rows_out), :] = jnp.dot(pick_x, piece, preferred_element_type=f32).astype(bf16)
        out_ref[q, pl.ds(rows_out, rows_out), :] = jnp.dot(pick_g, piece, preferred_element_type=f32).astype(bf16)
        out_ref[q, pl.ds(2 * rows_out, wide.shape[0]), :] = wide
        out_ref[q, pl.ds(2 * rows_out + wide.shape[0], rest.shape[0]), :] = rest


def pieces_of(core_ref, ny, nx):
    core = core_ref[0]
    return [
        (jnp.where(core == 0, y, x), jnp.where(core == 0, x, y)) for y in range(ny) for x in range(nx)
    ]


def pack_kernel(gate_ref, up_ref, down_ref, out_ref):
    height, width = gate_ref.shape
    out_ref[pl.ds(0, height), :] = gate_ref[...]
    out_ref[pl.ds(height, height), :] = up_ref[...]
    for k in range(height // width):
        out_ref[pl.ds(2 * height + k * width, width), :] = down_ref[:, pl.ds(k * width, width)]


def expert_kernel(core_ref, rows_hbm, *refs):
    weights_hbm = refs[0:5]
    back_ref, hidden_ref, both_ref, rows_ref = refs[5:9]
    weights, acc_ref, sems = refs[9:13], refs[13], refs[14]
    middle = weights_hbm[3].shape[0]
    targets = (rows_ref, *weights[:3], weights[3].at[pl.ds(0, middle)], weights[3].at[pl.ds(middle, middle)])
    copies = [
        pltpu.make_async_copy(source, target, sems.at[i])
        for i, (source, target) in enumerate(zip((rows_hbm, *weights_hbm), targets, strict=True))
    ]
    for copy in copies:
        copy.start()
    ny, nx, _, width = rows_ref.shape
    count = hidden_ref.shape[0]
    pieces = pieces_of(core_ref, ny, nx)
    height = ny * nx * width
    copies[0].wait()
    x = jnp.concatenate([rows_ref[a, b, pl.ds(0, count), :] for a, b in pieces], axis=1)
    g = jnp.concatenate([rows_ref[a, b, pl.ds(count, count), :] for a, b in pieces], axis=1)
    for k, block in enumerate(weights):
        copies[1 + k].wait()
        if k == 3:
            copies[5].wait()
        w_both = jnp.concatenate([block[pl.ds(0, height), :], block[pl.ds(height, height), :]], axis=1)
        w_down = jnp.concatenate(
            [block[pl.ds(2 * height + i * width, width), :] for i in range(ny * nx)], axis=1
        )
        pre = jnp.dot(x, w_both, preferred_element_type=f32)
        gate_pre, up_pre = pre[:, :width], pre[:, width:]
        d_hidden = contract(g, w_down, 1, 1)
        sig = jax.nn.sigmoid(gate_pre)
        gate_act = gate_pre * sig
        hidden_ref[:, pl.ds(k * width, width)] = (gate_act * up_pre).astype(bf16)
        d_gate = d_hidden * up_pre * (sig * (1.0 + gate_pre * (1.0 - sig)))
        d_up = d_hidden * gate_act
        both = jnp.concatenate([d_gate.astype(bf16), d_up.astype(bf16)], axis=1)
        both_ref[:, pl.ds(2 * k * width, 2 * width)] = both
        back = contract(both, w_both, 1, 1)
        acc_ref[...] = back if k == 0 else acc_ref[...] + back
    for j, (a, b) in enumerate(pieces):
        back_ref[a, b] = acc_ref[:, pl.ds(j * width, width)].astype(bf16)


def weight_kernel(core_ref, rows_ref, hidden_ref, both_ref, *outs):
    ny, nx, _, width = rows_ref.shape
    count = hidden_ref.shape[0]
    height = ny * nx * width
    for j, (a, b) in enumerate(pieces_of(core_ref, ny, nx)):
        pairs = contract(rows_ref[a, b, pl.ds(0, count), :], both_ref[...], 0, 0).astype(bf16)
        downs = contract(hidden_ref[...], rows_ref[a, b, pl.ds(count, count), :], 0, 0).astype(bf16)
        for k, out_ref in enumerate(outs):
            out_ref[pl.ds(j * width, width), :] = pairs[:, 2 * k * width : (2 * k + 1) * width]
            out_ref[pl.ds(height + j * width, width), :] = pairs[:, (2 * k + 1) * width : (2 * k + 2) * width]
            out_ref[pl.ds(2 * height + j * width, width), :] = downs[k * width : (k + 1) * width]


def weight_sum_kernel(p0, p1, p2, p3, gate_ref, up_ref, down_ref):
    def summed(part):
        return (
            (p0[part, 0].astype(f32) + p1[part, 0].astype(f32)) + (p2[part, 0].astype(f32) + p3[part, 0].astype(f32))
        ).astype(bf16)

    gate_ref[...] = summed(0)
    up_ref[...] = summed(1)
    down = summed(2)
    size = down_ref.shape[0]
    for k in range(down.shape[0] // size):
        down_ref[:, pl.ds(k * size, size)] = down[k * size : (k + 1) * size]


def norm_kernel(core_ref, parts_ref, gain_ref, act_ref, slope_ref, cross_ref, stats_ref):
    ny, nx, height, _ = parts_ref.shape
    part = height * 2 // 3
    blocks = []
    for a, b in pieces_of(core_ref, ny, nx):
        block = parts_ref[a, b].astype(f32)
        blocks.append(unpacked(block[:part], block[part:]))
    values = jnp.concatenate(blocks, axis=0)
    channels = values.shape[0]
    mean = jnp.sum(values, axis=0, keepdims=True) / channels
    centred = values - mean
    inv = lax.rsqrt(jnp.sum(centred * centred, axis=0, keepdims=True) / channels + norm_eps)
    gain = gain_ref[...]
    normed = centred * inv
    scaled = normed * gain
    sig = jax.nn.sigmoid(scaled)
    act_ref[...] = (scaled * sig).astype(bf16)
    slope = sig * (1.0 + scaled * (1.0 - sig)) * gain
    slope_ref[...] = slope.astype(bf16)
    cross_ref[...] = (slope * normed).astype(bf16)
    stats_ref[0:1, :] = mean
    stats_ref[1:2, :] = inv


def line_sum_kernel(parts_ref, out_ref):
    acc = parts_ref[0].astype(f32)
    for j in range(1, parts_ref.shape[0]):
        acc = acc + parts_ref[j].astype(f32)
    out_ref[...] = acc.astype(bf16)


def spread_kernel(rows_ref, out_ref, *, capacity, pitch):
    count, rows_in, _ = rows_ref.shape
    rows_out = rows_in // capacity * pitch
    into, outof = iota((rows_out, rows_in), 0), iota((rows_out, rows_in), 1)
    spread = one_if((outof == (into // pitch) * capacity + into % pitch) & (into % pitch < capacity))
    for q in range(count):
        moved = jnp.dot(spread, rows_ref[q], preferred_element_type=f32)
        out_ref[pl.ds(q * rows_out, rows_out), :] = moved.astype(bf16)


def mix_kernel(core_ref, *refs):
    sources, outs, local, sems = refs[:7], refs[7:10], refs[10:17], refs[17]
    kept_ref, given_ref, blocks_ref = outs
    back_ref, returned_ref, own_ref, proj_ref, slope_ref, cross_ref, act_ref = local
    core = core_ref[0]
    copies = [
        pltpu.make_async_copy(source, target, sems.at[i])
        for i, (source, target) in enumerate(zip(sources, local, strict=True))
    ]
    for copy in copies:
        copy.start()
    for copy in copies[:3]:
        copy.wait()
    moe = contract(back_ref[...], returned_ref[...], 0, 0)
    mix = (own_ref[...].astype(f32) + moe).astype(bf16)
    for copy in copies[3:]:
        copy.wait()
    d_act = contract(proj_ref[...], mix, 1, 1)
    lanes = 128

    def as_rows(line):
        rest = line[:, lanes:]
        return [line[:, :lanes], jnp.concatenate([rest, jnp.zeros_like(rest)], axis=1)]

    tail = []
    for ref in (slope_ref, cross_ref):
        line = jnp.sum(ref[...].astype(f32) * d_act, axis=0, keepdims=True)
        high = line.astype(bf16).astype(f32)
        tail += as_rows(high) + as_rows(line - high)
    tail = jnp.concatenate(tail, axis=0).astype(bf16)
    count = blocks_ref.shape[0]
    part = d_act.shape[0] // count
    for j in range(count):
        wide, rest = packed(d_act[j * part : (j + 1) * part])
        blocks_ref[j, pl.ds(0, part), :] = wide.astype(bf16)
        blocks_ref[j, pl.ds(part, part // 2), :] = rest.astype(bf16)
        blocks_ref[j, pl.ds(part * 3 // 2, 8), :] = tail
    grad = jnp.dot(act_ref[...], mix, preferred_element_type=f32)
    size = kept_ref.shape[1]
    for k in range(kept_ref.shape[0]):
        even = grad[2 * k * size : (2 * k + 1) * size]
        odd = grad[(2 * k + 1) * size : (2 * k + 2) * size]
        kept_ref[k] = jnp.where(core == 0, even, odd).astype(bf16)
        given_ref[k] = jnp.where(core == 0, odd, even).astype(bf16)


def conv_grad_kernel(blocks_ref, norm_ref, gain_ref, stats_ref, out_ref, head_ref, *, channels):
    count, _, _ = blocks_ref.shape
    acc = blocks_ref[0].astype(f32)
    for j in range(1, count):
        acc = acc + blocks_ref[j].astype(f32)
    part = out_ref.shape[0]
    grad_act = unpacked(acc[:part], acc[part : part * 3 // 2])
    tail = acc[part * 3 // 2 :]

    def line(at):
        rest = tail[at + 1 : at + 2] + tail[at + 3 : at + 4]
        return jnp.concatenate([tail[at : at + 1] + tail[at + 2 : at + 3], rest[:, : rest.shape[1] // 2]], axis=1)

    mean, inv = stats_ref[0:1, :], stats_ref[1:2, :]
    gain = gain_ref[...]
    normed = (norm_ref[...].astype(f32) - mean) * inv
    grad_normed = grad_act * silu_grad(normed * gain) * gain
    out = inv * (grad_normed - line(0) / channels - normed * (line(4) / channels))
    out_ref[...] = out
    head_ref[...] = out[:, : head_ref.shape[1]]


def body(
    moe_input,
    out_grad,
    route_ids,
    route_weights,
    expert_gate,
    expert_up,
    expert_down,
    proj_weight,
    glu_value,
    glu_gate,
    conv_taps,
    norm_input,
    norm_gain,
):
    groups = lax.axis_size(SP)
    ny, nx = lax.axis_size("ty"), lax.axis_size("tx")
    lane_count = ny * nx
    lane_index = lax.axis_index(TP)
    tok_rows, model_width = moe_input.shape
    top_count = route_ids.shape[1]
    capacity = tok_rows * top_count * 3 // (2 * groups)
    total = groups * capacity
    width = model_width // lane_count
    pitch = 40
    back_pitch = 24
    channel_part = norm_input.shape[0]
    channels = channel_part * lane_count
    struct = jax.ShapeDtypeStruct

    sent, back_place, own_grad = pl.pallas_call(
        lambda *refs: prep_kernel(*refs, experts=groups),
        in_specs=[scalar()] + [pl.BlockSpec(memory_space=pltpu.HBM)] * 4,
        out_specs=[whole()] * 3,
        out_shape=[
            struct((groups * pitch, width), bf16),
            struct((groups * back_pitch, tok_rows), bf16),
            struct((tok_rows, width), bf16),
        ],
        scratch_shapes=[
            pltpu.VMEM((top_count, tok_rows), i32),
            pltpu.VMEM((top_count, tok_rows), f32),
            pltpu.VMEM((tok_rows, width), bf16),
            pltpu.SemaphoreType.DMA((4,)),
        ],
        compiler_params=params(58),
        name="prep",
    )(lane_index.astype(i32).reshape(1), route_ids.T, route_weights.T, moe_input, out_grad)

    part = exchanged(sent.reshape(groups, pitch, width), SP)

    core = lax.axis_index("core").astype(i32).reshape(1)
    first_groups, second_groups = line_groups(ny, nx)
    w_gate, w_up, w_down = expert_gate[0], expert_up[0], expert_down[0]
    ff = w_gate.shape[1]
    hbm = pl.BlockSpec(memory_space=pltpu.HBM)
    w_gate, w_up, w_down, _ = lax.optimization_barrier((w_gate, w_up, w_down, sent))
    own_weights = pl.pallas_call(
        pack_kernel,
        out_shape=struct((3 * model_width, ff), bf16),
        in_specs=[whole()] * 3,
        out_specs=whole(),
        compiler_params=params(58),
        cost_estimate=cost(8 * total * model_width * ff, 6 * model_width * ff),
        name="pack",
    )(w_gate, w_up, w_down)
    onward, backward, across = [line_pairs(ny, nx, by) for by in (1, -1, 2)]
    weights = (
        own_weights,
        lax.ppermute(own_weights, PLANE, onward),
        lax.ppermute(own_weights, PLANE, backward),
    )

    quarter = total // nx
    norm_rows = channel_part * 3 // 2
    rows_height = 2 * quarter + norm_rows
    quarters = pl.pallas_call(
        lambda *refs: compact_kernel(*refs, capacity=capacity, pitch=pitch),
        out_shape=struct((nx, rows_height, width), bf16),
        in_specs=[whole(), whole()],
        out_specs=whole(),
        compiler_params=params(16),
        name="compact",
    )(part.reshape(groups * pitch, width), norm_input)
    quarters, *weights = lax.optimization_barrier((exchanged(quarters, PLANE, first_groups), *weights))
    middle = weights[0].shape[0] // 2
    weights += [lax.ppermute(weights[1][:middle], PLANE, onward), lax.ppermute(weights[2][middle:], PLANE, backward)]
    gathered = exchanged(jnp.broadcast_to(quarters[None], (ny, *quarters.shape)), PLANE, second_groups)

    packed_weights = pltpu.VMEM((3 * model_width, ff), bf16)
    back, hidden, both = pl.pallas_call(
        expert_kernel,
        in_specs=[scalar()] + [hbm] * 6,
        out_specs=[whole()] * 3,
        out_shape=[
            struct((ny, nx, quarter, width), bf16),
            struct((quarter, nx * ff), bf16),
            struct((quarter, 2 * nx * ff), bf16),
        ],
        scratch_shapes=[
            pltpu.VMEM((ny, nx, rows_height, width), bf16),
            packed_weights,
            packed_weights,
            packed_weights,
            packed_weights,
            pltpu.VMEM((quarter, model_width), f32),
            pltpu.SemaphoreType.DMA((6,)),
        ],
        compiler_params=params(58),
        cost_estimate=cost(10 * total * model_width * ff, 10 * total * model_width),
        name="expert",
    )(core, gathered, *weights)

    line_parts = exchanged(back, PLANE, second_groups)
    wgrads = pl.pallas_call(
        weight_kernel,
        in_specs=[scalar()] + [whole()] * 3,
        out_specs=[whole()] * nx,
        out_shape=[struct((3 * model_width, ff), bf16)] * nx,
        compiler_params=params(58),
        cost_estimate=cost(6 * total * model_width * ff, 10 * total * model_width),
        name="weights",
    )(core, gathered, hidden, both)
    line_parts, *wgrads = lax.optimization_barrier((line_parts, *wgrads))
    line_rows = pl.pallas_call(
        line_sum_kernel,
        out_shape=struct((nx, quarter, width), bf16),
        in_specs=[whole()],
        out_specs=whole(),
        compiler_params=params(16),
        name="line_sum",
    )(line_parts)
    own_rows = exchanged(line_rows, PLANE, first_groups)
    summed_grad = pl.pallas_call(
        lambda *refs: spread_kernel(*refs, capacity=capacity, pitch=back_pitch),
        out_shape=struct((groups * back_pitch, width), bf16),
        in_specs=[whole()],
        out_specs=whole(),
        compiler_params=params(16),
        name="spread",
    )(own_rows)
    returned = exchanged(summed_grad.reshape(groups, back_pitch, width), SP)

    sent_wgrads = lax.optimization_barrier((summed_grad, *wgrads[1:]))[1:]
    from_across = lax.ppermute(sent_wgrads[2], PLANE, across)
    line_wgrads = (
        wgrads[0],
        lax.ppermute(sent_wgrads[0], PLANE, backward),
        lax.ppermute(sent_wgrads[1], PLANE, onward),
        from_across,
    )

    act, slope, cross, stats = pl.pallas_call(
        norm_kernel,
        grid_spec=pltpu.PrefetchScalarGridSpec(
            num_scalar_prefetch=1,
            grid=(1,),
            in_specs=[
                pl.BlockSpec((ny, nx, norm_rows, width), lambda i, m: (0, 0, 2 * quarter // norm_rows, 0)),
                pl.BlockSpec((channels, 1), lambda i, m: (0, 0)),
            ],
            out_specs=[pl.BlockSpec((channels, tok_rows), lambda i, m: (0, 0))] * 3
            + [pl.BlockSpec((2, tok_rows), lambda i, m: (0, 0))],
        ),
        out_shape=[struct((channels, tok_rows), bf16)] * 3 + [struct((2, tok_rows), f32)],
        compiler_params=params(58),
        cost_estimate=cost(6 * total * model_width * ff, 10 * total * model_width),
        name="norm",
    )(core, gathered, norm_gain[:, None])

    proj_size = channels // groups
    block_rows = norm_rows + 8
    mix_inputs = (
        back_place,
        returned.reshape(groups * back_pitch, width),
        own_grad,
        proj_weight,
        slope,
        cross,
        act,
    )
    kept, given, blocks = pl.pallas_call(
        mix_kernel,
        out_shape=[
            struct((groups // 2, proj_size, width), bf16),
            struct((groups // 2, proj_size, width), bf16),
            struct((lane_count, block_rows, width), bf16),
        ],
        in_specs=[scalar()] + [pl.BlockSpec(memory_space=pltpu.HBM)] * len(mix_inputs),
        out_specs=[whole()] * 3,
        scratch_shapes=[pltpu.VMEM(value.shape, value.dtype) for value in mix_inputs]
        + [pltpu.SemaphoreType.DMA((len(mix_inputs),))],
        compiler_params=params(58),
        name="mix",
    )(core, *mix_inputs)
    arrived = exchanged(blocks, TP)
    from_pair = lax.ppermute(given, "core", [(0, 1), (1, 0)])
    chip_sum = (kept.astype(f32) + from_pair.astype(f32)).astype(bf16)
    chip_sum, arrived = lax.optimization_barrier((chip_sum, arrived))
    grad_proj = jnp.sum(exchanged(chip_sum, "z").astype(f32), axis=0)

    taps_count = conv_taps.shape[1]
    reach_back = taps_count - 1
    gain_own = lax.dynamic_slice_in_dim(norm_gain, lane_index * channel_part, channel_part, 0)
    grad_conv, head = pl.pallas_call(
        lambda *refs: conv_grad_kernel(*refs, channels=channels),
        out_shape=[struct((channel_part, tok_rows), f32), struct((channel_part, reach_back), f32)],
        in_specs=[whole()] * 4,
        out_specs=[whole()] * 2,
        compiler_params=params(16),
        name="conv_grad",
    )(arrived, norm_input, gain_own[:, None], stats)

    pairs = [(i, i - 1) for i in range(1, groups)]
    ahead_rows = lax.ppermute(head, SP, pairs)
    extended = jnp.concatenate([grad_conv, ahead_rows], axis=1)
    grad_glu = jnp.zeros_like(grad_conv)
    for tap_index in range(taps_count):
        grad_glu = (
            grad_glu
            + conv_taps[:, tap_index : tap_index + 1]
            * extended[:, reach_back - tap_index : reach_back - tap_index + tok_rows]
        )
    sigmoid_gate = jax.nn.sigmoid(glu_gate.astype(f32))
    grad_value = (grad_glu * sigmoid_gate).astype(bf16)
    grad_glu_gate = (
        grad_glu * glu_value.astype(f32) * sigmoid_gate * (1.0 - sigmoid_gate)
    ).astype(bf16)
    sum_rows = 256
    sum_steps = model_width // sum_rows
    parts = [value.reshape(3, sum_steps, sum_rows, ff) for value in line_wgrads]
    gate_wgrad, up_wgrad, down_grad = pl.pallas_call(
        weight_sum_kernel,
        grid=(sum_steps,),
        in_specs=[pl.BlockSpec((3, 1, sum_rows, ff), lambda i: (0, i, 0, 0))] * 4,
        out_specs=[
            pl.BlockSpec((sum_rows, ff), lambda i: (i, 0)),
            pl.BlockSpec((sum_rows, ff), lambda i: (i, 0)),
            pl.BlockSpec((ff, sum_rows), lambda i: (0, i)),
        ],
        out_shape=[
            struct((model_width, ff), bf16),
            struct((model_width, ff), bf16),
            struct((ff, model_width), bf16),
        ],
        compiler_params=params(58),
        cost_estimate=cost(6 * total * model_width * ff, 10 * total * model_width),
        name="weight_sum",
    )(*parts)
    return (gate_wgrad[None], up_wgrad[None], down_grad[None], grad_proj, grad_value, grad_glu_gate)


def solution(mesh):
    finer = Mesh(mesh.devices.reshape(mesh.shape["sp"] // 2, 2, 4, 4), ("z", "core", "ty", "tx"))
    return jax.shard_map(
        body,
        mesh=finer,
        in_specs=(
            P(SP, None),
            P(SP, None),
            P(SP, None),
            P(SP, None),
            P(SP, None, TP),
            P(SP, None, TP),
            P(SP, TP, None),
            P(None, TP),
            P(TP, SP),
            P(TP, SP),
            P(TP, None),
            P(TP, SP),
            P(),
        ),
        out_specs=(
            P(SP, None, TP),
            P(SP, None, TP),
            P(SP, TP, None),
            P(SP, TP),
            P(TP, SP),
            P(TP, SP),
        ),
        check_vma=False,
    )
```

```python
import jax
import jax.numpy as jnp
from jax import lax
from jax.experimental import pallas as pl
from jax.experimental.pallas import tpu as pltpu
from jax.sharding import Mesh
from jax.sharding import PartitionSpec as P

TP = ("ty", "tx")
SP = ("z", "core")
PLANE = ("core", "ty", "tx")


norm_eps = 1e-05

bf16, f32, i32 = jnp.bfloat16, jnp.float32, jnp.int32


def exchanged(blocks, axis, index_groups=None):
    return lax.all_to_all(blocks, axis, 0, 0, axis_index_groups=index_groups, tiled=True)


def line_groups(ny, nx):
    along_x = [[y * nx + x for x in range(nx)] for y in range(ny)]
    along_y = [[y * nx + x for y in range(ny)] for x in range(nx)]

    def of_core_one(lines):
        return [[ny * nx + i for i in line] for line in lines]

    return along_x + of_core_one(along_y), along_y + of_core_one(along_x)


def line_pairs(ny, nx, by):
    pairs = []
    for y in range(ny):
        for x in range(nx):
            pairs.append((y * nx + x, y * nx + (x + by) % nx))
            pairs.append((ny * nx + y * nx + x, ny * nx + (y + by) % ny * nx + x))
    return pairs


def silu_grad(pre):
    sig = jax.nn.sigmoid(pre)
    return sig * (1.0 + pre * (1.0 - sig))


def contract(a, b, dim_a, dim_b):
    return lax.dot_general(a, b, (((dim_a,), (dim_b,)), ((), ())), preferred_element_type=f32)


def iota(shape, dim):
    return lax.broadcasted_iota(i32, shape, dim)


def whole():
    return pl.BlockSpec(memory_space=pltpu.VMEM)


def scalar():
    return pl.BlockSpec(memory_space=pltpu.SMEM)


def params(mib):
    return pltpu.CompilerParams(vmem_limit_bytes=mib * 1024 * 1024)


def cost(flops, size):
    return pl.CostEstimate(flops=flops, bytes_accessed=size, transcendentals=0)


def one_if(condition):
    return jnp.where(condition, 1.0, 0.0).astype(bf16)


def prep_kernel(lane_ref, ids_hbm, scale_hbm, input_hbm, grad_hbm, *refs, experts):
    sent_ref, back_ref, own_ref, ids_ref, scale_ref, input_ref, sems = refs
    tok, width = input_ref.shape
    columns = pl.ds(pl.multiple_of(lane_ref[0] * width, width), width)
    copies = [
        pltpu.make_async_copy(ids_hbm, ids_ref, sems.at[0]),
        pltpu.make_async_copy(scale_hbm, scale_ref, sems.at[1]),
        pltpu.make_async_copy(input_hbm.at[:, columns], input_ref, sems.at[2]),
        pltpu.make_async_copy(grad_hbm.at[:, columns], own_ref, sems.at[3]),
    ]
    for copy in copies:
        copy.start()
    for copy in copies:
        copy.wait()
    e0, e1 = ids_ref[0:1, :], ids_ref[1:2, :]
    s0, s1 = scale_ref[0:1, :], scale_ref[1:2, :]
    rows = iota((experts, tok), 0)
    hit0, hit1 = rows == e0, rows == e1
    earlier = one_if(iota((tok, tok), 0) < iota((tok, tok), 1))
    before = jnp.dot(one_if(hit0 | hit1), earlier, preferred_element_type=f32)
    slot0 = jnp.sum(jnp.where(hit0, before, 0.0), axis=0, keepdims=True).astype(i32)
    slot1 = jnp.sum(jnp.where(hit1, before, 0.0), axis=0, keepdims=True).astype(i32)
    x = input_ref[...]
    grad = own_ref[...]
    diagonal = iota((tok, tok), 0) == iota((tok, tok), 1)
    c0 = jnp.sum(jnp.where(diagonal, s0, 0.0), axis=1, keepdims=True)
    c1 = jnp.sum(jnp.where(diagonal, s1, 0.0), axis=1, keepdims=True)
    g = grad.astype(f32)
    g0, g1 = (g * c0).astype(bf16), (g * c1).astype(bf16)
    pitch = sent_ref.shape[0] // experts
    r = iota((sent_ref.shape[0], tok), 0)
    a0, a1 = e0 * pitch + slot0, e1 * pitch + slot1
    half = pitch // 2
    sent = jnp.dot(one_if((r == a0) | (r == a1)), x, preferred_element_type=f32)
    sent = sent + jnp.dot(one_if(r == a0 + half), g0, preferred_element_type=f32)
    sent = sent + jnp.dot(one_if(r == a1 + half), g1, preferred_element_type=f32)
    sent_ref[...] = sent.astype(bf16)
    back_pitch = back_ref.shape[0] // experts
    r = iota((back_ref.shape[0], tok), 0)
    back_ref[...] = one_if((r == e0 * back_pitch + slot0) | (r == e1 * back_pitch + slot1))


def packed(block):
    lanes = 128
    wide = block[:, :lanes]
    rest = block[:, lanes:]
    rows = rest.shape[0] // 2
    return wide, jnp.concatenate([rest[:rows], rest[rows:]], axis=1)


def unpacked(wide, rest):
    lanes = rest.shape[1] // 2
    tail = jnp.concatenate([rest[:, :lanes], rest[:, lanes:]], axis=0)
    return jnp.concatenate([wide, tail], axis=1)


def compact_kernel(part_ref, norm_ref, out_ref, *, capacity, pitch):
    count = out_ref.shape[0]
    rows_in = part_ref.shape[0] // count
    rows_out = rows_in // pitch * capacity
    into, outof = iota((rows_out, rows_in), 0), iota((rows_out, rows_in), 1)
    pick_x = one_if(outof == (into // capacity) * pitch + into % capacity)
    pick_g = one_if(outof == (into // capacity) * pitch + into % capacity + pitch // 2)
    wide, rest = packed(norm_ref[...].astype(f32))
    wide, rest = wide.astype(bf16), rest.astype(bf16)
    for q in range(count):
        piece = part_ref[pl.ds(q * rows_in, rows_in), :]
        out_ref[q, pl.ds(0, rows_out), :] = jnp.dot(pick_x, piece, preferred_element_type=f32).astype(bf16)
        out_ref[q, pl.ds(rows_out, rows_out), :] = jnp.dot(pick_g, piece, preferred_element_type=f32).astype(bf16)
        out_ref[q, pl.ds(2 * rows_out, wide.shape[0]), :] = wide
        out_ref[q, pl.ds(2 * rows_out + wide.shape[0], rest.shape[0]), :] = rest


def pieces_of(core_ref, ny, nx):
    core = core_ref[0]
    return [
        (jnp.where(core == 0, y, x), jnp.where(core == 0, x, y)) for y in range(ny) for x in range(nx)
    ]


def pack_kernel(gate_ref, up_ref, down_ref, out_ref):
    height, width = gate_ref.shape
    out_ref[pl.ds(0, height), :] = gate_ref[...]
    out_ref[pl.ds(height, height), :] = up_ref[...]
    for k in range(height // width):
        out_ref[pl.ds(2 * height + k * width, width), :] = down_ref[:, pl.ds(k * width, width)]


def expert_kernel(core_ref, rows_hbm, *refs):
    weights_hbm = refs[0:5]
    back_ref, hidden_ref, both_ref, rows_ref = refs[5:9]
    weights, acc_ref, sems = refs[9:13], refs[13], refs[14]
    middle = weights_hbm[3].shape[0]
    targets = (rows_ref, *weights[:3], weights[3].at[pl.ds(0, middle)], weights[3].at[pl.ds(middle, middle)])
    copies = [
        pltpu.make_async_copy(source, target, sems.at[i])
        for i, (source, target) in enumerate(zip((rows_hbm, *weights_hbm), targets, strict=True))
    ]
    for copy in copies:
        copy.start()
    ny, nx, _, width = rows_ref.shape
    count = hidden_ref.shape[0]
    pieces = pieces_of(core_ref, ny, nx)
    height = ny * nx * width
    copies[0].wait()
    x = jnp.concatenate([rows_ref[a, b, pl.ds(0, count), :] for a, b in pieces], axis=1)
    g = jnp.concatenate([rows_ref[a, b, pl.ds(count, count), :] for a, b in pieces], axis=1)
    for k, block in enumerate(weights):
        copies[1 + k].wait()
        if k == 3:
            copies[5].wait()
        w_both = jnp.concatenate([block[pl.ds(0, height), :], block[pl.ds(height, height), :]], axis=1)
        w_down = jnp.concatenate(
            [block[pl.ds(2 * height + i * width, width), :] for i in range(ny * nx)], axis=1
        )
        pre = jnp.dot(x, w_both, preferred_element_type=f32)
        gate_pre, up_pre = pre[:, :width], pre[:, width:]
        d_hidden = contract(g, w_down, 1, 1)
        sig = jax.nn.sigmoid(gate_pre)
        gate_act = gate_pre * sig
        hidden_ref[:, pl.ds(k * width, width)] = (gate_act * up_pre).astype(bf16)
        d_gate = d_hidden * up_pre * (sig * (1.0 + gate_pre * (1.0 - sig)))
        d_up = d_hidden * gate_act
        both = jnp.concatenate([d_gate.astype(bf16), d_up.astype(bf16)], axis=1)
        both_ref[:, pl.ds(2 * k * width, 2 * width)] = both
        back = contract(both, w_both, 1, 1)
        acc_ref[...] = back if k == 0 else acc_ref[...] + back
    for j, (a, b) in enumerate(pieces):
        back_ref[a, b] = acc_ref[:, pl.ds(j * width, width)].astype(bf16)


def weight_kernel(core_ref, rows_ref, hidden_ref, both_ref, *outs):
    ny, nx, _, width = rows_ref.shape
    count = hidden_ref.shape[0]
    height = ny * nx * width
    for j, (a, b) in enumerate(pieces_of(core_ref, ny, nx)):
        pairs = contract(rows_ref[a, b, pl.ds(0, count), :], both_ref[...], 0, 0).astype(bf16)
        downs = contract(hidden_ref[...], rows_ref[a, b, pl.ds(count, count), :], 0, 0).astype(bf16)
        for k, out_ref in enumerate(outs):
            out_ref[pl.ds(j * width, width), :] = pairs[:, 2 * k * width : (2 * k + 1) * width]
            out_ref[pl.ds(height + j * width, width), :] = pairs[:, (2 * k + 1) * width : (2 * k + 2) * width]
            out_ref[pl.ds(2 * height + j * width, width), :] = downs[k * width : (k + 1) * width]


def weight_sum_kernel(p0, p1, p2, p3, gate_ref, up_ref, down_ref):
    def summed(part):
        return (
            (p0[part, 0].astype(f32) + p1[part, 0].astype(f32)) + (p2[part, 0].astype(f32) + p3[part, 0].astype(f32))
        ).astype(bf16)

    gate_ref[...] = summed(0)
    up_ref[...] = summed(1)
    down = summed(2)
    size = down_ref.shape[0]
    for k in range(down.shape[0] // size):
        down_ref[:, pl.ds(k * size, size)] = down[k * size : (k + 1) * size]


def norm_kernel(core_ref, parts_ref, gain_ref, act_ref, slope_ref, cross_ref, stats_ref):
    ny, nx, height, _ = parts_ref.shape
    part = height * 2 // 3
    blocks = []
    for a, b in pieces_of(core_ref, ny, nx):
        block = parts_ref[a, b].astype(f32)
        blocks.append(unpacked(block[:part], block[part:]))
    values = jnp.concatenate(blocks, axis=0)
    channels = values.shape[0]
    mean = jnp.sum(values, axis=0, keepdims=True) / channels
    centred = values - mean
    inv = lax.rsqrt(jnp.sum(centred * centred, axis=0, keepdims=True) / channels + norm_eps)
    gain = gain_ref[...]
    normed = centred * inv
    scaled = normed * gain
    sig = jax.nn.sigmoid(scaled)
    act_ref[...] = (scaled * sig).astype(bf16)
    slope = sig * (1.0 + scaled * (1.0 - sig)) * gain
    slope_ref[...] = slope.astype(bf16)
    cross_ref[...] = (slope * normed).astype(bf16)
    stats_ref[0:1, :] = mean
    stats_ref[1:2, :] = inv


def line_sum_kernel(parts_ref, out_ref):
    acc = parts_ref[0].astype(f32)
    for j in range(1, parts_ref.shape[0]):
        acc = acc + parts_ref[j].astype(f32)
    out_ref[...] = acc.astype(bf16)


def spread_kernel(rows_ref, out_ref, *, capacity, pitch):
    count, rows_in, _ = rows_ref.shape
    rows_out = rows_in // capacity * pitch
    into, outof = iota((rows_out, rows_in), 0), iota((rows_out, rows_in), 1)
    spread = one_if((outof == (into // pitch) * capacity + into % pitch) & (into % pitch < capacity))
    for q in range(count):
        moved = jnp.dot(spread, rows_ref[q], preferred_element_type=f32)
        out_ref[pl.ds(q * rows_out, rows_out), :] = moved.astype(bf16)


def mix_kernel(core_ref, *refs):
    sources, outs, local, sems = refs[:7], refs[7:10], refs[10:17], refs[17]
    kept_ref, given_ref, blocks_ref = outs
    back_ref, returned_ref, own_ref, proj_ref, slope_ref, cross_ref, act_ref = local
    core = core_ref[0]
    copies = [
        pltpu.make_async_copy(source, target, sems.at[i])
        for i, (source, target) in enumerate(zip(sources, local, strict=True))
    ]
    for copy in copies:
        copy.start()
    for copy in copies[:3]:
        copy.wait()
    moe = contract(back_ref[...], returned_ref[...], 0, 0)
    mix = (own_ref[...].astype(f32) + moe).astype(bf16)
    for copy in copies[3:]:
        copy.wait()
    d_act = contract(proj_ref[...], mix, 1, 1)
    lanes = 128

    def as_rows(line):
        rest = line[:, lanes:]
        return [line[:, :lanes], jnp.concatenate([rest, jnp.zeros_like(rest)], axis=1)]

    tail = []
    for ref in (slope_ref, cross_ref):
        line = jnp.sum(ref[...].astype(f32) * d_act, axis=0, keepdims=True)
        high = line.astype(bf16).astype(f32)
        tail += as_rows(high) + as_rows(line - high)
    tail = jnp.concatenate(tail, axis=0).astype(bf16)
    count = blocks_ref.shape[0]
    part = d_act.shape[0] // count
    for j in range(count):
        wide, rest = packed(d_act[j * part : (j + 1) * part])
        blocks_ref[j, pl.ds(0, part), :] = wide.astype(bf16)
        blocks_ref[j, pl.ds(part, part // 2), :] = rest.astype(bf16)
        blocks_ref[j, pl.ds(part * 3 // 2, 8), :] = tail
    grad = jnp.dot(act_ref[...], mix, preferred_element_type=f32)
    size = kept_ref.shape[1]
    for k in range(kept_ref.shape[0]):
        even = grad[2 * k * size : (2 * k + 1) * size]
        odd = grad[(2 * k + 1) * size : (2 * k + 2) * size]
        kept_ref[k] = jnp.where(core == 0, even, odd).astype(bf16)
        given_ref[k] = jnp.where(core == 0, odd, even).astype(bf16)


def conv_grad_kernel(blocks_ref, norm_ref, gain_ref, stats_ref, out_ref, head_ref, *, channels):
    count, _, _ = blocks_ref.shape
    acc = blocks_ref[0].astype(f32)
    for j in range(1, count):
        acc = acc + blocks_ref[j].astype(f32)
    part = out_ref.shape[0]
    grad_act = unpacked(acc[:part], acc[part : part * 3 // 2])
    tail = acc[part * 3 // 2 :]

    def line(at):
        rest = tail[at + 1 : at + 2] + tail[at + 3 : at + 4]
        return jnp.concatenate([tail[at : at + 1] + tail[at + 2 : at + 3], rest[:, : rest.shape[1] // 2]], axis=1)

    mean, inv = stats_ref[0:1, :], stats_ref[1:2, :]
    gain = gain_ref[...]
    normed = (norm_ref[...].astype(f32) - mean) * inv
    grad_normed = grad_act * silu_grad(normed * gain) * gain
    out = inv * (grad_normed - line(0) / channels - normed * (line(4) / channels))
    out_ref[...] = out
    head_ref[...] = out[:, : head_ref.shape[1]]


def body(
    moe_input,
    out_grad,
    route_ids,
    route_weights,
    expert_gate,
    expert_up,
    expert_down,
    proj_weight,
    glu_value,
    glu_gate,
    conv_taps,
    norm_input,
    norm_gain,
):
    groups = lax.axis_size(SP)
    ny, nx = lax.axis_size("ty"), lax.axis_size("tx")
    lane_count = ny * nx
    lane_index = lax.axis_index(TP)
    tok_rows, model_width = moe_input.shape
    top_count = route_ids.shape[1]
    capacity = tok_rows * top_count * 3 // (2 * groups)
    total = groups * capacity
    width = model_width // lane_count
    pitch = 40
    back_pitch = 24
    channel_part = norm_input.shape[0]
    channels = channel_part * lane_count
    struct = jax.ShapeDtypeStruct

    sent, back_place, own_grad = pl.pallas_call(
        lambda *refs: prep_kernel(*refs, experts=groups),
        in_specs=[scalar()] + [pl.BlockSpec(memory_space=pltpu.HBM)] * 4,
        out_specs=[whole()] * 3,
        out_shape=[
            struct((groups * pitch, width), bf16),
            struct((groups * back_pitch, tok_rows), bf16),
            struct((tok_rows, width), bf16),
        ],
        scratch_shapes=[
            pltpu.VMEM((top_count, tok_rows), i32),
            pltpu.VMEM((top_count, tok_rows), f32),
            pltpu.VMEM((tok_rows, width), bf16),
            pltpu.SemaphoreType.DMA((4,)),
        ],
        compiler_params=params(58),
        name="prep",
    )(lane_index.astype(i32).reshape(1), route_ids.T, route_weights.T, moe_input, out_grad)

    part = exchanged(sent.reshape(groups, pitch, width), SP)

    core = lax.axis_index("core").astype(i32).reshape(1)
    first_groups, second_groups = line_groups(ny, nx)
    w_gate, w_up, w_down = expert_gate[0], expert_up[0], expert_down[0]
    ff = w_gate.shape[1]
    hbm = pl.BlockSpec(memory_space=pltpu.HBM)
    w_gate, w_up, w_down, _ = lax.optimization_barrier((w_gate, w_up, w_down, sent))
    own_weights = pl.pallas_call(
        pack_kernel,
        out_shape=struct((3 * model_width, ff), bf16),
        in_specs=[whole()] * 3,
        out_specs=whole(),
        compiler_params=params(58),
        cost_estimate=cost(8 * total * model_width * ff, 6 * model_width * ff),
        name="pack",
    )(w_gate, w_up, w_down)
    onward, backward, across = [line_pairs(ny, nx, by) for by in (1, -1, 2)]
    weights = (
        own_weights,
        lax.ppermute(own_weights, PLANE, onward),
        lax.ppermute(own_weights, PLANE, backward),
    )

    quarter = total // nx
    norm_rows = channel_part * 3 // 2
    rows_height = 2 * quarter + norm_rows
    quarters = pl.pallas_call(
        lambda *refs: compact_kernel(*refs, capacity=capacity, pitch=pitch),
        out_shape=struct((nx, rows_height, width), bf16),
        in_specs=[whole(), whole()],
        out_specs=whole(),
        compiler_params=params(16),
        name="compact",
    )(part.reshape(groups * pitch, width), norm_input)
    quarters, *weights = lax.optimization_barrier((exchanged(quarters, PLANE, first_groups), *weights))
    middle = weights[0].shape[0] // 2
    weights += [lax.ppermute(weights[1][:middle], PLANE, onward), lax.ppermute(weights[2][middle:], PLANE, backward)]
    gathered = exchanged(jnp.broadcast_to(quarters[None], (ny, *quarters.shape)), PLANE, second_groups)

    packed_weights = pltpu.VMEM((3 * model_width, ff), bf16)
    back, hidden, both = pl.pallas_call(
        expert_kernel,
        in_specs=[scalar()] + [hbm] * 6,
        out_specs=[whole()] * 3,
        out_shape=[
            struct((ny, nx, quarter, width), bf16),
            struct((quarter, nx * ff), bf16),
            struct((quarter, 2 * nx * ff), bf16),
        ],
        scratch_shapes=[
            pltpu.VMEM((ny, nx, rows_height, width), bf16),
            packed_weights,
            packed_weights,
            packed_weights,
            packed_weights,
            pltpu.VMEM((quarter, model_width), f32),
            pltpu.SemaphoreType.DMA((6,)),
        ],
        compiler_params=params(58),
        cost_estimate=cost(10 * total * model_width * ff, 10 * total * model_width),
        name="expert",
    )(core, gathered, *weights)

    line_parts = exchanged(back, PLANE, second_groups)
    wgrads = pl.pallas_call(
        weight_kernel,
        in_specs=[scalar()] + [whole()] * 3,
        out_specs=[whole()] * nx,
        out_shape=[struct((3 * model_width, ff), bf16)] * nx,
        compiler_params=params(58),
        cost_estimate=cost(6 * total * model_width * ff, 10 * total * model_width),
        name="weights",
    )(core, gathered, hidden, both)
    line_parts, *wgrads = lax.optimization_barrier((line_parts, *wgrads))
    line_rows = pl.pallas_call(
        line_sum_kernel,
        out_shape=struct((nx, quarter, width), bf16),
        in_specs=[whole()],
        out_specs=whole(),
        compiler_params=params(16),
        name="line_sum",
    )(line_parts)
    own_rows = exchanged(line_rows, PLANE, first_groups)
    summed_grad = pl.pallas_call(
        lambda *refs: spread_kernel(*refs, capacity=capacity, pitch=back_pitch),
        out_shape=struct((groups * back_pitch, width), bf16),
        in_specs=[whole()],
        out_specs=whole(),
        compiler_params=params(16),
        name="spread",
    )(own_rows)
    returned = exchanged(summed_grad.reshape(groups, back_pitch, width), SP)

    sent_wgrads = lax.optimization_barrier((summed_grad, *wgrads[1:]))[1:]
    from_ahead = lax.ppermute(sent_wgrads[0], PLANE, backward)
    from_behind = lax.ppermute(sent_wgrads[1], PLANE, onward)
    from_across = lax.ppermute(sent_wgrads[2], PLANE, across)
    line_wgrads = (wgrads[0], from_ahead, from_behind, from_across)

    act, slope, cross, stats = pl.pallas_call(
        norm_kernel,
        grid_spec=pltpu.PrefetchScalarGridSpec(
            num_scalar_prefetch=1,
            grid=(1,),
            in_specs=[
                pl.BlockSpec((ny, nx, norm_rows, width), lambda i, m: (0, 0, 2 * quarter // norm_rows, 0)),
                pl.BlockSpec((channels, 1), lambda i, m: (0, 0)),
            ],
            out_specs=[pl.BlockSpec((channels, tok_rows), lambda i, m: (0, 0))] * 3
            + [pl.BlockSpec((2, tok_rows), lambda i, m: (0, 0))],
        ),
        out_shape=[struct((channels, tok_rows), bf16)] * 3 + [struct((2, tok_rows), f32)],
        compiler_params=params(58),
        cost_estimate=cost(6 * total * model_width * ff, 10 * total * model_width),
        name="norm",
    )(core, gathered, norm_gain[:, None])

    proj_size = channels // groups
    block_rows = norm_rows + 8
    mix_inputs = (
        back_place,
        returned.reshape(groups * back_pitch, width),
        own_grad,
        proj_weight,
        slope,
        cross,
        act,
    )
    kept, given, blocks = pl.pallas_call(
        mix_kernel,
        out_shape=[
            struct((groups // 2, proj_size, width), bf16),
            struct((groups // 2, proj_size, width), bf16),
            struct((lane_count, block_rows, width), bf16),
        ],
        in_specs=[scalar()] + [pl.BlockSpec(memory_space=pltpu.HBM)] * len(mix_inputs),
        out_specs=[whole()] * 3,
        scratch_shapes=[pltpu.VMEM(value.shape, value.dtype) for value in mix_inputs]
        + [pltpu.SemaphoreType.DMA((len(mix_inputs),))],
        compiler_params=params(58),
        name="mix",
    )(core, *mix_inputs)
    arrived = exchanged(blocks, TP)
    from_pair = lax.ppermute(given, "core", [(0, 1), (1, 0)])
    chip_sum = (kept.astype(f32) + from_pair.astype(f32)).astype(bf16)
    chip_sum, arrived = lax.optimization_barrier((chip_sum, arrived))
    proj_parts = exchanged(chip_sum, "z")
    grad_proj = jnp.sum(proj_parts.astype(f32), axis=0)

    taps_count = conv_taps.shape[1]
    reach_back = taps_count - 1
    gain_own = lax.dynamic_slice_in_dim(norm_gain, lane_index * channel_part, channel_part, 0)
    grad_conv, head = pl.pallas_call(
        lambda *refs: conv_grad_kernel(*refs, channels=channels),
        out_shape=[struct((channel_part, tok_rows), f32), struct((channel_part, reach_back), f32)],
        in_specs=[whole()] * 4,
        out_specs=[whole()] * 2,
        compiler_params=params(16),
        name="conv_grad",
    )(arrived, norm_input, gain_own[:, None], stats)

    pairs = [(i, i - 1) for i in range(1, groups)]
    ahead_rows = lax.ppermute(head, SP, pairs)
    extended = jnp.concatenate([grad_conv, ahead_rows], axis=1)
    grad_glu = jnp.zeros_like(grad_conv)
    for tap_index in range(taps_count):
        grad_glu = (
            grad_glu
            + conv_taps[:, tap_index : tap_index + 1]
            * extended[:, reach_back - tap_index : reach_back - tap_index + tok_rows]
        )
    sigmoid_gate = jax.nn.sigmoid(glu_gate.astype(f32))
    grad_value = (grad_glu * sigmoid_gate).astype(bf16)
    grad_glu_gate = (
        grad_glu * glu_value.astype(f32) * sigmoid_gate * (1.0 - sigmoid_gate)
    ).astype(bf16)
    sum_rows = 256
    sum_steps = model_width // sum_rows
    parts = [value.reshape(3, sum_steps, sum_rows, ff) for value in line_wgrads]
    gate_wgrad, up_wgrad, down_grad = pl.pallas_call(
        weight_sum_kernel,
        grid=(sum_steps,),
        in_specs=[pl.BlockSpec((3, 1, sum_rows, ff), lambda i: (0, i, 0, 0))] * 4,
        out_specs=[
            pl.BlockSpec((sum_rows, ff), lambda i: (i, 0)),
            pl.BlockSpec((sum_rows, ff), lambda i: (i, 0)),
            pl.BlockSpec((ff, sum_rows), lambda i: (0, i)),
        ],
        out_shape=[
            struct((model_width, ff), bf16),
            struct((model_width, ff), bf16),
            struct((ff, model_width), bf16),
        ],
        compiler_params=params(58),
        cost_estimate=cost(6 * total * model_width * ff, 10 * total * model_width),
        name="weight_sum",
    )(*parts)
    return (gate_wgrad[None], up_wgrad[None], down_grad[None], grad_proj, grad_value, grad_glu_gate)


def solution(mesh):
    finer = Mesh(mesh.devices.reshape(mesh.shape["sp"] // 2, 2, 4, 4), ("z", "core", "ty", "tx"))
    return jax.shard_map(
        body,
        mesh=finer,
        in_specs=(
            P(SP, None),
            P(SP, None),
            P(SP, None),
            P(SP, None),
            P(SP, None, TP),
            P(SP, None, TP),
            P(SP, TP, None),
            P(None, TP),
            P(TP, SP),
            P(TP, SP),
            P(TP, None),
            P(TP, SP),
            P(),
        ),
        out_specs=(
            P(SP, None, TP),
            P(SP, None, TP),
            P(SP, TP, None),
            P(SP, TP),
            P(TP, SP),
            P(TP, SP),
        ),
        check_vma=False,
    )
```

```python
import jax
import jax.numpy as jnp
from jax import lax
from jax.experimental import pallas as pl
from jax.experimental.pallas import tpu as pltpu
from jax.sharding import Mesh
from jax.sharding import PartitionSpec as P

TP = ("ty", "tx")
SP = ("z", "core")
PLANE = ("core", "ty", "tx")


norm_eps = 1e-05

bf16, f32, i32 = jnp.bfloat16, jnp.float32, jnp.int32


def exchanged(blocks, axis, index_groups=None):
    return lax.all_to_all(blocks, axis, 0, 0, axis_index_groups=index_groups, tiled=True)


def line_groups(ny, nx):
    along_x = [[y * nx + x for x in range(nx)] for y in range(ny)]
    along_y = [[y * nx + x for y in range(ny)] for x in range(nx)]

    def of_core_one(lines):
        return [[ny * nx + i for i in line] for line in lines]

    return along_x + of_core_one(along_y), along_y + of_core_one(along_x)


def line_pairs(ny, nx, by):
    pairs = []
    for y in range(ny):
        for x in range(nx):
            pairs.append((y * nx + x, y * nx + (x + by) % nx))
            pairs.append((ny * nx + y * nx + x, ny * nx + (y + by) % ny * nx + x))
    return pairs


def silu_grad(pre):
    sig = jax.nn.sigmoid(pre)
    return sig * (1.0 + pre * (1.0 - sig))


def contract(a, b, dim_a, dim_b):
    return lax.dot_general(a, b, (((dim_a,), (dim_b,)), ((), ())), preferred_element_type=f32)


def iota(shape, dim):
    return lax.broadcasted_iota(i32, shape, dim)


def whole():
    return pl.BlockSpec(memory_space=pltpu.VMEM)


def scalar():
    return pl.BlockSpec(memory_space=pltpu.SMEM)


def params(mib):
    return pltpu.CompilerParams(vmem_limit_bytes=mib * 1024 * 1024)


def cost(flops, size):
    return pl.CostEstimate(flops=flops, bytes_accessed=size, transcendentals=0)


def one_if(condition):
    return jnp.where(condition, 1.0, 0.0).astype(bf16)


def prep_kernel(lane_ref, ids_hbm, scale_hbm, input_hbm, grad_hbm, *refs, experts):
    sent_ref, back_ref, own_ref, ids_ref, scale_ref, input_ref, sems = refs
    tok, width = input_ref.shape
    columns = pl.ds(pl.multiple_of(lane_ref[0] * width, width), width)
    copies = [
        pltpu.make_async_copy(ids_hbm, ids_ref, sems.at[0]),
        pltpu.make_async_copy(scale_hbm, scale_ref, sems.at[1]),
        pltpu.make_async_copy(input_hbm.at[:, columns], input_ref, sems.at[2]),
        pltpu.make_async_copy(grad_hbm.at[:, columns], own_ref, sems.at[3]),
    ]
    for copy in copies:
        copy.start()
    for copy in copies:
        copy.wait()
    e0, e1 = ids_ref[0:1, :], ids_ref[1:2, :]
    s0, s1 = scale_ref[0:1, :], scale_ref[1:2, :]
    rows = iota((experts, tok), 0)
    hit0, hit1 = rows == e0, rows == e1
    earlier = one_if(iota((tok, tok), 0) < iota((tok, tok), 1))
    before = jnp.dot(one_if(hit0 | hit1), earlier, preferred_element_type=f32)
    slot0 = jnp.sum(jnp.where(hit0, before, 0.0), axis=0, keepdims=True).astype(i32)
    slot1 = jnp.sum(jnp.where(hit1, before, 0.0), axis=0, keepdims=True).astype(i32)
    x = input_ref[...]
    grad = own_ref[...]
    diagonal = iota((tok, tok), 0) == iota((tok, tok), 1)
    c0 = jnp.sum(jnp.where(diagonal, s0, 0.0), axis=1, keepdims=True)
    c1 = jnp.sum(jnp.where(diagonal, s1, 0.0), axis=1, keepdims=True)
    g = grad.astype(f32)
    g0, g1 = (g * c0).astype(bf16), (g * c1).astype(bf16)
    pitch = sent_ref.shape[0] // experts
    r = iota((sent_ref.shape[0], tok), 0)
    a0, a1 = e0 * pitch + slot0, e1 * pitch + slot1
    half = pitch // 2
    sent = jnp.dot(one_if((r == a0) | (r == a1)), x, preferred_element_type=f32)
    sent = sent + jnp.dot(one_if(r == a0 + half), g0, preferred_element_type=f32)
    sent = sent + jnp.dot(one_if(r == a1 + half), g1, preferred_element_type=f32)
    sent_ref[...] = sent.astype(bf16)
    back_pitch = back_ref.shape[0] // experts
    r = iota((back_ref.shape[0], tok), 0)
    back_ref[...] = one_if((r == e0 * back_pitch + slot0) | (r == e1 * back_pitch + slot1))


def packed(block):
    lanes = 128
    wide = block[:, :lanes]
    rest = block[:, lanes:]
    rows = rest.shape[0] // 2
    return wide, jnp.concatenate([rest[:rows], rest[rows:]], axis=1)


def unpacked(wide, rest):
    lanes = rest.shape[1] // 2
    tail = jnp.concatenate([rest[:, :lanes], rest[:, lanes:]], axis=0)
    return jnp.concatenate([wide, tail], axis=1)


def compact_kernel(part_ref, norm_ref, out_ref, *, capacity, pitch):
    count = out_ref.shape[0]
    rows_in = part_ref.shape[0] // count
    rows_out = rows_in // pitch * capacity
    into, outof = iota((rows_out, rows_in), 0), iota((rows_out, rows_in), 1)
    pick_x = one_if(outof == (into // capacity) * pitch + into % capacity)
    pick_g = one_if(outof == (into // capacity) * pitch + into % capacity + pitch // 2)
    wide, rest = packed(norm_ref[...].astype(f32))
    wide, rest = wide.astype(bf16), rest.astype(bf16)
    for q in range(count):
        piece = part_ref[pl.ds(q * rows_in, rows_in), :]
        out_ref[q, pl.ds(0, rows_out), :] = jnp.dot(pick_x, piece, preferred_element_type=f32).astype(bf16)
        out_ref[q, pl.ds(rows_out, rows_out), :] = jnp.dot(pick_g, piece, preferred_element_type=f32).astype(bf16)
        out_ref[q, pl.ds(2 * rows_out, wide.shape[0]), :] = wide
        out_ref[q, pl.ds(2 * rows_out + wide.shape[0], rest.shape[0]), :] = rest


def pieces_of(core_ref, ny, nx):
    core = core_ref[0]
    return [
        (jnp.where(core == 0, y, x), jnp.where(core == 0, x, y)) for y in range(ny) for x in range(nx)
    ]


def pack_kernel(gate_ref, up_ref, down_ref, out_ref):
    height, width = gate_ref.shape
    out_ref[pl.ds(0, height), :] = gate_ref[...]
    out_ref[pl.ds(height, height), :] = up_ref[...]
    for k in range(height // width):
        out_ref[pl.ds(2 * height + k * width, width), :] = down_ref[:, pl.ds(k * width, width)]


def expert_kernel(core_ref, rows_ref, *refs):
    weights_hbm = refs[0:5]
    back_ref, hidden_ref, both_ref = refs[5:8]
    weights, acc_ref, sems = refs[8:12], refs[12], refs[13]
    middle = weights_hbm[3].shape[0]
    targets = (*weights[:3], weights[3].at[pl.ds(0, middle)], weights[3].at[pl.ds(middle, middle)])
    copies = [
        pltpu.make_async_copy(source, target, sems.at[i])
        for i, (source, target) in enumerate(zip(weights_hbm, targets, strict=True))
    ]
    for copy in copies:
        copy.start()
    ny, nx, _, width = rows_ref.shape
    count = hidden_ref.shape[0]
    pieces = pieces_of(core_ref, ny, nx)
    height = ny * nx * width
    x = jnp.concatenate([rows_ref[a, b, pl.ds(0, count), :] for a, b in pieces], axis=1)
    g = jnp.concatenate([rows_ref[a, b, pl.ds(count, count), :] for a, b in pieces], axis=1)
    for k, block in enumerate(weights):
        copies[k].wait()
        if k == 3:
            copies[4].wait()
        w_both = jnp.concatenate([block[pl.ds(0, height), :], block[pl.ds(height, height), :]], axis=1)
        w_down = jnp.concatenate(
            [block[pl.ds(2 * height + i * width, width), :] for i in range(ny * nx)], axis=1
        )
        pre = jnp.dot(x, w_both, preferred_element_type=f32)
        gate_pre, up_pre = pre[:, :width], pre[:, width:]
        d_hidden = contract(g, w_down, 1, 1)
        sig = jax.nn.sigmoid(gate_pre)
        gate_act = gate_pre * sig
        hidden_ref[:, pl.ds(k * width, width)] = (gate_act * up_pre).astype(bf16)
        d_gate = d_hidden * up_pre * (sig * (1.0 + gate_pre * (1.0 - sig)))
        d_up = d_hidden * gate_act
        both = jnp.concatenate([d_gate.astype(bf16), d_up.astype(bf16)], axis=1)
        both_ref[:, pl.ds(2 * k * width, 2 * width)] = both
        back = contract(both, w_both, 1, 1)
        acc_ref[...] = back if k == 0 else acc_ref[...] + back
    for j, (a, b) in enumerate(pieces):
        back_ref[a, b] = acc_ref[:, pl.ds(j * width, width)].astype(bf16)


def row_pack_kernel(core_ref, rows_ref, hidden_ref, both_ref, onward_ref, backward_ref, across_ref):
    ny, nx, _, width = rows_ref.shape
    count = hidden_ref.shape[0]
    for j, (a, b) in enumerate(pieces_of(core_ref, ny, nx)):
        rows = rows_ref[a, b, pl.ds(0, 2 * count), :]
        onward_ref[pl.ds(2 * j * count, 2 * count), :] = rows
        backward_ref[pl.ds(2 * j * count, 2 * count), :] = rows
    start = 2 * ny * nx * count
    for k, out_ref, at in ((2, onward_ref, start), (1, backward_ref, start), (3, across_ref, 0)):
        out_ref[pl.ds(at, count), :] = hidden_ref[:, pl.ds(k * width, width)]
        out_ref[pl.ds(at + count, count), :] = both_ref[:, pl.ds(2 * k * width, width)]
        out_ref[pl.ds(at + 2 * count, count), :] = both_ref[:, pl.ds((2 * k + 1) * width, width)]


def weight_kernel(own_ref, behind_ref, ahead_ref, low_ref, high_ref, across_ref, hidden_ref, both_ref, *outs):
    gate_ref, up_ref, down_ref = outs
    count, width = hidden_ref.shape[0], own_ref.shape[1]
    number = down_ref.shape[1] // width
    start = 2 * number * count

    def units(part, own):
        at = part * count
        return jnp.concatenate(
            [
                own,
                behind_ref[pl.ds(start + at, count), :],
                ahead_ref[pl.ds(start + at, count), :],
                across_ref[pl.ds(at, count), :],
            ],
            axis=0,
        )

    hidden = units(0, hidden_ref[:, :width])
    both = jnp.concatenate(
        [units(1, both_ref[:, :width]), units(2, both_ref[:, width : 2 * width])], axis=1
    )
    half = number // 2
    for j in range(number):
        far_ref, i = (low_ref, j) if j < half else (high_ref, j - half)

        def rows(part):
            at = (2 * j + part) * count
            near = [ref[pl.ds(at, count), :] for ref in (own_ref, behind_ref, ahead_ref)]
            return jnp.concatenate([*near, far_ref[pl.ds((2 * i + part) * count, count), :]], axis=0)

        pair = contract(rows(0), both, 0, 0)
        at = pl.ds(j * width, width)
        gate_ref[at, :] = pair[:, :width].astype(bf16)
        up_ref[at, :] = pair[:, width:].astype(bf16)
        down_ref[:, at] = contract(hidden, rows(1), 0, 0).astype(bf16)


def norm_kernel(core_ref, parts_ref, gain_ref, act_ref, slope_ref, cross_ref, stats_ref):
    ny, nx, height, _ = parts_ref.shape
    part = height * 2 // 3
    blocks = []
    for a, b in pieces_of(core_ref, ny, nx):
        block = parts_ref[a, b].astype(f32)
        blocks.append(unpacked(block[:part], block[part:]))
    values = jnp.concatenate(blocks, axis=0)
    channels = values.shape[0]
    mean = jnp.sum(values, axis=0, keepdims=True) / channels
    centred = values - mean
    inv = lax.rsqrt(jnp.sum(centred * centred, axis=0, keepdims=True) / channels + norm_eps)
    gain = gain_ref[...]
    normed = centred * inv
    scaled = normed * gain
    sig = jax.nn.sigmoid(scaled)
    act_ref[...] = (scaled * sig).astype(bf16)
    slope = sig * (1.0 + scaled * (1.0 - sig)) * gain
    slope_ref[...] = slope.astype(bf16)
    cross_ref[...] = (slope * normed).astype(bf16)
    stats_ref[0:1, :] = mean
    stats_ref[1:2, :] = inv


def line_sum_kernel(parts_ref, out_ref):
    acc = parts_ref[0].astype(f32)
    for j in range(1, parts_ref.shape[0]):
        acc = acc + parts_ref[j].astype(f32)
    out_ref[...] = acc.astype(bf16)


def spread_kernel(rows_ref, out_ref, *, capacity, pitch):
    count, rows_in, _ = rows_ref.shape
    rows_out = rows_in // capacity * pitch
    into, outof = iota((rows_out, rows_in), 0), iota((rows_out, rows_in), 1)
    spread = one_if((outof == (into // pitch) * capacity + into % pitch) & (into % pitch < capacity))
    for q in range(count):
        moved = jnp.dot(spread, rows_ref[q], preferred_element_type=f32)
        out_ref[pl.ds(q * rows_out, rows_out), :] = moved.astype(bf16)


def mix_kernel(core_ref, *refs):
    sources, outs, local, sems = refs[:7], refs[7:10], refs[10:17], refs[17]
    kept_ref, given_ref, blocks_ref = outs
    back_ref, returned_ref, own_ref, proj_ref, slope_ref, cross_ref, act_ref = local
    core = core_ref[0]
    copies = [
        pltpu.make_async_copy(source, target, sems.at[i])
        for i, (source, target) in enumerate(zip(sources, local, strict=True))
    ]
    for copy in copies:
        copy.start()
    for copy in copies[:3]:
        copy.wait()
    moe = contract(back_ref[...], returned_ref[...], 0, 0)
    mix = (own_ref[...].astype(f32) + moe).astype(bf16)
    for copy in copies[3:]:
        copy.wait()
    d_act = contract(proj_ref[...], mix, 1, 1)
    lanes = 128

    def as_rows(line):
        rest = line[:, lanes:]
        return [line[:, :lanes], jnp.concatenate([rest, jnp.zeros_like(rest)], axis=1)]

    tail = []
    for ref in (slope_ref, cross_ref):
        line = jnp.sum(ref[...].astype(f32) * d_act, axis=0, keepdims=True)
        high = line.astype(bf16).astype(f32)
        tail += as_rows(high) + as_rows(line - high)
    tail = jnp.concatenate(tail, axis=0).astype(bf16)
    count = blocks_ref.shape[0]
    part = d_act.shape[0] // count
    for j in range(count):
        wide, rest = packed(d_act[j * part : (j + 1) * part])
        blocks_ref[j, pl.ds(0, part), :] = wide.astype(bf16)
        blocks_ref[j, pl.ds(part, part // 2), :] = rest.astype(bf16)
        blocks_ref[j, pl.ds(part * 3 // 2, 8), :] = tail
    grad = jnp.dot(act_ref[...], mix, preferred_element_type=f32)
    size = kept_ref.shape[1]
    for k in range(kept_ref.shape[0]):
        even = grad[2 * k * size : (2 * k + 1) * size]
        odd = grad[(2 * k + 1) * size : (2 * k + 2) * size]
        kept_ref[k] = jnp.where(core == 0, even, odd).astype(bf16)
        given_ref[k] = jnp.where(core == 0, odd, even).astype(bf16)


def conv_grad_kernel(blocks_ref, norm_ref, gain_ref, stats_ref, out_ref, head_ref, *, channels):
    count, _, _ = blocks_ref.shape
    acc = blocks_ref[0].astype(f32)
    for j in range(1, count):
        acc = acc + blocks_ref[j].astype(f32)
    part = out_ref.shape[0]
    grad_act = unpacked(acc[:part], acc[part : part * 3 // 2])
    tail = acc[part * 3 // 2 :]

    def line(at):
        rest = tail[at + 1 : at + 2] + tail[at + 3 : at + 4]
        return jnp.concatenate([tail[at : at + 1] + tail[at + 2 : at + 3], rest[:, : rest.shape[1] // 2]], axis=1)

    mean, inv = stats_ref[0:1, :], stats_ref[1:2, :]
    gain = gain_ref[...]
    normed = (norm_ref[...].astype(f32) - mean) * inv
    grad_normed = grad_act * silu_grad(normed * gain) * gain
    out = inv * (grad_normed - line(0) / channels - normed * (line(4) / channels))
    out_ref[...] = out
    head_ref[...] = out[:, : head_ref.shape[1]]


def body(
    moe_input,
    out_grad,
    route_ids,
    route_weights,
    expert_gate,
    expert_up,
    expert_down,
    proj_weight,
    glu_value,
    glu_gate,
    conv_taps,
    norm_input,
    norm_gain,
):
    groups = lax.axis_size(SP)
    ny, nx = lax.axis_size("ty"), lax.axis_size("tx")
    lane_count = ny * nx
    lane_index = lax.axis_index(TP)
    tok_rows, model_width = moe_input.shape
    top_count = route_ids.shape[1]
    capacity = tok_rows * top_count * 3 // (2 * groups)
    total = groups * capacity
    width = model_width // lane_count
    pitch = 40
    back_pitch = 24
    channel_part = norm_input.shape[0]
    channels = channel_part * lane_count
    struct = jax.ShapeDtypeStruct

    sent, back_place, own_grad = pl.pallas_call(
        lambda *refs: prep_kernel(*refs, experts=groups),
        in_specs=[scalar()] + [pl.BlockSpec(memory_space=pltpu.HBM)] * 4,
        out_specs=[whole()] * 3,
        out_shape=[
            struct((groups * pitch, width), bf16),
            struct((groups * back_pitch, tok_rows), bf16),
            struct((tok_rows, width), bf16),
        ],
        scratch_shapes=[
            pltpu.VMEM((top_count, tok_rows), i32),
            pltpu.VMEM((top_count, tok_rows), f32),
            pltpu.VMEM((tok_rows, width), bf16),
            pltpu.SemaphoreType.DMA((4,)),
        ],
        compiler_params=params(58),
        name="prep",
    )(lane_index.astype(i32).reshape(1), route_ids.T, route_weights.T, moe_input, out_grad)

    part = exchanged(sent.reshape(groups, pitch, width), SP)

    core = lax.axis_index("core").astype(i32).reshape(1)
    first_groups, second_groups = line_groups(ny, nx)
    w_gate, w_up, w_down = expert_gate[0], expert_up[0], expert_down[0]
    ff = w_gate.shape[1]
    hbm = pl.BlockSpec(memory_space=pltpu.HBM)
    w_gate, w_up, w_down, _ = lax.optimization_barrier((w_gate, w_up, w_down, sent))
    own_weights = pl.pallas_call(
        pack_kernel,
        out_shape=struct((3 * model_width, ff), bf16),
        in_specs=[whole()] * 3,
        out_specs=whole(),
        compiler_params=params(58),
        cost_estimate=cost(8 * total * model_width * ff, 6 * model_width * ff),
        name="pack",
    )(w_gate, w_up, w_down)
    onward, backward, across = [line_pairs(ny, nx, by) for by in (1, -1, 2)]
    weights = (
        own_weights,
        lax.ppermute(own_weights, PLANE, onward),
        lax.ppermute(own_weights, PLANE, backward),
    )

    quarter = total // nx
    norm_rows = channel_part * 3 // 2
    rows_height = 2 * quarter + norm_rows
    quarters = pl.pallas_call(
        lambda *refs: compact_kernel(*refs, capacity=capacity, pitch=pitch),
        out_shape=struct((nx, rows_height, width), bf16),
        in_specs=[whole(), whole()],
        out_specs=whole(),
        compiler_params=params(16),
        name="compact",
    )(part.reshape(groups * pitch, width), norm_input)
    quarters, *weights = lax.optimization_barrier((exchanged(quarters, PLANE, first_groups), *weights))
    middle = weights[0].shape[0] // 2
    weights += [
        lax.ppermute(weights[1][:middle], PLANE, onward),
        lax.ppermute(weights[2][middle:], PLANE, backward),
    ]
    gathered = exchanged(jnp.broadcast_to(quarters[None], (ny, *quarters.shape)), PLANE, second_groups)

    packed_weights = pltpu.VMEM((3 * model_width, ff), bf16)
    back, hidden, both = pl.pallas_call(
        expert_kernel,
        in_specs=[scalar(), whole()] + [hbm] * 5,
        out_specs=[whole()] * 3,
        out_shape=[
            struct((ny, nx, quarter, width), bf16),
            struct((quarter, nx * ff), bf16),
            struct((quarter, 2 * nx * ff), bf16),
        ],
        scratch_shapes=[
            packed_weights,
            packed_weights,
            packed_weights,
            packed_weights,
            pltpu.VMEM((quarter, model_width), f32),
            pltpu.SemaphoreType.DMA((5,)),
        ],
        compiler_params=params(50),
        cost_estimate=cost(10 * total * model_width * ff, 10 * total * model_width),
        name="expert",
    )(core, gathered, *weights)

    line_parts = exchanged(back, PLANE, second_groups)
    unit_rows = 3 * quarter
    buffer_rows = 2 * lane_count * quarter + unit_rows
    to_onward, to_backward, to_across = pl.pallas_call(
        row_pack_kernel,
        in_specs=[scalar()] + [whole()] * 3,
        out_specs=[whole()] * 3,
        out_shape=[
            struct((buffer_rows, width), bf16),
            struct((buffer_rows, width), bf16),
            struct((unit_rows, width), bf16),
        ],
        compiler_params=params(58),
        cost_estimate=cost(6 * total * model_width * ff, 10 * total * model_width),
        name="row_pack",
    )(core, gathered, hidden, both)
    line_parts, to_onward, to_backward, to_across = lax.optimization_barrier(
        (line_parts, to_onward, to_backward, to_across)
    )
    line_rows = pl.pallas_call(
        line_sum_kernel,
        out_shape=struct((nx, quarter, width), bf16),
        in_specs=[whole()],
        out_specs=whole(),
        compiler_params=params(16),
        name="line_sum",
    )(line_parts)
    own_rows = exchanged(line_rows, PLANE, first_groups)
    summed_grad = pl.pallas_call(
        lambda *refs: spread_kernel(*refs, capacity=capacity, pitch=back_pitch),
        out_shape=struct((groups * back_pitch, width), bf16),
        in_specs=[whole()],
        out_specs=whole(),
        compiler_params=params(16),
        name="spread",
    )(own_rows)
    returned = exchanged(summed_grad.reshape(groups, back_pitch, width), SP)

    own_buffer = to_onward
    summed_grad, to_onward, to_backward, to_across = lax.optimization_barrier(
        (summed_grad, to_onward, to_backward, to_across)
    )
    from_behind = lax.ppermute(to_onward, PLANE, onward)
    from_ahead = lax.ppermute(to_backward, PLANE, backward)
    from_across = lax.ppermute(to_across, PLANE, across)
    far_rows = lane_count * quarter
    far_low = lax.ppermute(from_behind[:far_rows], PLANE, onward)
    far_high = lax.ppermute(from_ahead[far_rows : 2 * far_rows], PLANE, backward)

    act, slope, cross, stats = pl.pallas_call(
        norm_kernel,
        grid_spec=pltpu.PrefetchScalarGridSpec(
            num_scalar_prefetch=1,
            grid=(1,),
            in_specs=[
                pl.BlockSpec((ny, nx, norm_rows, width), lambda i, m: (0, 0, 2 * quarter // norm_rows, 0)),
                pl.BlockSpec((channels, 1), lambda i, m: (0, 0)),
            ],
            out_specs=[pl.BlockSpec((channels, tok_rows), lambda i, m: (0, 0))] * 3
            + [pl.BlockSpec((2, tok_rows), lambda i, m: (0, 0))],
        ),
        out_shape=[struct((channels, tok_rows), bf16)] * 3 + [struct((2, tok_rows), f32)],
        compiler_params=params(58),
        cost_estimate=cost(6 * total * model_width * ff, 10 * total * model_width),
        name="norm",
    )(core, gathered, norm_gain[:, None])

    proj_size = channels // groups
    block_rows = norm_rows + 8
    mix_inputs = (
        back_place,
        returned.reshape(groups * back_pitch, width),
        own_grad,
        proj_weight,
        slope,
        cross,
        act,
    )
    kept, given, blocks = pl.pallas_call(
        mix_kernel,
        out_shape=[
            struct((groups // 2, proj_size, width), bf16),
            struct((groups // 2, proj_size, width), bf16),
            struct((lane_count, block_rows, width), bf16),
        ],
        in_specs=[scalar()] + [pl.BlockSpec(memory_space=pltpu.HBM)] * len(mix_inputs),
        out_specs=[whole()] * 3,
        scratch_shapes=[pltpu.VMEM(value.shape, value.dtype) for value in mix_inputs]
        + [pltpu.SemaphoreType.DMA((len(mix_inputs),))],
        compiler_params=params(58),
        name="mix",
    )(core, *mix_inputs)
    arrived = exchanged(blocks, TP)
    from_pair = lax.ppermute(given, "core", [(0, 1), (1, 0)])
    chip_sum = (kept.astype(f32) + from_pair.astype(f32)).astype(bf16)
    chip_sum, arrived = lax.optimization_barrier((chip_sum, arrived))
    proj_parts = exchanged(chip_sum, "z")
    grad_proj = jnp.sum(proj_parts.astype(f32), axis=0)

    taps_count = conv_taps.shape[1]
    reach_back = taps_count - 1
    gain_own = lax.dynamic_slice_in_dim(norm_gain, lane_index * channel_part, channel_part, 0)
    grad_conv, head = pl.pallas_call(
        lambda *refs: conv_grad_kernel(*refs, channels=channels),
        out_shape=[struct((channel_part, tok_rows), f32), struct((channel_part, reach_back), f32)],
        in_specs=[whole()] * 4,
        out_specs=[whole()] * 2,
        compiler_params=params(16),
        name="conv_grad",
    )(arrived, norm_input, gain_own[:, None], stats)

    pairs = [(i, i - 1) for i in range(1, groups)]
    ahead_rows = lax.ppermute(head, SP, pairs)
    extended = jnp.concatenate([grad_conv, ahead_rows], axis=1)
    grad_glu = jnp.zeros_like(grad_conv)
    for tap_index in range(taps_count):
        grad_glu = (
            grad_glu
            + conv_taps[:, tap_index : tap_index + 1]
            * extended[:, reach_back - tap_index : reach_back - tap_index + tok_rows]
        )
    sigmoid_gate = jax.nn.sigmoid(glu_gate.astype(f32))
    grad_value = (grad_glu * sigmoid_gate).astype(bf16)
    grad_glu_gate = (
        grad_glu * glu_value.astype(f32) * sigmoid_gate * (1.0 - sigmoid_gate)
    ).astype(bf16)
    gate_wgrad, up_wgrad, down_grad = pl.pallas_call(
        weight_kernel,
        in_specs=[whole()] * 8,
        out_specs=[whole()] * 3,
        out_shape=[
            struct((model_width, ff), bf16),
            struct((model_width, ff), bf16),
            struct((ff, model_width), bf16),
        ],
        compiler_params=params(58),
        cost_estimate=cost(6 * total * model_width * ff, 10 * total * model_width),
        name="weight_sum",
    )(own_buffer, from_behind, from_ahead, far_low, far_high, from_across, hidden, both)
    return (gate_wgrad[None], up_wgrad[None], down_grad[None], grad_proj, grad_value, grad_glu_gate)


def solution(mesh):
    finer = Mesh(mesh.devices.reshape(mesh.shape["sp"] // 2, 2, 4, 4), ("z", "core", "ty", "tx"))
    return jax.shard_map(
        body,
        mesh=finer,
        in_specs=(
            P(SP, None),
            P(SP, None),
            P(SP, None),
            P(SP, None),
            P(SP, None, TP),
            P(SP, None, TP),
            P(SP, TP, None),
            P(None, TP),
            P(TP, SP),
            P(TP, SP),
            P(TP, None),
            P(TP, SP),
            P(),
        ),
        out_specs=(
            P(SP, None, TP),
            P(SP, None, TP),
            P(SP, TP, None),
            P(SP, TP),
            P(TP, SP),
            P(TP, SP),
        ),
        check_vma=False,
    )
```

```python
import jax
import jax.numpy as jnp
from jax import lax
from jax.experimental import pallas as pl
from jax.experimental.pallas import tpu as pltpu
from jax.sharding import Mesh
from jax.sharding import PartitionSpec as P

TP = ("ty", "tx")
SP = ("z", "core")
PLANE = ("core", "ty", "tx")


norm_eps = 1e-05

bf16, f32, i32 = jnp.bfloat16, jnp.float32, jnp.int32


def exchanged(blocks, axis, index_groups=None):
    return lax.all_to_all(blocks, axis, 0, 0, axis_index_groups=index_groups, tiled=True)


def line_groups(ny, nx):
    along_x = [[y * nx + x for x in range(nx)] for y in range(ny)]
    along_y = [[y * nx + x for y in range(ny)] for x in range(nx)]

    def of_core_one(lines):
        return [[ny * nx + i for i in line] for line in lines]

    return along_x + of_core_one(along_y), along_y + of_core_one(along_x)


def line_pairs(ny, nx, by):
    pairs = []
    for y in range(ny):
        for x in range(nx):
            pairs.append((y * nx + x, y * nx + (x + by) % nx))
            pairs.append((ny * nx + y * nx + x, ny * nx + (y + by) % ny * nx + x))
    return pairs


def silu_grad(pre):
    sig = jax.nn.sigmoid(pre)
    return sig * (1.0 + pre * (1.0 - sig))


def contract(a, b, dim_a, dim_b):
    return lax.dot_general(a, b, (((dim_a,), (dim_b,)), ((), ())), preferred_element_type=f32)


def iota(shape, dim):
    return lax.broadcasted_iota(i32, shape, dim)


def whole():
    return pl.BlockSpec(memory_space=pltpu.VMEM)


def scalar():
    return pl.BlockSpec(memory_space=pltpu.SMEM)


def params(mib):
    return pltpu.CompilerParams(vmem_limit_bytes=mib * 1024 * 1024)


def cost(flops, size):
    return pl.CostEstimate(flops=flops, bytes_accessed=size, transcendentals=0)


def one_if(condition):
    return jnp.where(condition, 1.0, 0.0).astype(bf16)


def prep_kernel(lane_ref, ids_hbm, scale_hbm, input_hbm, grad_hbm, *refs, experts):
    sent_ref, back_ref, own_ref, ids_ref, scale_ref, input_ref, sems = refs
    tok, width = input_ref.shape
    columns = pl.ds(pl.multiple_of(lane_ref[0] * width, width), width)
    copies = [
        pltpu.make_async_copy(ids_hbm, ids_ref, sems.at[0]),
        pltpu.make_async_copy(scale_hbm, scale_ref, sems.at[1]),
        pltpu.make_async_copy(input_hbm.at[:, columns], input_ref, sems.at[2]),
        pltpu.make_async_copy(grad_hbm.at[:, columns], own_ref, sems.at[3]),
    ]
    for copy in copies:
        copy.start()
    for copy in copies:
        copy.wait()
    e0, e1 = ids_ref[0:1, :], ids_ref[1:2, :]
    s0, s1 = scale_ref[0:1, :], scale_ref[1:2, :]
    rows = iota((experts, tok), 0)
    hit0, hit1 = rows == e0, rows == e1
    earlier = one_if(iota((tok, tok), 0) < iota((tok, tok), 1))
    before = jnp.dot(one_if(hit0 | hit1), earlier, preferred_element_type=f32)
    slot0 = jnp.sum(jnp.where(hit0, before, 0.0), axis=0, keepdims=True).astype(i32)
    slot1 = jnp.sum(jnp.where(hit1, before, 0.0), axis=0, keepdims=True).astype(i32)
    x = input_ref[...]
    grad = own_ref[...]
    diagonal = iota((tok, tok), 0) == iota((tok, tok), 1)
    c0 = jnp.sum(jnp.where(diagonal, s0, 0.0), axis=1, keepdims=True)
    c1 = jnp.sum(jnp.where(diagonal, s1, 0.0), axis=1, keepdims=True)
    g = grad.astype(f32)
    g0, g1 = (g * c0).astype(bf16), (g * c1).astype(bf16)
    pitch = sent_ref.shape[0] // experts
    r = iota((sent_ref.shape[0], tok), 0)
    a0, a1 = e0 * pitch + slot0, e1 * pitch + slot1
    half = pitch // 2
    sent = jnp.dot(one_if((r == a0) | (r == a1)), x, preferred_element_type=f32)
    sent = sent + jnp.dot(one_if(r == a0 + half), g0, preferred_element_type=f32)
    sent = sent + jnp.dot(one_if(r == a1 + half), g1, preferred_element_type=f32)
    sent_ref[...] = sent.astype(bf16)
    back_pitch = back_ref.shape[0] // experts
    r = iota((back_ref.shape[0], tok), 0)
    back_ref[...] = one_if((r == e0 * back_pitch + slot0) | (r == e1 * back_pitch + slot1))


def packed(block):
    lanes = 128
    wide = block[:, :lanes]
    rest = block[:, lanes:]
    rows = rest.shape[0] // 2
    return wide, jnp.concatenate([rest[:rows], rest[rows:]], axis=1)


def unpacked(wide, rest):
    lanes = rest.shape[1] // 2
    tail = jnp.concatenate([rest[:, :lanes], rest[:, lanes:]], axis=0)
    return jnp.concatenate([wide, tail], axis=1)


def compact_kernel(part_ref, norm_ref, out_ref, *, capacity, pitch):
    count = out_ref.shape[0]
    rows_in = part_ref.shape[0] // count
    rows_out = rows_in // pitch * capacity
    into, outof = iota((rows_out, rows_in), 0), iota((rows_out, rows_in), 1)
    pick_x = one_if(outof == (into // capacity) * pitch + into % capacity)
    pick_g = one_if(outof == (into // capacity) * pitch + into % capacity + pitch // 2)
    wide, rest = packed(norm_ref[...].astype(f32))
    wide, rest = wide.astype(bf16), rest.astype(bf16)
    for q in range(count):
        piece = part_ref[pl.ds(q * rows_in, rows_in), :]
        out_ref[q, pl.ds(0, rows_out), :] = jnp.dot(pick_x, piece, preferred_element_type=f32).astype(bf16)
        out_ref[q, pl.ds(rows_out, rows_out), :] = jnp.dot(pick_g, piece, preferred_element_type=f32).astype(bf16)
        out_ref[q, pl.ds(2 * rows_out, wide.shape[0]), :] = wide
        out_ref[q, pl.ds(2 * rows_out + wide.shape[0], rest.shape[0]), :] = rest


def pieces_of(core_ref, ny, nx):
    core = core_ref[0]
    return [
        (jnp.where(core == 0, y, x), jnp.where(core == 0, x, y)) for y in range(ny) for x in range(nx)
    ]


def pack_kernel(gate_ref, up_ref, down_ref, out_ref):
    height, width = gate_ref.shape
    out_ref[pl.ds(0, height), :] = gate_ref[...]
    out_ref[pl.ds(height, height), :] = up_ref[...]
    for k in range(height // width):
        out_ref[pl.ds(2 * height + k * width, width), :] = down_ref[:, pl.ds(k * width, width)]


def expert_kernel(core_ref, rows_hbm, *refs):
    weights_hbm = refs[0:5]
    back_ref, hidden_ref, both_ref, rows_ref = refs[5:9]
    weights, acc_ref, sems = refs[9:13], refs[13], refs[14]
    middle = weights_hbm[3].shape[0]
    targets = (rows_ref, *weights[:3], weights[3].at[pl.ds(0, middle)], weights[3].at[pl.ds(middle, middle)])
    copies = [
        pltpu.make_async_copy(source, target, sems.at[i])
        for i, (source, target) in enumerate(zip((rows_hbm, *weights_hbm), targets, strict=True))
    ]
    for copy in copies:
        copy.start()
    ny, nx, _, width = rows_ref.shape
    count = hidden_ref.shape[0]
    pieces = pieces_of(core_ref, ny, nx)
    height = ny * nx * width
    copies[0].wait()
    x = jnp.concatenate([rows_ref[a, b, pl.ds(0, count), :] for a, b in pieces], axis=1)
    g = jnp.concatenate([rows_ref[a, b, pl.ds(count, count), :] for a, b in pieces], axis=1)
    for k, block in enumerate(weights):
        copies[1 + k].wait()
        if k == 3:
            copies[5].wait()
        w_both = jnp.concatenate([block[pl.ds(0, height), :], block[pl.ds(height, height), :]], axis=1)
        w_down = jnp.concatenate(
            [block[pl.ds(2 * height + i * width, width), :] for i in range(ny * nx)], axis=1
        )
        pre = jnp.dot(x, w_both, preferred_element_type=f32)
        gate_pre, up_pre = pre[:, :width], pre[:, width:]
        d_hidden = contract(g, w_down, 1, 1)
        sig = jax.nn.sigmoid(gate_pre)
        gate_act = gate_pre * sig
        hidden_ref[:, pl.ds(k * width, width)] = (gate_act * up_pre).astype(bf16)
        d_gate = d_hidden * up_pre * (sig * (1.0 + gate_pre * (1.0 - sig)))
        d_up = d_hidden * gate_act
        both = jnp.concatenate([d_gate.astype(bf16), d_up.astype(bf16)], axis=1)
        both_ref[:, pl.ds(2 * k * width, 2 * width)] = both
        back = contract(both, w_both, 1, 1)
        acc_ref[...] = back if k == 0 else acc_ref[...] + back
    for j, (a, b) in enumerate(pieces):
        back_ref[a, b] = acc_ref[:, pl.ds(j * width, width)].astype(bf16)


def row_pack_kernel(core_ref, rows_ref, hidden_ref, both_ref, onward_ref, backward_ref, across_ref):
    ny, nx, _, width = rows_ref.shape
    count = hidden_ref.shape[0]
    for j, (a, b) in enumerate(pieces_of(core_ref, ny, nx)):
        rows = rows_ref[a, b, pl.ds(0, 2 * count), :]
        onward_ref[pl.ds(2 * j * count, 2 * count), :] = rows
        backward_ref[pl.ds(2 * j * count, 2 * count), :] = rows
    start = 2 * ny * nx * count
    for k, out_ref, at in ((2, onward_ref, start), (1, backward_ref, start), (3, across_ref, 0)):
        out_ref[pl.ds(at, count), :] = hidden_ref[:, pl.ds(k * width, width)]
        out_ref[pl.ds(at + count, count), :] = both_ref[:, pl.ds(2 * k * width, width)]
        out_ref[pl.ds(at + 2 * count, count), :] = both_ref[:, pl.ds((2 * k + 1) * width, width)]


def weight_kernel(own_ref, behind_ref, ahead_ref, low_ref, high_ref, across_ref, hidden_ref, both_ref, *outs):
    gate_ref, up_ref, down_ref = outs
    count, width = hidden_ref.shape[0], own_ref.shape[1]
    number = down_ref.shape[1] // width
    start = 2 * number * count

    def units(part, own):
        at = part * count
        return jnp.concatenate(
            [
                own,
                behind_ref[pl.ds(start + at, count), :],
                ahead_ref[pl.ds(start + at, count), :],
                across_ref[pl.ds(at, count), :],
            ],
            axis=0,
        )

    hidden = units(0, hidden_ref[:, :width])
    both = jnp.concatenate(
        [units(1, both_ref[:, :width]), units(2, both_ref[:, width : 2 * width])], axis=1
    )
    half = number // 2
    for j in range(number):
        far_ref, i = (low_ref, j) if j < half else (high_ref, j - half)

        def rows(part):
            at = (2 * j + part) * count
            near = [ref[pl.ds(at, count), :] for ref in (own_ref, behind_ref, ahead_ref)]
            return jnp.concatenate([*near, far_ref[pl.ds((2 * i + part) * count, count), :]], axis=0)

        pair = contract(rows(0), both, 0, 0)
        at = pl.ds(j * width, width)
        gate_ref[at, :] = pair[:, :width].astype(bf16)
        up_ref[at, :] = pair[:, width:].astype(bf16)
        down_ref[:, at] = contract(hidden, rows(1), 0, 0).astype(bf16)


def norm_kernel(core_ref, parts_ref, gain_ref, act_ref, slope_ref, cross_ref, stats_ref):
    ny, nx, height, _ = parts_ref.shape
    part = height * 2 // 3
    blocks = []
    for a, b in pieces_of(core_ref, ny, nx):
        block = parts_ref[a, b].astype(f32)
        blocks.append(unpacked(block[:part], block[part:]))
    values = jnp.concatenate(blocks, axis=0)
    channels = values.shape[0]
    mean = jnp.sum(values, axis=0, keepdims=True) / channels
    centred = values - mean
    inv = lax.rsqrt(jnp.sum(centred * centred, axis=0, keepdims=True) / channels + norm_eps)
    gain = gain_ref[...]
    normed = centred * inv
    scaled = normed * gain
    sig = jax.nn.sigmoid(scaled)
    act_ref[...] = (scaled * sig).astype(bf16)
    slope = sig * (1.0 + scaled * (1.0 - sig)) * gain
    slope_ref[...] = slope.astype(bf16)
    cross_ref[...] = (slope * normed).astype(bf16)
    stats_ref[0:1, :] = mean
    stats_ref[1:2, :] = inv


def line_sum_kernel(parts_ref, out_ref):
    acc = parts_ref[0].astype(f32)
    for j in range(1, parts_ref.shape[0]):
        acc = acc + parts_ref[j].astype(f32)
    out_ref[...] = acc.astype(bf16)


def spread_kernel(rows_ref, out_ref, *, capacity, pitch):
    count, rows_in, _ = rows_ref.shape
    rows_out = rows_in // capacity * pitch
    into, outof = iota((rows_out, rows_in), 0), iota((rows_out, rows_in), 1)
    spread = one_if((outof == (into // pitch) * capacity + into % pitch) & (into % pitch < capacity))
    for q in range(count):
        moved = jnp.dot(spread, rows_ref[q], preferred_element_type=f32)
        out_ref[pl.ds(q * rows_out, rows_out), :] = moved.astype(bf16)


def mix_kernel(core_ref, *refs):
    sources, outs, local, sems = refs[:7], refs[7:10], refs[10:17], refs[17]
    kept_ref, given_ref, blocks_ref = outs
    back_ref, returned_ref, own_ref, proj_ref, slope_ref, cross_ref, act_ref = local
    core = core_ref[0]
    copies = [
        pltpu.make_async_copy(source, target, sems.at[i])
        for i, (source, target) in enumerate(zip(sources, local, strict=True))
    ]
    for copy in copies:
        copy.start()
    for copy in copies[:3]:
        copy.wait()
    moe = contract(back_ref[...], returned_ref[...], 0, 0)
    mix = (own_ref[...].astype(f32) + moe).astype(bf16)
    for copy in copies[3:]:
        copy.wait()
    d_act = contract(proj_ref[...], mix, 1, 1)
    lanes = 128

    def as_rows(line):
        rest = line[:, lanes:]
        return [line[:, :lanes], jnp.concatenate([rest, jnp.zeros_like(rest)], axis=1)]

    tail = []
    for ref in (slope_ref, cross_ref):
        line = jnp.sum(ref[...].astype(f32) * d_act, axis=0, keepdims=True)
        high = line.astype(bf16).astype(f32)
        tail += as_rows(high) + as_rows(line - high)
    tail = jnp.concatenate(tail, axis=0).astype(bf16)
    count = blocks_ref.shape[0]
    part = d_act.shape[0] // count
    for j in range(count):
        wide, rest = packed(d_act[j * part : (j + 1) * part])
        blocks_ref[j, pl.ds(0, part), :] = wide.astype(bf16)
        blocks_ref[j, pl.ds(part, part // 2), :] = rest.astype(bf16)
        blocks_ref[j, pl.ds(part * 3 // 2, 8), :] = tail
    grad = jnp.dot(act_ref[...], mix, preferred_element_type=f32)
    size = kept_ref.shape[1]
    for k in range(kept_ref.shape[0]):
        even = grad[2 * k * size : (2 * k + 1) * size]
        odd = grad[(2 * k + 1) * size : (2 * k + 2) * size]
        kept_ref[k] = jnp.where(core == 0, even, odd).astype(bf16)
        given_ref[k] = jnp.where(core == 0, odd, even).astype(bf16)


def conv_grad_kernel(blocks_ref, norm_ref, gain_ref, stats_ref, out_ref, head_ref, *, channels):
    count, _, _ = blocks_ref.shape
    acc = blocks_ref[0].astype(f32)
    for j in range(1, count):
        acc = acc + blocks_ref[j].astype(f32)
    part = out_ref.shape[0]
    grad_act = unpacked(acc[:part], acc[part : part * 3 // 2])
    tail = acc[part * 3 // 2 :]

    def line(at):
        rest = tail[at + 1 : at + 2] + tail[at + 3 : at + 4]
        return jnp.concatenate([tail[at : at + 1] + tail[at + 2 : at + 3], rest[:, : rest.shape[1] // 2]], axis=1)

    mean, inv = stats_ref[0:1, :], stats_ref[1:2, :]
    gain = gain_ref[...]
    normed = (norm_ref[...].astype(f32) - mean) * inv
    grad_normed = grad_act * silu_grad(normed * gain) * gain
    out = inv * (grad_normed - line(0) / channels - normed * (line(4) / channels))
    out_ref[...] = out
    head_ref[...] = out[:, : head_ref.shape[1]]


def body(
    moe_input,
    out_grad,
    route_ids,
    route_weights,
    expert_gate,
    expert_up,
    expert_down,
    proj_weight,
    glu_value,
    glu_gate,
    conv_taps,
    norm_input,
    norm_gain,
):
    groups = lax.axis_size(SP)
    ny, nx = lax.axis_size("ty"), lax.axis_size("tx")
    lane_count = ny * nx
    lane_index = lax.axis_index(TP)
    tok_rows, model_width = moe_input.shape
    top_count = route_ids.shape[1]
    capacity = tok_rows * top_count * 3 // (2 * groups)
    total = groups * capacity
    width = model_width // lane_count
    pitch = 40
    back_pitch = 24
    channel_part = norm_input.shape[0]
    channels = channel_part * lane_count
    struct = jax.ShapeDtypeStruct

    sent, back_place, own_grad = pl.pallas_call(
        lambda *refs: prep_kernel(*refs, experts=groups),
        in_specs=[scalar()] + [pl.BlockSpec(memory_space=pltpu.HBM)] * 4,
        out_specs=[whole()] * 3,
        out_shape=[
            struct((groups * pitch, width), bf16),
            struct((groups * back_pitch, tok_rows), bf16),
            struct((tok_rows, width), bf16),
        ],
        scratch_shapes=[
            pltpu.VMEM((top_count, tok_rows), i32),
            pltpu.VMEM((top_count, tok_rows), f32),
            pltpu.VMEM((tok_rows, width), bf16),
            pltpu.SemaphoreType.DMA((4,)),
        ],
        compiler_params=params(58),
        name="prep",
    )(lane_index.astype(i32).reshape(1), route_ids.T, route_weights.T, moe_input, out_grad)

    part = exchanged(sent.reshape(groups, pitch, width), SP)

    core = lax.axis_index("core").astype(i32).reshape(1)
    first_groups, second_groups = line_groups(ny, nx)
    w_gate, w_up, w_down = expert_gate[0], expert_up[0], expert_down[0]
    ff = w_gate.shape[1]
    hbm = pl.BlockSpec(memory_space=pltpu.HBM)
    w_gate, w_up, w_down, _ = lax.optimization_barrier((w_gate, w_up, w_down, sent))
    own_weights = pl.pallas_call(
        pack_kernel,
        out_shape=struct((3 * model_width, ff), bf16),
        in_specs=[whole()] * 3,
        out_specs=whole(),
        compiler_params=params(58),
        cost_estimate=cost(8 * total * model_width * ff, 6 * model_width * ff),
        name="pack",
    )(w_gate, w_up, w_down)
    onward, backward, across = [line_pairs(ny, nx, by) for by in (1, -1, 2)]
    weights = (
        own_weights,
        lax.ppermute(own_weights, PLANE, onward),
        lax.ppermute(own_weights, PLANE, backward),
    )

    quarter = total // nx
    norm_rows = channel_part * 3 // 2
    rows_height = 2 * quarter + norm_rows
    quarters = pl.pallas_call(
        lambda *refs: compact_kernel(*refs, capacity=capacity, pitch=pitch),
        out_shape=struct((nx, rows_height, width), bf16),
        in_specs=[whole(), whole()],
        out_specs=whole(),
        compiler_params=params(16),
        name="compact",
    )(part.reshape(groups * pitch, width), norm_input)
    quarters = exchanged(quarters, PLANE, first_groups)
    weights = list(weights)
    middle = weights[0].shape[0] // 2
    weights += [
        lax.ppermute(weights[1][:middle], PLANE, onward),
        lax.ppermute(weights[2][middle:], PLANE, backward),
    ]
    gathered = exchanged(jnp.broadcast_to(quarters[None], (ny, *quarters.shape)), PLANE, second_groups)

    packed_weights = pltpu.VMEM((3 * model_width, ff), bf16)
    back, hidden, both = pl.pallas_call(
        expert_kernel,
        in_specs=[scalar()] + [hbm] * 6,
        out_specs=[whole()] * 3,
        out_shape=[
            struct((ny, nx, quarter, width), bf16),
            struct((quarter, nx * ff), bf16),
            struct((quarter, 2 * nx * ff), bf16),
        ],
        scratch_shapes=[
            pltpu.VMEM((ny, nx, rows_height, width), bf16),
            packed_weights,
            packed_weights,
            packed_weights,
            packed_weights,
            pltpu.VMEM((quarter, model_width), f32),
            pltpu.SemaphoreType.DMA((6,)),
        ],
        compiler_params=params(58),
        cost_estimate=cost(10 * total * model_width * ff, 10 * total * model_width),
        name="expert",
    )(core, gathered, *weights)

    line_parts = exchanged(back, PLANE, second_groups)
    unit_rows = 3 * quarter
    buffer_rows = 2 * lane_count * quarter + unit_rows
    to_onward, to_backward, to_across = pl.pallas_call(
        row_pack_kernel,
        in_specs=[scalar()] + [whole()] * 3,
        out_specs=[whole()] * 3,
        out_shape=[
            struct((buffer_rows, width), bf16),
            struct((buffer_rows, width), bf16),
            struct((unit_rows, width), bf16),
        ],
        compiler_params=params(58),
        cost_estimate=cost(6 * total * model_width * ff, 10 * total * model_width),
        name="row_pack",
    )(core, gathered, hidden, both)
    line_parts, to_onward, to_backward, to_across = lax.optimization_barrier(
        (line_parts, to_onward, to_backward, to_across)
    )
    line_rows = pl.pallas_call(
        line_sum_kernel,
        out_shape=struct((nx, quarter, width), bf16),
        in_specs=[whole()],
        out_specs=whole(),
        compiler_params=params(16),
        name="line_sum",
    )(line_parts)
    own_rows = exchanged(line_rows, PLANE, first_groups)
    summed_grad = pl.pallas_call(
        lambda *refs: spread_kernel(*refs, capacity=capacity, pitch=back_pitch),
        out_shape=struct((groups * back_pitch, width), bf16),
        in_specs=[whole()],
        out_specs=whole(),
        compiler_params=params(16),
        name="spread",
    )(own_rows)
    returned = exchanged(summed_grad.reshape(groups, back_pitch, width), SP)

    own_buffer = to_onward
    summed_grad, to_onward, to_backward, to_across = lax.optimization_barrier(
        (summed_grad, to_onward, to_backward, to_across)
    )
    from_behind = lax.ppermute(to_onward, PLANE, onward)
    from_ahead = lax.ppermute(to_backward, PLANE, backward)
    from_across = lax.ppermute(to_across, PLANE, across)
    far_rows = lane_count * quarter
    far_low = lax.ppermute(from_behind[:far_rows], PLANE, onward)
    far_high = lax.ppermute(from_ahead[far_rows : 2 * far_rows], PLANE, backward)

    act, slope, cross, stats = pl.pallas_call(
        norm_kernel,
        grid_spec=pltpu.PrefetchScalarGridSpec(
            num_scalar_prefetch=1,
            grid=(1,),
            in_specs=[
                pl.BlockSpec((ny, nx, norm_rows, width), lambda i, m: (0, 0, 2 * quarter // norm_rows, 0)),
                pl.BlockSpec((channels, 1), lambda i, m: (0, 0)),
            ],
            out_specs=[pl.BlockSpec((channels, tok_rows), lambda i, m: (0, 0))] * 3
            + [pl.BlockSpec((2, tok_rows), lambda i, m: (0, 0))],
        ),
        out_shape=[struct((channels, tok_rows), bf16)] * 3 + [struct((2, tok_rows), f32)],
        compiler_params=params(58),
        cost_estimate=cost(6 * total * model_width * ff, 10 * total * model_width),
        name="norm",
    )(core, gathered, norm_gain[:, None])

    proj_size = channels // groups
    block_rows = norm_rows + 8
    mix_inputs = (
        back_place,
        returned.reshape(groups * back_pitch, width),
        own_grad,
        proj_weight,
        slope,
        cross,
        act,
    )
    kept, given, blocks = pl.pallas_call(
        mix_kernel,
        out_shape=[
            struct((groups // 2, proj_size, width), bf16),
            struct((groups // 2, proj_size, width), bf16),
            struct((lane_count, block_rows, width), bf16),
        ],
        in_specs=[scalar()] + [pl.BlockSpec(memory_space=pltpu.HBM)] * len(mix_inputs),
        out_specs=[whole()] * 3,
        scratch_shapes=[pltpu.VMEM(value.shape, value.dtype) for value in mix_inputs]
        + [pltpu.SemaphoreType.DMA((len(mix_inputs),))],
        compiler_params=params(58),
        name="mix",
    )(core, *mix_inputs)
    arrived = exchanged(blocks, TP)
    from_pair = lax.ppermute(given, "core", [(0, 1), (1, 0)])
    chip_sum = (kept.astype(f32) + from_pair.astype(f32)).astype(bf16)
    chip_sum, arrived = lax.optimization_barrier((chip_sum, arrived))
    proj_parts = exchanged(chip_sum, "z")
    grad_proj = jnp.sum(proj_parts.astype(f32), axis=0)

    taps_count = conv_taps.shape[1]
    reach_back = taps_count - 1
    gain_own = lax.dynamic_slice_in_dim(norm_gain, lane_index * channel_part, channel_part, 0)
    grad_conv, head = pl.pallas_call(
        lambda *refs: conv_grad_kernel(*refs, channels=channels),
        out_shape=[struct((channel_part, tok_rows), f32), struct((channel_part, reach_back), f32)],
        in_specs=[whole()] * 4,
        out_specs=[whole()] * 2,
        compiler_params=params(16),
        name="conv_grad",
    )(arrived, norm_input, gain_own[:, None], stats)

    pairs = [(i, i - 1) for i in range(1, groups)]
    ahead_rows = lax.ppermute(head, SP, pairs)
    extended = jnp.concatenate([grad_conv, ahead_rows], axis=1)
    grad_glu = jnp.zeros_like(grad_conv)
    for tap_index in range(taps_count):
        grad_glu = (
            grad_glu
            + conv_taps[:, tap_index : tap_index + 1]
            * extended[:, reach_back - tap_index : reach_back - tap_index + tok_rows]
        )
    sigmoid_gate = jax.nn.sigmoid(glu_gate.astype(f32))
    grad_value = (grad_glu * sigmoid_gate).astype(bf16)
    grad_glu_gate = (
        grad_glu * glu_value.astype(f32) * sigmoid_gate * (1.0 - sigmoid_gate)
    ).astype(bf16)
    gate_wgrad, up_wgrad, down_grad = pl.pallas_call(
        weight_kernel,
        in_specs=[whole()] * 8,
        out_specs=[whole()] * 3,
        out_shape=[
            struct((model_width, ff), bf16),
            struct((model_width, ff), bf16),
            struct((ff, model_width), bf16),
        ],
        compiler_params=params(58),
        cost_estimate=cost(6 * total * model_width * ff, 10 * total * model_width),
        name="weight_sum",
    )(own_buffer, from_behind, from_ahead, far_low, far_high, from_across, hidden, both)
    return (gate_wgrad[None], up_wgrad[None], down_grad[None], grad_proj, grad_value, grad_glu_gate)


def solution(mesh):
    finer = Mesh(mesh.devices.reshape(mesh.shape["sp"] // 2, 2, 4, 4), ("z", "core", "ty", "tx"))
    return jax.shard_map(
        body,
        mesh=finer,
        in_specs=(
            P(SP, None),
            P(SP, None),
            P(SP, None),
            P(SP, None),
            P(SP, None, TP),
            P(SP, None, TP),
            P(SP, TP, None),
            P(None, TP),
            P(TP, SP),
            P(TP, SP),
            P(TP, None),
            P(TP, SP),
            P(),
        ),
        out_specs=(
            P(SP, None, TP),
            P(SP, None, TP),
            P(SP, TP, None),
            P(SP, TP),
            P(TP, SP),
            P(TP, SP),
        ),
        check_vma=False,
    )
```

```python
import jax
import jax.numpy as jnp
from jax import lax
from jax.experimental import pallas as pl
from jax.experimental.pallas import tpu as pltpu
from jax.sharding import Mesh
from jax.sharding import PartitionSpec as P

TP = ("ty", "tx")
SP = ("z", "core")
PLANE = ("core", "ty", "tx")


norm_eps = 1e-05

bf16, f32, i32 = jnp.bfloat16, jnp.float32, jnp.int32


def exchanged(blocks, axis, index_groups=None):
    return lax.all_to_all(blocks, axis, 0, 0, axis_index_groups=index_groups, tiled=True)


def line_groups(ny, nx):
    along_x = [[y * nx + x for x in range(nx)] for y in range(ny)]
    along_y = [[y * nx + x for y in range(ny)] for x in range(nx)]

    def of_core_one(lines):
        return [[ny * nx + i for i in line] for line in lines]

    return along_x + of_core_one(along_y), along_y + of_core_one(along_x)


def line_pairs(ny, nx, by):
    pairs = []
    for y in range(ny):
        for x in range(nx):
            pairs.append((y * nx + x, y * nx + (x + by) % nx))
            pairs.append((ny * nx + y * nx + x, ny * nx + (y + by) % ny * nx + x))
    return pairs


def silu_grad(pre):
    sig = jax.nn.sigmoid(pre)
    return sig * (1.0 + pre * (1.0 - sig))


def contract(a, b, dim_a, dim_b):
    return lax.dot_general(a, b, (((dim_a,), (dim_b,)), ((), ())), preferred_element_type=f32)


def iota(shape, dim):
    return lax.broadcasted_iota(i32, shape, dim)


def whole():
    return pl.BlockSpec(memory_space=pltpu.VMEM)


def scalar():
    return pl.BlockSpec(memory_space=pltpu.SMEM)


def params(mib):
    return pltpu.CompilerParams(vmem_limit_bytes=mib * 1024 * 1024)


def cost(flops, size):
    return pl.CostEstimate(flops=flops, bytes_accessed=size, transcendentals=0)


def one_if(condition):
    return jnp.where(condition, 1.0, 0.0).astype(bf16)


def prep_kernel(lane_ref, ids_hbm, scale_hbm, input_hbm, grad_hbm, *refs, experts):
    sent_ref, back_ref, own_ref, ids_ref, scale_ref, input_ref, sems = refs
    tok, width = input_ref.shape
    columns = pl.ds(pl.multiple_of(lane_ref[0] * width, width), width)
    copies = [
        pltpu.make_async_copy(ids_hbm, ids_ref, sems.at[0]),
        pltpu.make_async_copy(scale_hbm, scale_ref, sems.at[1]),
        pltpu.make_async_copy(input_hbm.at[:, columns], input_ref, sems.at[2]),
        pltpu.make_async_copy(grad_hbm.at[:, columns], own_ref, sems.at[3]),
    ]
    for copy in copies:
        copy.start()
    for copy in copies:
        copy.wait()
    e0, e1 = ids_ref[0:1, :], ids_ref[1:2, :]
    s0, s1 = scale_ref[0:1, :], scale_ref[1:2, :]
    rows = iota((experts, tok), 0)
    hit0, hit1 = rows == e0, rows == e1
    earlier = one_if(iota((tok, tok), 0) < iota((tok, tok), 1))
    before = jnp.dot(one_if(hit0 | hit1), earlier, preferred_element_type=f32)
    slot0 = jnp.sum(jnp.where(hit0, before, 0.0), axis=0, keepdims=True).astype(i32)
    slot1 = jnp.sum(jnp.where(hit1, before, 0.0), axis=0, keepdims=True).astype(i32)
    x = input_ref[...]
    grad = own_ref[...]
    diagonal = iota((tok, tok), 0) == iota((tok, tok), 1)
    c0 = jnp.sum(jnp.where(diagonal, s0, 0.0), axis=1, keepdims=True)
    c1 = jnp.sum(jnp.where(diagonal, s1, 0.0), axis=1, keepdims=True)
    g = grad.astype(f32)
    g0, g1 = (g * c0).astype(bf16), (g * c1).astype(bf16)
    pitch = sent_ref.shape[0] // experts
    r = iota((sent_ref.shape[0], tok), 0)
    a0, a1 = e0 * pitch + slot0, e1 * pitch + slot1
    half = pitch // 2
    sent = jnp.dot(one_if((r == a0) | (r == a1)), x, preferred_element_type=f32)
    sent = sent + jnp.dot(one_if(r == a0 + half), g0, preferred_element_type=f32)
    sent = sent + jnp.dot(one_if(r == a1 + half), g1, preferred_element_type=f32)
    sent_ref[...] = sent.astype(bf16)
    back_pitch = back_ref.shape[0] // experts
    r = iota((back_ref.shape[0], tok), 0)
    back_ref[...] = one_if((r == e0 * back_pitch + slot0) | (r == e1 * back_pitch + slot1))


def packed(block):
    lanes = 128
    wide = block[:, :lanes]
    rest = block[:, lanes:]
    rows = rest.shape[0] // 2
    return wide, jnp.concatenate([rest[:rows], rest[rows:]], axis=1)


def unpacked(wide, rest):
    lanes = rest.shape[1] // 2
    tail = jnp.concatenate([rest[:, :lanes], rest[:, lanes:]], axis=0)
    return jnp.concatenate([wide, tail], axis=1)


def compact_kernel(part_ref, norm_ref, out_ref, *, capacity, pitch):
    count = out_ref.shape[0]
    rows_in = part_ref.shape[0] // count
    rows_out = rows_in // pitch * capacity
    into, outof = iota((rows_out, rows_in), 0), iota((rows_out, rows_in), 1)
    pick_x = one_if(outof == (into // capacity) * pitch + into % capacity)
    pick_g = one_if(outof == (into // capacity) * pitch + into % capacity + pitch // 2)
    wide, rest = packed(norm_ref[...].astype(f32))
    wide, rest = wide.astype(bf16), rest.astype(bf16)
    for q in range(count):
        piece = part_ref[pl.ds(q * rows_in, rows_in), :]
        out_ref[q, pl.ds(0, rows_out), :] = jnp.dot(pick_x, piece, preferred_element_type=f32).astype(bf16)
        out_ref[q, pl.ds(rows_out, rows_out), :] = jnp.dot(pick_g, piece, preferred_element_type=f32).astype(bf16)
        out_ref[q, pl.ds(2 * rows_out, wide.shape[0]), :] = wide
        out_ref[q, pl.ds(2 * rows_out + wide.shape[0], rest.shape[0]), :] = rest


def pieces_of(core_ref, ny, nx):
    core = core_ref[0]
    return [
        (jnp.where(core == 0, y, x), jnp.where(core == 0, x, y)) for y in range(ny) for x in range(nx)
    ]


def pack_kernel(gate_ref, up_ref, down_ref, out_ref):
    height, width = gate_ref.shape
    out_ref[pl.ds(0, height), :] = gate_ref[...]
    out_ref[pl.ds(height, height), :] = up_ref[...]
    for k in range(height // width):
        out_ref[pl.ds(2 * height + k * width, width), :] = down_ref[:, pl.ds(k * width, width)]


def expert_kernel(core_ref, rows_hbm, *refs):
    weights_hbm = refs[0:5]
    back_ref, hidden_ref, both_ref, rows_ref = refs[5:9]
    weights, acc_ref, sems = refs[9:13], refs[13], refs[14]
    middle = weights_hbm[3].shape[0]
    targets = (rows_ref, *weights[:3], weights[3].at[pl.ds(0, middle)], weights[3].at[pl.ds(middle, middle)])
    copies = [
        pltpu.make_async_copy(source, target, sems.at[i])
        for i, (source, target) in enumerate(zip((rows_hbm, *weights_hbm), targets, strict=True))
    ]
    for copy in copies:
        copy.start()
    ny, nx, _, width = rows_ref.shape
    count = hidden_ref.shape[0]
    pieces = pieces_of(core_ref, ny, nx)
    height = ny * nx * width
    copies[0].wait()
    x = jnp.concatenate([rows_ref[a, b, pl.ds(0, count), :] for a, b in pieces], axis=1)
    g = jnp.concatenate([rows_ref[a, b, pl.ds(count, count), :] for a, b in pieces], axis=1)
    for k, block in enumerate(weights):
        copies[1 + k].wait()
        if k == 3:
            copies[5].wait()
        w_both = jnp.concatenate([block[pl.ds(0, height), :], block[pl.ds(height, height), :]], axis=1)
        w_down = jnp.concatenate(
            [block[pl.ds(2 * height + i * width, width), :] for i in range(ny * nx)], axis=1
        )
        pre = jnp.dot(x, w_both, preferred_element_type=f32)
        gate_pre, up_pre = pre[:, :width], pre[:, width:]
        d_hidden = contract(g, w_down, 1, 1)
        sig = jax.nn.sigmoid(gate_pre)
        gate_act = gate_pre * sig
        hidden_ref[:, pl.ds(k * width, width)] = (gate_act * up_pre).astype(bf16)
        d_gate = d_hidden * up_pre * (sig * (1.0 + gate_pre * (1.0 - sig)))
        d_up = d_hidden * gate_act
        both = jnp.concatenate([d_gate.astype(bf16), d_up.astype(bf16)], axis=1)
        both_ref[:, pl.ds(2 * k * width, 2 * width)] = both
        back = contract(both, w_both, 1, 1)
        acc_ref[...] = back if k == 0 else acc_ref[...] + back
    for j, (a, b) in enumerate(pieces):
        back_ref[a, b] = acc_ref[:, pl.ds(j * width, width)].astype(bf16)


def row_pack_kernel(core_ref, rows_ref, hidden_ref, both_ref, onward_ref, backward_ref, across_ref):
    ny, nx, _, width = rows_ref.shape
    count = hidden_ref.shape[0]
    for j, (a, b) in enumerate(pieces_of(core_ref, ny, nx)):
        rows = rows_ref[a, b, pl.ds(0, 2 * count), :]
        onward_ref[pl.ds(2 * j * count, 2 * count), :] = rows
        backward_ref[pl.ds(2 * j * count, 2 * count), :] = rows
    start = 2 * ny * nx * count
    for k, out_ref, at in ((2, onward_ref, start), (1, backward_ref, start), (3, across_ref, 0)):
        out_ref[pl.ds(at, count), :] = hidden_ref[:, pl.ds(k * width, width)]
        out_ref[pl.ds(at + count, count), :] = both_ref[:, pl.ds(2 * k * width, width)]
        out_ref[pl.ds(at + 2 * count, count), :] = both_ref[:, pl.ds((2 * k + 1) * width, width)]


def weight_kernel(own_ref, behind_ref, ahead_ref, low_ref, high_ref, across_ref, hidden_ref, both_ref, *outs):
    gate_ref, up_ref, down_ref = outs
    count, width = hidden_ref.shape[0], own_ref.shape[1]
    number = down_ref.shape[1] // width
    start = 2 * number * count

    def units(part, own):
        at = part * count
        return jnp.concatenate(
            [
                own,
                behind_ref[pl.ds(start + at, count), :],
                ahead_ref[pl.ds(start + at, count), :],
                across_ref[pl.ds(at, count), :],
            ],
            axis=0,
        )

    hidden = units(0, hidden_ref[:, :width])
    both = jnp.concatenate(
        [units(1, both_ref[:, :width]), units(2, both_ref[:, width : 2 * width])], axis=1
    )
    half = number // 2
    for j in range(number):
        far_ref, i = (low_ref, j) if j < half else (high_ref, j - half)

        def rows(part):
            at = (2 * j + part) * count
            near = [ref[pl.ds(at, count), :] for ref in (own_ref, behind_ref, ahead_ref)]
            return jnp.concatenate([*near, far_ref[pl.ds((2 * i + part) * count, count), :]], axis=0)

        pair = contract(rows(0), both, 0, 0)
        at = pl.ds(j * width, width)
        gate_ref[at, :] = pair[:, :width].astype(bf16)
        up_ref[at, :] = pair[:, width:].astype(bf16)
        down_ref[:, at] = contract(hidden, rows(1), 0, 0).astype(bf16)


def norm_kernel(core_ref, parts_ref, gain_ref, act_ref, slope_ref, cross_ref, stats_ref):
    ny, nx, height, _ = parts_ref.shape
    part = height * 2 // 3
    blocks = []
    for a, b in pieces_of(core_ref, ny, nx):
        block = parts_ref[a, b].astype(f32)
        blocks.append(unpacked(block[:part], block[part:]))
    values = jnp.concatenate(blocks, axis=0)
    channels = values.shape[0]
    mean = jnp.sum(values, axis=0, keepdims=True) / channels
    centred = values - mean
    inv = lax.rsqrt(jnp.sum(centred * centred, axis=0, keepdims=True) / channels + norm_eps)
    gain = gain_ref[...]
    normed = centred * inv
    scaled = normed * gain
    sig = jax.nn.sigmoid(scaled)
    act_ref[...] = (scaled * sig).astype(bf16)
    slope = sig * (1.0 + scaled * (1.0 - sig)) * gain
    slope_ref[...] = slope.astype(bf16)
    cross_ref[...] = (slope * normed).astype(bf16)
    stats_ref[0:1, :] = mean
    stats_ref[1:2, :] = inv


def line_sum_kernel(parts_ref, out_ref):
    acc = parts_ref[0].astype(f32)
    for j in range(1, parts_ref.shape[0]):
        acc = acc + parts_ref[j].astype(f32)
    out_ref[...] = acc.astype(bf16)


def spread_kernel(rows_ref, out_ref, *, capacity, pitch):
    count, rows_in, _ = rows_ref.shape
    rows_out = rows_in // capacity * pitch
    into, outof = iota((rows_out, rows_in), 0), iota((rows_out, rows_in), 1)
    spread = one_if((outof == (into // pitch) * capacity + into % pitch) & (into % pitch < capacity))
    for q in range(count):
        moved = jnp.dot(spread, rows_ref[q], preferred_element_type=f32)
        out_ref[pl.ds(q * rows_out, rows_out), :] = moved.astype(bf16)


def mix_kernel(core_ref, *refs):
    sources, outs, local, sems = refs[:7], refs[7:10], refs[10:17], refs[17]
    kept_ref, given_ref, blocks_ref = outs
    back_ref, returned_ref, own_ref, proj_ref, slope_ref, cross_ref, act_ref = local
    core = core_ref[0]
    copies = [
        pltpu.make_async_copy(source, target, sems.at[i])
        for i, (source, target) in enumerate(zip(sources, local, strict=True))
    ]
    for copy in copies:
        copy.start()
    for copy in copies[:3]:
        copy.wait()
    moe = contract(back_ref[...], returned_ref[...], 0, 0)
    mix = (own_ref[...].astype(f32) + moe).astype(bf16)
    copies[3].wait()
    d_act = contract(proj_ref[...], mix, 1, 1)
    copies[6].wait()
    grad = jnp.dot(act_ref[...], mix, preferred_element_type=f32)
    copies[4].wait()
    copies[5].wait()
    lanes = 128

    def as_rows(line):
        rest = line[:, lanes:]
        return [line[:, :lanes], jnp.concatenate([rest, jnp.zeros_like(rest)], axis=1)]

    tail = []
    for ref in (slope_ref, cross_ref):
        line = jnp.sum(ref[...].astype(f32) * d_act, axis=0, keepdims=True)
        high = line.astype(bf16).astype(f32)
        tail += as_rows(high) + as_rows(line - high)
    tail = jnp.concatenate(tail, axis=0).astype(bf16)
    count = blocks_ref.shape[0]
    part = d_act.shape[0] // count
    for j in range(count):
        wide, rest = packed(d_act[j * part : (j + 1) * part])
        blocks_ref[j, pl.ds(0, part), :] = wide.astype(bf16)
        blocks_ref[j, pl.ds(part, part // 2), :] = rest.astype(bf16)
        blocks_ref[j, pl.ds(part * 3 // 2, 8), :] = tail
    size = kept_ref.shape[1]
    for k in range(kept_ref.shape[0]):
        even = grad[2 * k * size : (2 * k + 1) * size]
        odd = grad[(2 * k + 1) * size : (2 * k + 2) * size]
        kept_ref[k] = jnp.where(core == 0, even, odd).astype(bf16)
        given_ref[k] = jnp.where(core == 0, odd, even).astype(bf16)


def conv_grad_kernel(blocks_ref, norm_ref, gain_ref, stats_ref, out_ref, head_ref, *, channels):
    count, _, _ = blocks_ref.shape
    acc = blocks_ref[0].astype(f32)
    for j in range(1, count):
        acc = acc + blocks_ref[j].astype(f32)
    part = out_ref.shape[0]
    grad_act = unpacked(acc[:part], acc[part : part * 3 // 2])
    tail = acc[part * 3 // 2 :]

    def line(at):
        rest = tail[at + 1 : at + 2] + tail[at + 3 : at + 4]
        return jnp.concatenate([tail[at : at + 1] + tail[at + 2 : at + 3], rest[:, : rest.shape[1] // 2]], axis=1)

    mean, inv = stats_ref[0:1, :], stats_ref[1:2, :]
    gain = gain_ref[...]
    normed = (norm_ref[...].astype(f32) - mean) * inv
    grad_normed = grad_act * silu_grad(normed * gain) * gain
    out = inv * (grad_normed - line(0) / channels - normed * (line(4) / channels))
    out_ref[...] = out
    head_ref[...] = out[:, : head_ref.shape[1]]


def body(
    moe_input,
    out_grad,
    route_ids,
    route_weights,
    expert_gate,
    expert_up,
    expert_down,
    proj_weight,
    glu_value,
    glu_gate,
    conv_taps,
    norm_input,
    norm_gain,
):
    groups = lax.axis_size(SP)
    ny, nx = lax.axis_size("ty"), lax.axis_size("tx")
    lane_count = ny * nx
    lane_index = lax.axis_index(TP)
    tok_rows, model_width = moe_input.shape
    top_count = route_ids.shape[1]
    capacity = tok_rows * top_count * 3 // (2 * groups)
    total = groups * capacity
    width = model_width // lane_count
    pitch = 40
    back_pitch = 24
    channel_part = norm_input.shape[0]
    channels = channel_part * lane_count
    struct = jax.ShapeDtypeStruct

    sent, back_place, own_grad = pl.pallas_call(
        lambda *refs: prep_kernel(*refs, experts=groups),
        in_specs=[scalar()] + [pl.BlockSpec(memory_space=pltpu.HBM)] * 4,
        out_specs=[whole()] * 3,
        out_shape=[
            struct((groups * pitch, width), bf16),
            struct((groups * back_pitch, tok_rows), bf16),
            struct((tok_rows, width), bf16),
        ],
        scratch_shapes=[
            pltpu.VMEM((top_count, tok_rows), i32),
            pltpu.VMEM((top_count, tok_rows), f32),
            pltpu.VMEM((tok_rows, width), bf16),
            pltpu.SemaphoreType.DMA((4,)),
        ],
        compiler_params=params(58),
        name="prep",
    )(lane_index.astype(i32).reshape(1), route_ids.T, route_weights.T, moe_input, out_grad)

    part = exchanged(sent.reshape(groups, pitch, width), SP)

    core = lax.axis_index("core").astype(i32).reshape(1)
    first_groups, second_groups = line_groups(ny, nx)
    w_gate, w_up, w_down = expert_gate[0], expert_up[0], expert_down[0]
    ff = w_gate.shape[1]
    hbm = pl.BlockSpec(memory_space=pltpu.HBM)
    w_gate, w_up, w_down, _ = lax.optimization_barrier((w_gate, w_up, w_down, sent))
    own_weights = pl.pallas_call(
        pack_kernel,
        out_shape=struct((3 * model_width, ff), bf16),
        in_specs=[whole()] * 3,
        out_specs=whole(),
        compiler_params=params(58),
        cost_estimate=cost(8 * total * model_width * ff, 6 * model_width * ff),
        name="pack",
    )(w_gate, w_up, w_down)
    onward, backward, across = [line_pairs(ny, nx, by) for by in (1, -1, 2)]
    weights = (
        own_weights,
        lax.ppermute(own_weights, PLANE, onward),
        lax.ppermute(own_weights, PLANE, backward),
    )

    quarter = total // nx
    norm_rows = channel_part * 3 // 2
    rows_height = 2 * quarter + norm_rows
    quarters = pl.pallas_call(
        lambda *refs: compact_kernel(*refs, capacity=capacity, pitch=pitch),
        out_shape=struct((nx, rows_height, width), bf16),
        in_specs=[whole(), whole()],
        out_specs=whole(),
        compiler_params=params(16),
        name="compact",
    )(part.reshape(groups * pitch, width), norm_input)
    quarters = exchanged(quarters, PLANE, first_groups)
    weights = list(weights)
    middle = weights[0].shape[0] // 2
    weights += [
        lax.ppermute(weights[1][:middle], PLANE, onward),
        lax.ppermute(weights[2][middle:], PLANE, backward),
    ]
    gathered = exchanged(jnp.broadcast_to(quarters[None], (ny, *quarters.shape)), PLANE, second_groups)

    packed_weights = pltpu.VMEM((3 * model_width, ff), bf16)
    back, hidden, both = pl.pallas_call(
        expert_kernel,
        in_specs=[scalar()] + [hbm] * 6,
        out_specs=[whole()] * 3,
        out_shape=[
            struct((ny, nx, quarter, width), bf16),
            struct((quarter, nx * ff), bf16),
            struct((quarter, 2 * nx * ff), bf16),
        ],
        scratch_shapes=[
            pltpu.VMEM((ny, nx, rows_height, width), bf16),
            packed_weights,
            packed_weights,
            packed_weights,
            packed_weights,
            pltpu.VMEM((quarter, model_width), f32),
            pltpu.SemaphoreType.DMA((6,)),
        ],
        compiler_params=params(58),
        cost_estimate=cost(10 * total * model_width * ff, 10 * total * model_width),
        name="expert",
    )(core, gathered, *weights)

    line_parts = exchanged(back, PLANE, second_groups)
    unit_rows = 3 * quarter
    buffer_rows = 2 * lane_count * quarter + unit_rows
    to_onward, to_backward, to_across = pl.pallas_call(
        row_pack_kernel,
        in_specs=[scalar()] + [whole()] * 3,
        out_specs=[whole()] * 3,
        out_shape=[
            struct((buffer_rows, width), bf16),
            struct((buffer_rows, width), bf16),
            struct((unit_rows, width), bf16),
        ],
        compiler_params=params(58),
        cost_estimate=cost(6 * total * model_width * ff, 10 * total * model_width),
        name="row_pack",
    )(core, gathered, hidden, both)
    line_parts, to_onward, to_backward, to_across = lax.optimization_barrier(
        (line_parts, to_onward, to_backward, to_across)
    )
    line_rows = pl.pallas_call(
        line_sum_kernel,
        out_shape=struct((nx, quarter, width), bf16),
        in_specs=[whole()],
        out_specs=whole(),
        compiler_params=params(16),
        name="line_sum",
    )(line_parts)
    own_rows = exchanged(line_rows, PLANE, first_groups)
    summed_grad = pl.pallas_call(
        lambda *refs: spread_kernel(*refs, capacity=capacity, pitch=back_pitch),
        out_shape=struct((groups * back_pitch, width), bf16),
        in_specs=[whole()],
        out_specs=whole(),
        compiler_params=params(16),
        name="spread",
    )(own_rows)
    returned = exchanged(summed_grad.reshape(groups, back_pitch, width), SP)

    own_buffer = to_onward
    summed_grad, to_onward, to_backward, to_across = lax.optimization_barrier(
        (summed_grad, to_onward, to_backward, to_across)
    )
    from_behind = lax.ppermute(to_onward, PLANE, onward)
    from_ahead = lax.ppermute(to_backward, PLANE, backward)
    from_across = lax.ppermute(to_across, PLANE, across)
    far_rows = lane_count * quarter
    far_low = lax.ppermute(from_behind[:far_rows], PLANE, onward)
    far_high = lax.ppermute(from_ahead[far_rows : 2 * far_rows], PLANE, backward)

    act, slope, cross, stats = pl.pallas_call(
        norm_kernel,
        grid_spec=pltpu.PrefetchScalarGridSpec(
            num_scalar_prefetch=1,
            grid=(1,),
            in_specs=[
                pl.BlockSpec((ny, nx, norm_rows, width), lambda i, m: (0, 0, 2 * quarter // norm_rows, 0)),
                pl.BlockSpec((channels, 1), lambda i, m: (0, 0)),
            ],
            out_specs=[pl.BlockSpec((channels, tok_rows), lambda i, m: (0, 0))] * 3
            + [pl.BlockSpec((2, tok_rows), lambda i, m: (0, 0))],
        ),
        out_shape=[struct((channels, tok_rows), bf16)] * 3 + [struct((2, tok_rows), f32)],
        compiler_params=params(58),
        cost_estimate=cost(6 * total * model_width * ff, 10 * total * model_width),
        name="norm",
    )(core, gathered, norm_gain[:, None])

    proj_size = channels // groups
    block_rows = norm_rows + 8
    mix_inputs = (
        back_place,
        returned.reshape(groups * back_pitch, width),
        own_grad,
        proj_weight,
        slope,
        cross,
        act,
    )
    kept, given, blocks = pl.pallas_call(
        mix_kernel,
        out_shape=[
            struct((groups // 2, proj_size, width), bf16),
            struct((groups // 2, proj_size, width), bf16),
            struct((lane_count, block_rows, width), bf16),
        ],
        in_specs=[scalar()] + [pl.BlockSpec(memory_space=pltpu.HBM)] * len(mix_inputs),
        out_specs=[whole()] * 3,
        scratch_shapes=[pltpu.VMEM(value.shape, value.dtype) for value in mix_inputs]
        + [pltpu.SemaphoreType.DMA((len(mix_inputs),))],
        compiler_params=params(58),
        name="mix",
    )(core, *mix_inputs)
    arrived = exchanged(blocks, TP)
    from_pair = lax.ppermute(given, "core", [(0, 1), (1, 0)])
    chip_sum = (kept.astype(f32) + from_pair.astype(f32)).astype(bf16)
    chip_sum, arrived = lax.optimization_barrier((chip_sum, arrived))
    proj_parts = exchanged(chip_sum, "z")
    grad_proj = jnp.sum(proj_parts.astype(f32), axis=0)

    taps_count = conv_taps.shape[1]
    reach_back = taps_count - 1
    gain_own = lax.dynamic_slice_in_dim(norm_gain, lane_index * channel_part, channel_part, 0)
    grad_conv, head = pl.pallas_call(
        lambda *refs: conv_grad_kernel(*refs, channels=channels),
        out_shape=[struct((channel_part, tok_rows), f32), struct((channel_part, reach_back), f32)],
        in_specs=[whole()] * 4,
        out_specs=[whole()] * 2,
        compiler_params=params(16),
        name="conv_grad",
    )(arrived, norm_input, gain_own[:, None], stats)

    pairs = [(i, i - 1) for i in range(1, groups)]
    ahead_rows = lax.ppermute(head, SP, pairs)
    extended = jnp.concatenate([grad_conv, ahead_rows], axis=1)
    grad_glu = jnp.zeros_like(grad_conv)
    for tap_index in range(taps_count):
        grad_glu = (
            grad_glu
            + conv_taps[:, tap_index : tap_index + 1]
            * extended[:, reach_back - tap_index : reach_back - tap_index + tok_rows]
        )
    sigmoid_gate = jax.nn.sigmoid(glu_gate.astype(f32))
    grad_value = (grad_glu * sigmoid_gate).astype(bf16)
    grad_glu_gate = (
        grad_glu * glu_value.astype(f32) * sigmoid_gate * (1.0 - sigmoid_gate)
    ).astype(bf16)
    gate_wgrad, up_wgrad, down_grad = pl.pallas_call(
        weight_kernel,
        in_specs=[whole()] * 8,
        out_specs=[whole()] * 3,
        out_shape=[
            struct((model_width, ff), bf16),
            struct((model_width, ff), bf16),
            struct((ff, model_width), bf16),
        ],
        compiler_params=params(58),
        cost_estimate=cost(6 * total * model_width * ff, 10 * total * model_width),
        name="weight_sum",
    )(own_buffer, from_behind, from_ahead, far_low, far_high, from_across, hidden, both)
    return (gate_wgrad[None], up_wgrad[None], down_grad[None], grad_proj, grad_value, grad_glu_gate)


def solution(mesh):
    finer = Mesh(mesh.devices.reshape(mesh.shape["sp"] // 2, 2, 4, 4), ("z", "core", "ty", "tx"))
    return jax.shard_map(
        body,
        mesh=finer,
        in_specs=(
            P(SP, None),
            P(SP, None),
            P(SP, None),
            P(SP, None),
            P(SP, None, TP),
            P(SP, None, TP),
            P(SP, TP, None),
            P(None, TP),
            P(TP, SP),
            P(TP, SP),
            P(TP, None),
            P(TP, SP),
            P(),
        ),
        out_specs=(
            P(SP, None, TP),
            P(SP, None, TP),
            P(SP, TP, None),
            P(SP, TP),
            P(TP, SP),
            P(TP, SP),
        ),
        check_vma=False,
    )
```
